256 devices in a mesh: sp: 32 (over z, y), tp: 4 (over x), dp: 2 (over core).
Axes of the slice: x: 4, y: 4, z: 8, core: 2. Of those that a mesh axis runs over, the one named last changes fastest.
Arguments:
- latent: bfloat16 [2, 32768, 2048], P('dp', 'sp'), may hold values from -4 to 4
- context: bfloat16 [2, 768, 2048], P('dp', 'sp'), may hold values from -6 to 6
- cond: float32 [2, 2048], P('dp'), may hold values from -6 to 6
- ctx_cond: float32 [2048], replicated, may hold values from -6 to 6
- norm_gain: float32 [2048], replicated, may hold values from 0.1 to 1.9
- mod_shift: bfloat16 [2048, 2048], P('sp', 'tp'), may hold values from -0.125 to 0.125
- mod_scale: bfloat16 [2048, 2048], P('sp', 'tp'), may hold values from -0.125 to 0.125
- mod_gate: bfloat16 [2048, 2048], P('sp', 'tp'), may hold values from -0.125 to 0.125
- w_query: bfloat16 [2048, 2048], P(None, 'tp'), may hold values from -0.125 to 0.125
- w_key: bfloat16 [2048, 512], P(None, 'tp'), may hold values from -0.125 to 0.125
- w_value: bfloat16 [2048, 512], P(None, 'tp'), may hold values from -0.125 to 0.125
- w_out: bfloat16 [2048, 2048], P('tp'), may hold values from -2 to 2
- q_gain: float32 [128], replicated, may hold values from 0.1 to 1.9
- k_gain: float32 [128], replicated, may hold values from 0.1 to 1.9
- sinks: float32 [16], P('tp'), may hold values from 3 to 8
Outputs:
- result: bfloat16 [2, 32768, 2048], P('dp', ('sp', 'tp'))
The draws below stay inside these ranges and needn't reach their ends.
All inputs are finite; a program needn't handle non-finite values.
Results may differ from the reference program's by a relative error of at most 0.013.
Values may be sent and summed in bfloat16 or wider, within the bound.
No kernel may reach another device: no remote copies, remote signals or barrier semaphores. Data moves between devices by JAX's collectives and lax.ppermute only.
A program may use at most 128 MiB of HBM per device.

```python
import jax
import jax.numpy as jnp
from jax import lax

D = 2048
HEADS = 16
KV_HEADS = 4
HEAD_DIM = 128
WINDOW = 128
GRID_W = 64
CTX = 768
SEQ = 32768
BATCH = 2
N_TP = 4


def block_levels(own_key, shape, shards, least, high):
    level = 1.0
    for axis_at, shards_of in shards:
        heights = jax.random.uniform(jax.random.fold_in(jax.random.fold_in(own_key, 6), axis_at), (shards_of,), jnp.float32, least / len(shards), high / len(shards))
        level = level * jnp.repeat(jnp.exp(heights), shape[axis_at] // shards_of).reshape((-1,) + (1,) * (len(shape) - 1 - axis_at))
    return level


def gaussian(stream_key, extent, deviation, bound, split=(), held_as=jnp.bfloat16):
    values = jax.random.normal(stream_key, extent, jnp.float32) * deviation
    if len(split) > 0:
        values = block_levels(stream_key, extent, split, -0.22, 0.18) * values
    return jnp.clip(values, min=-bound, max=bound).astype(held_as)


def setup_inputs(seed: int = 0) -> dict:
    splits = jax.random.split(jax.random.key(seed), 16)
    latent = gaussian(splits[0], (BATCH, SEQ, D), 0.5, 4.0, ((0, 2), (1, 32)))
    context = gaussian(splits[1], (BATCH, CTX, D), 1.0, 6.0, ((0, 2), (1, 32)))
    cond = gaussian(splits[2], (BATCH, D), 1.0, 6.0, ((0, 2),), jnp.float32)
    ctx_cond = gaussian(splits[3], (D,), 1.0, 6.0, (), jnp.float32)
    norm_gain = jnp.clip(1.0 + 0.18 * jax.random.normal(splits[4], (D,), jnp.float32), 0.1, 1.9)
    mod_shift = gaussian(splits[5], (D, D), D ** -0.5, 0.125, ((0, 32), (1, 4)))
    mod_scale = gaussian(splits[6], (D, D), D ** -0.5, 0.125, ((0, 32), (1, 4)))
    mod_gate = gaussian(splits[7], (D, D), D ** -0.5, 0.125, ((0, 32), (1, 4)))
    w_query = gaussian(splits[8], (D, HEADS * HEAD_DIM), D ** -0.5, 0.125, ((1, 4),))
    w_key = gaussian(splits[9], (D, KV_HEADS * HEAD_DIM), D ** -0.5, 0.125, ((1, 4),))
    w_value = gaussian(splits[10], (D, KV_HEADS * HEAD_DIM), D ** -0.5, 0.125, ((1, 4),))
    w_out = gaussian(splits[11], (HEADS * HEAD_DIM, D), (max(HEADS * HEAD_DIM // 256, 1)) ** -0.5, 2.0, ((0, 4),))
    q_gain = jnp.clip(1.0 + 0.18 * jax.random.normal(splits[12], (HEAD_DIM,), jnp.float32), 0.1, 1.9)
    k_gain = jnp.clip(1.0 + 0.18 * jax.random.normal(splits[13], (HEAD_DIM,), jnp.float32), 0.1, 1.9)
    sinks = jnp.clip(3.0 + 5.0 * jax.random.uniform(splits[14], (HEADS,), jnp.float32) ** block_levels(splits[14], (HEADS,), ((0, 4),), -0.2, 0.2), 3.0, 8.0)
    return dict(latent=latent, context=context, cond=cond, ctx_cond=ctx_cond, norm_gain=norm_gain, mod_shift=mod_shift, mod_scale=mod_scale, mod_gate=mod_gate, w_query=w_query, w_key=w_key, w_value=w_value, w_out=w_out, q_gain=q_gain, k_gain=k_gain, sinks=sinks)


NORM_EPSILON = 1e-06
ROPE_BASE = 10000.0

def head_norm(vectors, gain_row):
    return vectors * lax.rsqrt(lax.optimization_barrier(jnp.mean(vectors * vectors, axis=-1, keepdims=True)) + NORM_EPSILON) * gain_row.astype(jnp.float32)

def modulated(rows_in, gain_row, shift_row, scale_row):
    values = rows_in.astype(jnp.float32)
    normed = values * lax.rsqrt(lax.optimization_barrier(jnp.mean(values * values, axis=-1, keepdims=True)) + NORM_EPSILON) * gain_row.astype(jnp.float32)
    return (normed * (1.0 + scale_row) + shift_row).astype(jnp.bfloat16)

def rotate_half(halves, coords):
    quarter = halves.shape[-1] // 2
    frequency = ROPE_BASE ** (-jnp.arange(quarter, dtype=jnp.float32) / quarter)
    angles = coords.astype(jnp.float32)[:, None] * frequency
    cosine_part = jnp.cos(angles)[:, None, :]
    sine_part = jnp.sin(angles)[:, None, :]
    first_part = halves[..., :quarter]
    second_part = halves[..., quarter:]
    return jnp.concatenate([first_part * cosine_part - second_part * sine_part, second_part * cosine_part + first_part * sine_part], axis=-1)

def rotate(vectors, positions):
    half_dim = vectors.shape[-1] // 2
    return jnp.concatenate([rotate_half(vectors[..., :half_dim], positions // GRID_W), rotate_half(vectors[..., half_dim:], positions % GRID_W)], axis=-1)

def window_attention(lat_queries, lat_keys, lat_values, ctx_keys, ctx_values, sinks):
    seq_len = lat_queries.shape[0]
    group_size = HEADS // KV_HEADS
    score_scale = HEAD_DIM ** (-0.5)
    block_count = seq_len // WINDOW
    query_blocks = lat_queries.reshape(block_count, WINDOW, KV_HEADS, group_size, HEAD_DIM)
    padded_keys = jnp.pad(lat_keys, ((WINDOW, WINDOW), (0, 0), (0, 0)))
    padded_values = jnp.pad(lat_values, ((WINDOW, WINDOW), (0, 0), (0, 0)))
    sink_exp = jnp.exp(sinks.astype(jnp.float32)).reshape(KV_HEADS, group_size)
    key_rows = jnp.arange(3 * WINDOW, dtype=jnp.int32)
    query_rows = jnp.arange(WINDOW, dtype=jnp.int32)
    offset_rows = key_rows[None, :] - query_rows[:, None]
    in_band = (offset_rows >= 0) & (offset_rows <= 2 * WINDOW)
    ctx_key_f = ctx_keys.astype(jnp.float32)
    ctx_value_f = ctx_values.astype(jnp.float32)

    def one_block(inputs):
        block_queries, block_index = inputs
        first_row = (block_index * WINDOW).astype(jnp.int32)
        block_keys = lax.dynamic_slice_in_dim(padded_keys, first_row, 3 * WINDOW, 0).astype(jnp.float32)
        block_values = lax.dynamic_slice_in_dim(padded_values, first_row, 3 * WINDOW, 0).astype(jnp.float32)
        key_pos = first_row - WINDOW + key_rows
        in_window = in_band & ((key_pos >= 0) & (key_pos < seq_len))[None, :]
        block_q = block_queries.astype(jnp.float32)
        scores = jnp.einsum('qhgd,khd->hgqk', block_q, block_keys) * score_scale
        weights = jnp.where(in_window, jnp.exp(scores), 0.0)
        ctx_weights = jnp.exp(jnp.einsum('qhgd,chd->hgqc', block_q, ctx_key_f) * score_scale)
        denominator = lax.optimization_barrier(jnp.sum(weights, axis=-1)) + lax.optimization_barrier(jnp.sum(ctx_weights, axis=-1)) + sink_exp[:, :, None]
        local_probs = (weights / denominator[..., None]).astype(jnp.bfloat16).astype(jnp.float32)
        ctx_probs = (ctx_weights / denominator[..., None]).astype(jnp.bfloat16).astype(jnp.float32)
        block_out = jnp.einsum('hgqk,khd->qhgd', local_probs, block_values) + jnp.einsum('hgqc,chd->qhgd', ctx_probs, ctx_value_f)
        return block_out.astype(jnp.bfloat16).reshape(WINDOW, HEADS * HEAD_DIM)
    attended = lax.map(one_block, (query_blocks, jnp.arange(block_count, dtype=jnp.int32)))
    return attended.reshape(seq_len, HEADS * HEAD_DIM)

def reference(latent, context, cond, ctx_cond, norm_gain, mod_shift, mod_scale, mod_gate, w_query, w_key, w_value, w_out, q_gain, k_gain, sinks):
    seq_len = latent.shape[1]
    ctx_len = context.shape[1]
    group_cols = HEADS * HEAD_DIM // N_TP
    outputs = []
    for sample in range(latent.shape[0]):
        active = jax.nn.silu(jnp.stack([cond[sample].astype(jnp.float32), ctx_cond.astype(jnp.float32)])).astype(jnp.bfloat16)
        shifts = jnp.dot(active, mod_shift, preferred_element_type=jnp.float32)
        scales = jnp.dot(active, mod_scale, preferred_element_type=jnp.float32)
        gate_rows = jnp.dot(active[0:1], mod_gate, preferred_element_type=jnp.float32)
        lat_in = modulated(latent[sample], norm_gain, shifts[0], scales[0])
        ctx_in = modulated(context[sample], norm_gain, shifts[1], scales[1])
        positions = jnp.arange(seq_len, dtype=jnp.int32)
        lat_queries = rotate(head_norm(jnp.dot(lat_in, w_query, preferred_element_type=jnp.float32).reshape(seq_len, HEADS, HEAD_DIM), q_gain), positions).astype(jnp.bfloat16)
        lat_keys = rotate(head_norm(jnp.dot(lat_in, w_key, preferred_element_type=jnp.float32).reshape(seq_len, KV_HEADS, HEAD_DIM), k_gain), positions).astype(jnp.bfloat16)
        lat_values = jnp.dot(lat_in, w_value, preferred_element_type=jnp.float32).astype(jnp.bfloat16).reshape(seq_len, KV_HEADS, HEAD_DIM)
        ctx_keys = head_norm(jnp.dot(ctx_in, w_key, preferred_element_type=jnp.float32).reshape(ctx_len, KV_HEADS, HEAD_DIM), k_gain).astype(jnp.bfloat16)
        ctx_values = jnp.dot(ctx_in, w_value, preferred_element_type=jnp.float32).astype(jnp.bfloat16).reshape(ctx_len, KV_HEADS, HEAD_DIM)
        attended = window_attention(lat_queries, lat_keys, lat_values, ctx_keys, ctx_values, sinks)
        mixed_rows = jnp.zeros((seq_len, D), jnp.float32)
        for group_index in range(N_TP):
            partial_value = jnp.dot(attended[:, group_index * group_cols:(group_index + 1) * group_cols], w_out[group_index * group_cols:(group_index + 1) * group_cols], preferred_element_type=jnp.float32).astype(jnp.bfloat16)
            mixed_rows = mixed_rows + lax.optimization_barrier(partial_value).astype(jnp.float32)
        result = latent[sample].astype(jnp.float32) + gate_rows[0] * mixed_rows
        outputs.append(result.astype(jnp.bfloat16))
    return jnp.stack(outputs)
```

```python
import math

import jax
import jax.numpy as jnp
from jax import lax
from jax.experimental import pallas as pl
from jax.experimental.pallas import tpu as pltpu
from jax.sharding import Mesh, PartitionSpec as P

HEAD_DIM = 128
WINDOW = 128
GRID_W = 64
NORM_EPSILON = 1e-06
ROPE_BASE = 10000.0
D = 2048
ROWS = 24
NZ, NY, NX = 8, 4, 4
SP = ("z", "y")

F32 = jnp.float32
BF16 = jnp.bfloat16
QUERY_SCALE = HEAD_DIM ** (-0.5) * math.log2(math.e)


def sp_index():
    return lax.axis_index("z") * NY + lax.axis_index("y")


def params(vmem_mib=48):
    return pltpu.CompilerParams(vmem_limit_bytes=vmem_mib * 1024 * 1024)


def cost(flops, nbytes, trans=0):
    return pl.CostEstimate(flops=flops, bytes_accessed=nbytes, transcendentals=trans)


def partial_kernel(cond_ref, ctx_ref, shift_ref, scale_ref, gate_ref, out_ref):
    sp = sp_index()
    start = pl.multiple_of((sp // 2) * 128, 128)
    row = lax.broadcasted_iota(jnp.int32, (8, 128), 0)
    lane = lax.broadcasted_iota(jnp.int32, (8, 128), 1)
    rows = jnp.where(
        row == 0,
        cond_ref[:, pl.ds(start, 128)],
        jnp.where(row == 1, ctx_ref[:, pl.ds(start, 128)], 0.0),
    )
    active = rows / (1.0 + jnp.exp(-rows))
    active = jnp.where((lane // 64) == (sp % 2), active, 0.0).astype(BF16)

    def times(ref):
        matrix = ref[...]
        return jnp.dot(
            active, jnp.concatenate([matrix, matrix], axis=0), preferred_element_type=F32
        )

    shifts, scales, gates = times(shift_ref), times(scale_ref), times(gate_ref)
    pieces = []
    for values, at in ((shifts, 0), (scales, 0), (shifts, 1), (scales, 1), (gates, 0)):
        for i in range(4):
            pieces.append(values[at : at + 1, i * 128 : (i + 1) * 128])
    pieces.append(jnp.zeros((4, 128), F32))
    stacked = jnp.concatenate(pieces, axis=0).astype(BF16)
    out_ref[...] = jnp.broadcast_to(stacked[None], out_ref.shape)


def resum_kernel(in_ref, out_ref):
    total = jnp.sum(in_ref[...].astype(F32), axis=0).astype(BF16)
    out_ref[...] = jnp.broadcast_to(total[None], out_ref.shape)


def vectors_of(mod_ref, wanted):
    found = []
    for v in wanted:
        pieces = []
        for t in range(NX):
            rows = None
            for y in range(NY):
                part = mod_ref[y * NX + t].astype(F32)
                rows = part if rows is None else rows + part
            for i in range(4):
                pieces.append(rows[v * 4 + i : v * 4 + i + 1, :])
        found.append(jnp.concatenate(pieces, axis=1))
    return found


def modulated(rows, factor, shift):
    values = rows.astype(F32)
    inverse = lax.rsqrt(jnp.mean(values * values, axis=-1, keepdims=True) + NORM_EPSILON)
    return (values * inverse * factor + shift).astype(BF16)


def head_norm(v, gain):
    return v * lax.rsqrt(jnp.mean(v * v, axis=-1, keepdims=True) + NORM_EPSILON) * gain


def rotated(v, cosine, sine):
    lane = lax.broadcasted_iota(jnp.int32, v.shape, 1)
    odd = ((lane // 32) % 2) == 1
    swapped = jnp.where(odd, pltpu.roll(v, 32, 1), pltpu.roll(v, 96, 1))
    return v * cosine + swapped * sine


def edge_kernel(
    mod_ref, ctx_ref, first_ref, last_ref, wk_ref, wv_ref, gain_ref, kgain_ref,
    cosf_ref, sinf_ref, cosl_ref, sinl_ref, ctxkv_ref, firstkv_ref, lastkv_ref,
):
    shift_lat, scale_lat, shift_ctx, scale_ctx = vectors_of(mod_ref, (0, 1, 2, 3))
    gain = gain_ref[...]
    lat_factor = gain * (1.0 + scale_lat)
    ctx_factor = gain * (1.0 + scale_ctx)
    kgain = kgain_ref[...]
    wk, wv = wk_ref[...], wv_ref[...]
    rows = jnp.concatenate(
        [
            modulated(ctx_ref[...], ctx_factor, shift_ctx),
            modulated(first_ref[...], lat_factor, shift_lat),
            modulated(last_ref[...], lat_factor, shift_lat),
        ],
        axis=0,
    )
    keys = head_norm(jnp.dot(rows, wk, preferred_element_type=F32), kgain)
    values = jnp.dot(rows, wv, preferred_element_type=F32).astype(BF16)
    n = ctx_ref.shape[0]
    for y in range(NY):
        ctxkv_ref[y, :, :HEAD_DIM] = keys[:n].astype(BF16)
        ctxkv_ref[y, :, HEAD_DIM:] = values[:n]
    firstkv_ref[:, :HEAD_DIM] = rotated(keys[n : n + WINDOW], cosf_ref[...], sinf_ref[...]).astype(BF16)
    firstkv_ref[:, HEAD_DIM:] = values[n : n + WINDOW]
    lastkv_ref[:, :HEAD_DIM] = rotated(keys[n + WINDOW :], cosl_ref[...], sinl_ref[...]).astype(BF16)
    lastkv_ref[:, HEAD_DIM:] = values[n + WINDOW :]


def qkv_kernel(
    mod_ref, lat_ref, wq_ref, wk_ref, wv_ref, gain_ref, qgain_ref, kgain_ref,
    cos_ref, sin_ref, q_ref, k_ref, v_ref,
):
    shift_lat, scale_lat = vectors_of(mod_ref, (0, 1))
    rows = modulated(lat_ref[...], gain_ref[...] * (1.0 + scale_lat), shift_lat)
    cosine, sine = cos_ref[...], sin_ref[...]
    qgain = qgain_ref[...] * QUERY_SCALE
    queries = jnp.dot(rows, wq_ref[...], preferred_element_type=F32)
    for h in range(4):
        at = slice(h * HEAD_DIM, (h + 1) * HEAD_DIM)
        q_ref[:, at] = rotated(head_norm(queries[:, at], qgain), cosine, sine).astype(BF16)
    keys = jnp.dot(rows, wk_ref[...], preferred_element_type=F32)
    k_ref[...] = rotated(head_norm(keys, kgain_ref[...]), cosine, sine).astype(BF16)
    v_ref[...] = jnp.dot(rows, wv_ref[...], preferred_element_type=F32).astype(BF16)


def contract_last(a, b):
    return lax.dot_general(a, b, (((1,), (1,)), ((), ())), preferred_element_type=F32)


def attend_kernel(at_ref, q_ref, k_ref, v_ref, before_ref, after_ref, ctx_ref, sink_ref, out_ref):
    quarter, sp = at_ref[0], at_ref[1]
    head = HEAD_DIM
    first = pl.multiple_of(quarter * 256, 256)
    low = pl.multiple_of(jnp.maximum(first - WINDOW, 0), WINDOW)
    high = pl.multiple_of(jnp.minimum(first + 256, 1024 - WINDOW), WINDOW)
    is_first, is_last = quarter == 0, quarter == 3

    def window(ref, edge):
        before, after = before_ref[:, edge], after_ref[:, edge]
        return jnp.concatenate(
            [
                jnp.where(is_first, before, ref[pl.ds(low, WINDOW), :]),
                ref[pl.ds(first, 256), :],
                jnp.where(is_last, after, ref[pl.ds(high, WINDOW), :]),
            ],
            axis=0,
        )

    keys = window(k_ref, slice(0, head))
    values = window(v_ref, slice(head, 2 * head))
    ctx_keys = ctx_ref[:, :head]
    ctx_values = ctx_ref[:, head:]
    no_before = is_first & (sp == 0)
    no_after = is_last & (sp == NZ * NY - 1)
    query_at = lax.broadcasted_iota(jnp.int32, (4 * WINDOW, WINDOW), 0) % WINDOW
    key_at = lax.broadcasted_iota(jnp.int32, (4 * WINDOW, WINDOW), 1)
    in_before, in_after = key_at >= query_at, key_at <= query_at
    sink = jnp.concatenate(
        [jnp.exp(jnp.full((WINDOW, 1), sink_ref[0, h], F32)) for h in range(4)], axis=0
    )
    for block in range(2):
        rows = slice(block * WINDOW, (block + 1) * WINDOW)
        queries = jnp.concatenate(
            [q_ref[rows, h * head : (h + 1) * head] for h in range(4)], axis=0
        )
        near = slice(block * WINDOW, (block + 3) * WINDOW)
        local = jnp.exp2(contract_last(queries, keys[near]))
        allow_before, allow_after = in_before, in_after
        if block == 0:
            allow_before = in_before & jnp.logical_not(no_before)
        else:
            allow_after = in_after & jnp.logical_not(no_after)
        local = jnp.concatenate(
            [
                jnp.where(allow_before, local[:, :WINDOW], 0.0),
                local[:, WINDOW : 2 * WINDOW],
                jnp.where(allow_after, local[:, 2 * WINDOW :], 0.0),
            ],
            axis=1,
        )
        far = jnp.exp2(contract_last(queries, ctx_keys))
        total = (
            jnp.sum(local, axis=-1, keepdims=True) + jnp.sum(far, axis=-1, keepdims=True) + sink
        )
        mixed = jnp.dot(local.astype(BF16), values[near], preferred_element_type=F32) + jnp.dot(
            far.astype(BF16), ctx_values, preferred_element_type=F32
        )
        mixed = (mixed * (1.0 / total)).astype(BF16)
        for h in range(4):
            out_ref[rows, h * head : (h + 1) * head] = mixed[h * WINDOW : (h + 1) * WINDOW]


def out_kernel(
    at_ref, mod_ref, a0_ref, a1_ref, a2_ref, a3_ref, w0_ref,
    m1_ref, m2_ref, m3_ref, o1_ref, o2_ref, o3_ref, lat_ref, out_ref, gate_ref,
):
    part, sub = pl.program_id(0), pl.program_id(1)

    @pl.when((part == 0) & (sub == 0))
    def _():
        gate_ref[...] = jnp.broadcast_to(vectors_of(mod_ref, (4,))[0], gate_ref.shape)

    column = jnp.where(part == 0, at_ref[1], 1 - at_ref[1]) * 2 + sub
    own = jnp.dot(a0_ref[...], w0_ref[...], preferred_element_type=F32)
    gate = gate_ref[0:1, pl.ds(pl.multiple_of(column * 512, 512), 512)]

    def finish(w1, w2, w3):
        mixed = own
        for a, w in ((a1_ref, w1), (a2_ref, w2), (a3_ref, w3)):
            mixed = mixed + jnp.dot(a[...], w[...], preferred_element_type=F32)
        out_ref[...] = (lat_ref[...].astype(F32) + gate * mixed).astype(BF16)

    @pl.when(part == 0)
    def _():
        finish(m1_ref, m2_ref, m3_ref)

    @pl.when(part == 1)
    def _():
        finish(o1_ref, o2_ref, o3_ref)


def copies(array, axis):
    peers = lax.axis_size(axis)
    return lax.all_to_all(
        jnp.broadcast_to(array[None], (peers, *array.shape)), axis, 0, 0, tiled=True
    )


def shifted(array, axis, by):
    peers = lax.axis_size(axis)
    return lax.ppermute(array, axis, [(i, (i + by) % peers) for i in range(peers)])


def full(shape):
    return pl.BlockSpec(shape, lambda *_: (0,) * len(shape))


def per_device(
    latent, context, cond, ctx_cond, norm_gain, mod_shift, mod_scale, mod_gate,
    w_query, w_key, w_value, w_out, q_gain, k_gain, sinks,
):
    lat = latent[0]
    tok = lat.shape[0]
    sp = sp_index()
    tp = lax.axis_index("tp")
    dp = lax.axis_index("dp")

    partial = pl.pallas_call(
        partial_kernel,
        out_shape=jax.ShapeDtypeStruct((NZ, ROWS, 128), BF16),
        cost_estimate=cost(3 * 2 * 128 * 512 * 8, 3 * 64 * 512 * 2),
        name="partial",
    )(cond, ctx_cond[None], mod_shift, mod_scale, mod_gate)
    over_z = lax.all_to_all(partial, "z", 0, 0, tiled=True)
    resummed = pl.pallas_call(
        resum_kernel,
        out_shape=jax.ShapeDtypeStruct((NY * NX, ROWS, 128), BF16),
        name="resum",
    )(over_z)
    mod = lax.all_to_all(resummed, ("y", "tp"), 0, 0, tiled=True)

    ctx_rows = copies(context[0], "z").reshape(-1, D)
    n_ctx = ctx_rows.shape[0]

    half = lax.dynamic_slice_in_dim(w_out, dp * (D // 2), D // 2, 1)
    mine = [shifted(half, "tp", s) for s in (1, 2, 3)]
    other = [shifted(w, "dp", 1) for w in mine]

    positions = sp * tok + jnp.arange(tok, dtype=jnp.int32)
    quarter = HEAD_DIM // 4
    frequency = ROPE_BASE ** (-jnp.arange(quarter, dtype=F32) / quarter)
    by_row = (positions // GRID_W).astype(F32)[:, None] * frequency
    by_col = (positions % GRID_W).astype(F32)[:, None] * frequency
    angles = jnp.concatenate([by_row, by_row, by_col, by_col], axis=1)
    signs = jnp.where((jnp.arange(HEAD_DIM) // quarter) % 2 == 0, -1.0, 1.0).astype(F32)
    cosine, sine = jnp.cos(angles), jnp.sin(angles) * signs

    gain, qgain, kgain = norm_gain[None], q_gain[None], k_gain[None]
    edge_last = tok // WINDOW - 1
    kv_piece = jax.ShapeDtypeStruct((WINDOW, 2 * HEAD_DIM), BF16)
    table_first = pl.BlockSpec((WINDOW, HEAD_DIM), lambda i: (0, 0))
    table_last = pl.BlockSpec((WINDOW, HEAD_DIM), lambda i: (edge_last, 0))
    ctx_kv, first_kv, last_kv = pl.pallas_call(
        edge_kernel,
        grid=(1,),
        in_specs=[
            full((NY * NX, ROWS, 128)), full((n_ctx, D)),
            pl.BlockSpec((WINDOW, D), lambda i: (0, 0)),
            pl.BlockSpec((WINDOW, D), lambda i: (edge_last, 0)),
            full((D, HEAD_DIM)), full((D, HEAD_DIM)), full((1, D)), full((1, HEAD_DIM)),
            table_first, table_first, table_last, table_last,
        ],
        out_specs=[
            full((NY, n_ctx, 2 * HEAD_DIM)), full((WINDOW, 2 * HEAD_DIM)),
            full((WINDOW, 2 * HEAD_DIM)),
        ],
        out_shape=[
            jax.ShapeDtypeStruct((NY, n_ctx, 2 * HEAD_DIM), BF16), kv_piece, kv_piece,
        ],
        compiler_params=params(),
        cost_estimate=cost(2 * (n_ctx + 256) * D * 256, (n_ctx + 256) * D * 2 + D * 512),
        name="edge",
    )(mod, ctx_rows, lat, lat, w_key, w_value, gain, kgain, cosine, sine, cosine, sine)
    ctx_all = lax.all_to_all(ctx_kv, "y", 0, 0, tiled=True).reshape(-1, 2 * HEAD_DIM)
    peers = NZ * NY
    up = [(i, i + 1) for i in range(peers - 1)]
    before = lax.ppermute(last_kv, SP, up)
    after = lax.ppermute(first_kv, SP, [(j, i) for i, j in up])

    block = 256
    queries, keys, values = pl.pallas_call(
        qkv_kernel,
        grid=(tok // block,),
        in_specs=[
            full((NY * NX, ROWS, 128)),
            pl.BlockSpec((block, D), lambda i: (i, 0)),
            full((D, 4 * HEAD_DIM)), full((D, HEAD_DIM)), full((D, HEAD_DIM)),
            full((1, D)), full((1, HEAD_DIM)), full((1, HEAD_DIM)),
            pl.BlockSpec((block, HEAD_DIM), lambda i: (i, 0)),
            pl.BlockSpec((block, HEAD_DIM), lambda i: (i, 0)),
        ],
        out_specs=[
            pl.BlockSpec((block, 4 * HEAD_DIM), lambda i: (i, 0)),
            pl.BlockSpec((block, HEAD_DIM), lambda i: (i, 0)),
            pl.BlockSpec((block, HEAD_DIM), lambda i: (i, 0)),
        ],
        out_shape=[
            jax.ShapeDtypeStruct((tok, 4 * HEAD_DIM), BF16),
            jax.ShapeDtypeStruct((tok, HEAD_DIM), BF16),
            jax.ShapeDtypeStruct((tok, HEAD_DIM), BF16),
        ],
        compiler_params=params(),
        cost_estimate=cost(2 * tok * D * 768, tok * D * 2 + D * 768 * 2),
        name="qkv",
    )(mod, lat, w_query, w_key, w_value, gain, qgain, kgain, cosine, sine)

    sub = tok // NX
    pieces = []
    for s in (2, 1, 3, 0):
        to = (tp + s) % NX
        piece = pl.pallas_call(
            attend_kernel,
            grid_spec=pltpu.PrefetchScalarGridSpec(
                num_scalar_prefetch=1,
                grid=(1,),
                in_specs=[
                    pl.BlockSpec((sub, 4 * HEAD_DIM), lambda i, at: (at[0], 0)),
                    full((tok, HEAD_DIM)), full((tok, HEAD_DIM)),
                    full((WINDOW, 2 * HEAD_DIM)), full((WINDOW, 2 * HEAD_DIM)),
                    full((NY * n_ctx, 2 * HEAD_DIM)),
                    pl.BlockSpec(memory_space=pltpu.SMEM),
                ],
                out_specs=full((sub, 4 * HEAD_DIM)),
            ),
            out_shape=jax.ShapeDtypeStruct((sub, 4 * HEAD_DIM), BF16),
            compiler_params=params(),
            cost_estimate=cost(4 * 4 * sub * 1152 * HEAD_DIM, 2 << 20, 4 * sub * 1152),
            name=f"attend{s}",
        )(
            jnp.stack([to, sp]).astype(jnp.int32), queries, keys, values,
            before, after, ctx_all, sinks[None],
        )
        pieces.append((s, piece if s == 0 else shifted(piece, "tp", s)))
    arrived = dict(pieces)

    col = 512
    wide = pl.BlockSpec((sub, 4 * HEAD_DIM), lambda p, j, at: (0, 0))
    from_mine = pl.BlockSpec((4 * HEAD_DIM, col), lambda p, j, at: (0, jnp.where(p == 0, j, 1)))
    from_other = pl.BlockSpec((4 * HEAD_DIM, col), lambda p, j, at: (0, jnp.where(p == 0, 0, j)))

    def column(p, j, at):
        return jnp.where(p == 0, at[1], 1 - at[1]) * 2 + j

    result = pl.pallas_call(
        out_kernel,
        grid_spec=pltpu.PrefetchScalarGridSpec(
            num_scalar_prefetch=1,
            grid=(2, 2),
            in_specs=[
                full((NY * NX, ROWS, 128)), wide, wide, wide, wide,
                pl.BlockSpec((4 * HEAD_DIM, col), lambda p, j, at: (0, column(p, j, at))),
                from_mine, from_mine, from_mine, from_other, from_other, from_other,
                pl.BlockSpec((sub, col), lambda p, j, at: (at[0], column(p, j, at))),
            ],
            out_specs=pl.BlockSpec((sub, col), lambda p, j, at: (0, column(p, j, at))),
            scratch_shapes=[pltpu.VMEM((8, D), F32)],
        ),
        out_shape=jax.ShapeDtypeStruct((sub, D), BF16),
        compiler_params=params(),
        cost_estimate=cost(2 * sub * D * D, D * D * 2),
        name="project",
    )(
        jnp.stack([tp, dp]).astype(jnp.int32), mod, arrived[0], arrived[1], arrived[2],
        arrived[3], w_out, *mine, *other, lat,
    )
    return result[None]


def solution(mesh):
    grid = Mesh(mesh.devices.reshape(NZ, NY, NX, 2), ("z", "y", "tp", "dp"))
    in_specs = (
        P("dp", SP, None),
        P("dp", SP, None),
        P("dp", None),
        P(),
        P(),
        P(SP, "tp"),
        P(SP, "tp"),
        P(SP, "tp"),
        P(None, "tp"),
        P(None, "tp"),
        P(None, "tp"),
        P("tp", None),
        P(),
        P(),
        P("tp"),
    )
    out_specs = P("dp", ("z", "y", "tp"), None)
    return jax.shard_map(
        per_device, mesh=grid, in_specs=in_specs, out_specs=out_specs, check_vma=False
    )
```

```python
import math

import jax
import jax.numpy as jnp
from jax import lax
from jax.experimental import pallas as pl
from jax.experimental.pallas import tpu as pltpu
from jax.sharding import Mesh, PartitionSpec as P


HEAD_DIM = 128
WINDOW = 128
GRID_W = 64
NORM_EPSILON = 1e-06
ROPE_BASE = 10000.0
D = 2048
VECS = 20
NZ, NY, NX = 8, 4, 4
SP = ("z", "y")

F32 = jnp.float32
BF16 = jnp.bfloat16
QUERY_SCALE = HEAD_DIM ** (-0.5) * math.log2(math.e)


def sp_index():
    return lax.axis_index("z") * NY + lax.axis_index("y")


def params(vmem_mib):
    return pltpu.CompilerParams(vmem_limit_bytes=vmem_mib * 1024 * 1024)


def cost(flops, nbytes, trans=0):
    return pl.CostEstimate(flops=flops, bytes_accessed=nbytes, transcendentals=trans)


def partial_kernel(cond_in, ctx_in, shift_in, scale_in, gate_in, out_ref,
                   cond_ref, ctx_ref, shift_ref, scale_ref, gate_ref, sems):
    moves = [
        pltpu.make_async_copy(source, to, sems.at[i])
        for i, (source, to) in enumerate(
            (
                (cond_in, cond_ref), (ctx_in, ctx_ref), (shift_in, shift_ref),
                (scale_in, scale_ref), (gate_in, gate_ref),
            )
        )
    ]
    for move in moves:
        move.start()
    for move in moves:
        move.wait()
    sp = sp_index()
    start = pl.multiple_of((sp // 2) * 128, 128)
    row = lax.broadcasted_iota(jnp.int32, (8, 128), 0)
    lane = lax.broadcasted_iota(jnp.int32, (8, 128), 1)
    rows = jnp.where(
        row == 0,
        cond_ref[:, pl.ds(start, 128)],
        jnp.where(row == 1, ctx_ref[:, pl.ds(start, 128)], 0.0),
    )
    active = rows / (1.0 + jnp.exp(-rows))
    active = jnp.where((lane // 64) == (sp % 2), active, 0.0).astype(BF16)

    def times(ref):
        matrix = ref[...]
        return jnp.dot(
            active, jnp.concatenate([matrix, matrix], axis=0), preferred_element_type=F32
        )

    shifts, scales, gates = times(shift_ref), times(scale_ref), times(gate_ref)
    pieces = []
    for values, at in ((shifts, 0), (scales, 0), (shifts, 1), (scales, 1), (gates, 0)):
        for i in range(4):
            pieces.append(values[at : at + 1, i * 128 : (i + 1) * 128])
    pieces.append(jnp.zeros((4, 128), F32))
    stacked = jnp.concatenate(pieces, axis=0).astype(BF16)
    out_ref[...] = jnp.broadcast_to(stacked[None], out_ref.shape)


def resum_kernel(in_ref, out_ref):
    pieces = []
    for t in range(NX):
        rows = None
        for y in range(NY):
            part = in_ref[y * NX + t].astype(F32)
            rows = part if rows is None else rows + part
        pieces.append(rows[:VECS])
    total = jnp.concatenate(pieces, axis=0).astype(BF16)
    out_ref[...] = jnp.broadcast_to(total[None], out_ref.shape)


def vectors_of(mod_ref):
    rows = None
    for z in range(NZ):
        part = mod_ref[z].astype(F32)
        rows = part if rows is None else rows + part
    found = []
    for v in range(5):
        pieces = []
        for t in range(NX):
            for i in range(4):
                at = t * VECS + v * 4 + i
                pieces.append(rows[at : at + 1, :])
        found.append(jnp.concatenate(pieces, axis=1))
    return found


def normed(values):
    values = values.astype(F32)
    return values * lax.rsqrt(jnp.mean(values * values, axis=-1, keepdims=True) + NORM_EPSILON)


def head_norm(v, gain):
    return v * lax.rsqrt(jnp.mean(v * v, axis=-1, keepdims=True) + NORM_EPSILON) * gain


def rotated(v, cosine, sine):
    lane = lax.broadcasted_iota(jnp.int32, v.shape, 1)
    odd = ((lane // 32) % 2) == 1
    swapped = jnp.where(odd, pltpu.roll(v, 32, 1), pltpu.roll(v, 96, 1))
    return v * cosine + swapped * sine


def prenorm_kernel(lat_ref, out_ref):
    step = 64

    def body(i, carry):
        at = pl.ds(pl.multiple_of(i * step, step), step)
        out_ref[at, :] = normed(lat_ref[at, :]).astype(BF16)
        return carry

    lax.fori_loop(0, lat_ref.shape[0] // step, body, 0)


def context_kernel(mod_ref, ctx_ref, wk_ref, wv_ref, gain_ref, kgain_ref, kv_ref, vec_ref):
    shift_lat, scale_lat, shift_ctx, scale_ctx, gate = vectors_of(mod_ref)
    gain = gain_ref[...]
    vec_ref[0:1, :] = gain * (1.0 + scale_lat)
    vec_ref[1:2, :] = shift_lat
    vec_ref[2:3, :] = gate
    rows = (normed(ctx_ref[...]) * (gain * (1.0 + scale_ctx)) + shift_ctx).astype(BF16)
    keys = head_norm(jnp.dot(rows, wk_ref[...], preferred_element_type=F32), kgain_ref[...])
    values = jnp.dot(rows, wv_ref[...], preferred_element_type=F32)
    both = jnp.concatenate([keys, values], axis=1).astype(BF16)
    kv_ref[...] = jnp.broadcast_to(both[None], kv_ref.shape)


def qkv_kernel(
    lat_in, before_in, after_in, wq_in, wk_in, wv_in,
    vec_ref, qgain_ref, kgain_ref, rcos_ref, rsin_ref, ccos_ref, csin_ref,
    q_ref, near_ref, sum_ref, lat_ref, halo_ref, wq_ref, wk_ref, wv_ref, k_ref, v_ref, sems,
):
    step = 256
    tok = lat_in.shape[0]
    steps = tok // step
    qgain = qgain_ref[...] * QUERY_SCALE
    kgain = kgain_ref[...]

    def rows_move(i):
        at = pl.ds(pl.multiple_of(i * step, step), step)
        return pltpu.make_async_copy(lat_in.at[at, :], lat_ref.at[at, :], sems.at[i])

    others = [
        pltpu.make_async_copy(source, to, sems.at[steps + i])
        for i, (source, to) in enumerate(
            (
                (wk_in, wk_ref), (wv_in, wv_ref), (wq_in, wq_ref),
                (before_in, halo_ref.at[:WINDOW]), (after_in, halo_ref.at[WINDOW:]),
            )
        )
    ]
    others[0].start()
    others[1].start()
    rows_move(0).start()
    others[2].start()
    for i in range(1, steps):
        rows_move(i).start()
    others[3].start()
    others[4].start()

    def table(group):
        cosine = rcos_ref[pl.ds(group, 1), :] + ccos_ref[...]
        sine = rsin_ref[pl.ds(group, 1), :] + csin_ref[...]
        return cosine, sine

    def tables(first, count):
        both = [table(first + g) for g in range(count)]
        return jnp.concatenate([c for c, _ in both]), jnp.concatenate([s for _, s in both])

    def modulated(values):
        return (values * vec_ref[0:1, :] + vec_ref[1:2, :]).astype(BF16)

    others[0].wait()
    others[1].wait()

    def body(i, carry):
        @pl.when(i == 0)
        def _():
            others[2].wait()

        rows_move(i).wait()
        at = pl.ds(pl.multiple_of(i * step, step), step)
        to = pl.ds(pl.multiple_of(i * step + WINDOW, WINDOW), step)
        rows = modulated(lat_ref[at, :].astype(F32))
        cosine, sine = tables(2 + i * (step // GRID_W), step // GRID_W)
        keys = jnp.dot(rows, wk_ref[...], preferred_element_type=F32)
        queries = jnp.dot(rows, wq_ref[...], preferred_element_type=F32)
        k_ref[to, :] = rotated(head_norm(keys, kgain), cosine, sine).astype(BF16)
        v_ref[to, :] = jnp.dot(rows, wv_ref[...], preferred_element_type=F32).astype(BF16)
        for h in range(4):
            head = slice(h * HEAD_DIM, (h + 1) * HEAD_DIM)
            turned = rotated(head_norm(queries[:, head], qgain), cosine, sine).astype(BF16)
            for half in range(2):
                q_ref[i * 2 + half, h * WINDOW : (h + 1) * WINDOW, :] = turned[
                    half * WINDOW : (half + 1) * WINDOW
                ]
        return carry

    lax.fori_loop(0, steps, body, 0)
    others[3].wait()
    others[4].wait()

    def halo(i, carry):
        at = pl.ds(pl.multiple_of(i * WINDOW, WINDOW), WINDOW)
        to = pl.ds(pl.multiple_of(i * (tok + WINDOW), WINDOW), WINDOW)
        rows = modulated(normed(halo_ref[at, :]))
        cosine, sine = tables(i * ((tok + WINDOW) // GRID_W), WINDOW // GRID_W)
        keys = head_norm(jnp.dot(rows, wk_ref[...], preferred_element_type=F32), kgain)
        k_ref[to, :] = rotated(keys, cosine, sine).astype(BF16)
        v_ref[to, :] = jnp.dot(rows, wv_ref[...], preferred_element_type=F32).astype(BF16)
        return carry

    lax.fori_loop(0, 2, halo, 0)
    local_pass(q_ref, k_ref, v_ref, near_ref, sum_ref)


def contract_last(a, b):
    return lax.dot_general(a, b, (((1,), (1,)), ((), ())), preferred_element_type=F32)


def lanes_summed(values):
    parts = [values[:, i : i + 128] for i in range(0, values.shape[1], 128)]
    while len(parts) > 1:
        parts = [sum(parts[i : i + 2]) for i in range(0, len(parts), 2)]
    return parts[0]


def local_pass(q_ref, k_ref, v_ref, out_ref, sum_ref):
    sp = sp_index()
    blocks = q_ref.shape[0]
    query_at = lax.broadcasted_iota(jnp.int32, (4 * WINDOW, WINDOW), 0) % WINDOW
    key_at = lax.broadcasted_iota(jnp.int32, (4 * WINDOW, WINDOW), 1)
    in_before, in_after = key_at >= query_at, key_at <= query_at

    sum_ref[...] = jnp.zeros(sum_ref.shape, F32)

    def body(block, carry):
        near = pl.ds(pl.multiple_of(block * WINDOW, WINDOW), 3 * WINDOW)
        no_before = (block == 0) & (sp == 0)
        no_after = (block == blocks - 1) & (sp == NZ * NY - 1)
        local = jnp.exp2(contract_last(q_ref[block], k_ref[near, :]))
        local = jnp.concatenate(
            [
                jnp.where(in_before & jnp.logical_not(no_before), local[:, :WINDOW], 0.0),
                local[:, WINDOW : 2 * WINDOW],
                jnp.where(in_after & jnp.logical_not(no_after), local[:, 2 * WINDOW :], 0.0),
            ],
            axis=1,
        )
        total = jnp.sum(lanes_summed(local), axis=-1, keepdims=True)
        sum_ref[...] = jnp.where(key_at == block, total, sum_ref[...])
        out_ref[block] = jnp.dot(local.astype(BF16), v_ref[near, :], preferred_element_type=F32)
        return carry

    lax.fori_loop(0, blocks, body, 0)


def attend_kernel(by, q_ref, near_ref, sum_ref, ctx_ref, sink_ref, out_ref):
    quarter = (lax.axis_index("tp") + by) % NX
    head = HEAD_DIM
    sink = jnp.concatenate(
        [jnp.exp(jnp.full((WINDOW, 1), sink_ref[0, h], F32)) for h in range(4)], axis=0
    )

    lane = lax.broadcasted_iota(jnp.int32, sum_ref.shape, 1)

    def body(i, carry):
        block = quarter * 2 + i
        base = pl.ds(pl.multiple_of(i * WINDOW, WINDOW), WINDOW)
        far = jnp.exp2(contract_last(q_ref[block], ctx_ref[:, :head]))
        near_sum = jnp.where(lane == block, sum_ref[...], 0.0)
        total = jnp.sum(lanes_summed(far) + near_sum, axis=-1, keepdims=True) + sink
        mixed = near_ref[block] + jnp.dot(
            far.astype(BF16), ctx_ref[:, head:], preferred_element_type=F32
        )
        mixed = (mixed * (1.0 / total)).astype(BF16)
        for h in range(4):
            out_ref[base, h * head : (h + 1) * head] = mixed[h * WINDOW : (h + 1) * WINDOW]
        return carry

    lax.fori_loop(0, 2, body, 0)


def project_kernel(
    vec_ref, a0_ref, a1_ref, a2_ref, a3_ref, w0_in,
    m1_in, m2_in, m3_in, o1_in, o2_in, o3_in, lat_in, out_ref,
    w_ref, lat_ref, done_ref, sems,
):
    dp = lax.axis_index("dp")
    col = 512
    deep = 4 * HEAD_DIM
    sub = lat_ref.shape[0]
    first = pl.multiple_of(lax.axis_index("tp") * sub, sub)
    rows_move = pltpu.make_async_copy(lat_in.at[pl.ds(first, sub), :], lat_ref, sems.at[16])
    halves = (dp, 1 - dp)

    def columns(slot):
        return pl.multiple_of(halves[slot // 2] * (D // 2) + (slot % 2) * col, col)

    def moves(slot):
        later = slice((slot % 2) * col, (slot % 2 + 1) * col)
        group = (m1_in, m2_in, m3_in) if slot < 2 else (o1_in, o2_in, o3_in)
        sources = [w0_in.at[:, pl.ds(columns(slot), col)]] + [w.at[:, later] for w in group]
        return [
            pltpu.make_async_copy(
                source, w_ref.at[slot, pl.ds(s * deep, deep), :], sems.at[slot * 4 + s]
            )
            for s, source in enumerate(sources)
        ]

    for slot in range(4):
        for move in moves(slot):
            move.start()
        if slot == 0:
            rows_move.start()
    left = jnp.concatenate([a0_ref[...], a1_ref[...], a2_ref[...], a3_ref[...]], axis=1)
    rows_move.wait()
    for slot in range(4):
        for move in moves(slot):
            move.wait()
        wide = pl.ds(columns(slot), col)
        mixed = jnp.dot(left, w_ref[slot], preferred_element_type=F32)
        result = lat_ref[:, wide].astype(F32) + vec_ref[2:3, wide] * mixed
        done_ref[slot] = result.astype(BF16)
        pltpu.make_async_copy(done_ref.at[slot], out_ref.at[:, wide], sems.at[17 + slot]).start()
    for slot in range(4):
        wide = pl.ds(columns(slot), col)
        pltpu.make_async_copy(done_ref.at[slot], out_ref.at[:, wide], sems.at[17 + slot]).wait()


def shifted(array, axis, by):
    peers = lax.axis_size(axis)
    return lax.ppermute(array, axis, [(i, (i + by) % peers) for i in range(peers)])


VMEM = pl.BlockSpec(memory_space=pltpu.VMEM)
SMEM = pl.BlockSpec(memory_space=pltpu.SMEM)
HBM = pl.BlockSpec(memory_space=pltpu.HBM)


def call(kernel, outs, args, estimate, limit, scratch=(), in_specs=None, out_specs=None):
    shapes = [jax.ShapeDtypeStruct(s, t) for s, t in outs]
    single = len(shapes) == 1
    return pl.pallas_call(
        kernel,
        in_specs=in_specs or [VMEM] * len(args),
        out_specs=out_specs or (VMEM if single else [VMEM] * len(shapes)),
        out_shape=shapes[0] if single else shapes,
        scratch_shapes=list(scratch),
        compiler_params=params(limit),
        cost_estimate=estimate,
    )(*args)


def per_device(
    latent, context, cond, ctx_cond, norm_gain, mod_shift, mod_scale, mod_gate,
    w_query, w_key, w_value, w_out, q_gain, k_gain, sinks,
):
    lat = latent[0]
    tok = lat.shape[0]
    sub = tok // NX
    sp = sp_index()
    dp = lax.axis_index("dp")
    width = 4 * HEAD_DIM

    part = call(
        partial_kernel, [((NY * NX, 24, 128), BF16)],
        (cond, ctx_cond[None], mod_shift, mod_scale, mod_gate), cost(1 << 20, 1 << 18), 62,
        scratch=[
            pltpu.VMEM((1, D), F32), pltpu.VMEM((1, D), F32), pltpu.VMEM((64, 512), BF16),
            pltpu.VMEM((64, 512), BF16), pltpu.VMEM((64, 512), BF16),
            pltpu.SemaphoreType.DMA((5,)),
        ],
        in_specs=[HBM] * 5,
    )
    part = lax.all_to_all(part, ("y", "tp"), 0, 0, tiled=True)
    part = call(resum_kernel, [((NZ, NX * VECS, 128), BF16)], (part,), cost(1 << 20, 1 << 18), 4)
    mod = lax.all_to_all(part, "z", 0, 0, tiled=True)

    peers = NZ * NY
    up = [(i, i + 1) for i in range(peers - 1)]
    before = lax.ppermute(lat[tok - WINDOW :], SP, up)
    after = lax.ppermute(lat[:WINDOW], SP, [(j, i) for i, j in up])

    half = lax.dynamic_slice_in_dim(w_out, dp * (D // 2), D // 2, 1)
    mine, other = {}, {}
    for s in (1, 3, 2):
        mine[s] = shifted(half, "tp", s)
        other[s] = shifted(mine[s], "dp", 1)

    quarter = HEAD_DIM // 4
    lane = jnp.arange(HEAD_DIM)
    frequency = ROPE_BASE ** (-(lane % quarter).astype(F32) / quarter)
    sign = jnp.where((lane // quarter) % 2 == 0, -1.0, 1.0).astype(F32)
    by_row = lane < HEAD_DIM // 2
    grid_row = (sp * tok - WINDOW) // GRID_W + jnp.arange(24, dtype=jnp.int32)
    row_angle = grid_row.astype(F32)[:, None] * frequency
    col_angle = jnp.arange(GRID_W, dtype=F32)[:, None] * frequency
    row_cos = jnp.where(by_row, jnp.cos(row_angle), 0.0)
    row_sin = jnp.where(by_row, jnp.sin(row_angle) * sign, 0.0)
    col_cos = jnp.where(by_row, 0.0, jnp.cos(col_angle))
    col_sin = jnp.where(by_row, 0.0, jnp.sin(col_angle) * sign)

    block = pl.BlockSpec((256, D), lambda i: (i, 0))
    scaled = pl.pallas_call(
        prenorm_kernel,
        grid=(tok // 256,),
        in_specs=[block],
        out_specs=block,
        out_shape=jax.ShapeDtypeStruct((tok, D), BF16),
        compiler_params=params(60),
        cost_estimate=cost(tok * D * 4, tok * D * 4),
        name="prenorm",
    )(lat)
    rows = tok + 2 * WINDOW
    gain, qgain, kgain = norm_gain[None], q_gain[None], k_gain[None]
    n_ctx = context.shape[1]
    ctx_kv, vec = call(
        context_kernel,
        [((peers, n_ctx, 2 * HEAD_DIM), BF16), ((8, D), F32)],
        (mod, context[0], w_key, w_value, gain, kgain),
        cost(2 * n_ctx * D * 256, D * 512), 4,
    )
    ctx_all = lax.all_to_all(ctx_kv, SP, 0, 0, tiled=True).reshape(-1, 2 * HEAD_DIM)

    queries, near, sums = call(
        qkv_kernel,
        [
            ((tok // WINDOW, 4 * WINDOW, HEAD_DIM), BF16),
            ((tok // WINDOW, 4 * WINDOW, HEAD_DIM), F32), ((4 * WINDOW, 128), F32),
        ],
        (
            scaled, before, after, w_query, w_key, w_value, vec, qgain, kgain,
            row_cos, row_sin, col_cos, col_sin,
        ),
        cost(2 * tok * D * 768 + 16 * tok * 384 * HEAD_DIM, tok * D * 2 + D * 768 * 2), 60,
        scratch=[
            pltpu.VMEM((tok, D), BF16), pltpu.VMEM((2 * WINDOW, D), BF16),
            pltpu.VMEM((D, width), BF16), pltpu.VMEM((D, HEAD_DIM), BF16),
            pltpu.VMEM((D, HEAD_DIM), BF16), pltpu.VMEM((rows, HEAD_DIM), BF16),
            pltpu.VMEM((rows, HEAD_DIM), BF16), pltpu.SemaphoreType.DMA((tok // 256 + 5,)),
        ],
        in_specs=[HBM] * 6 + [VMEM] * 7,
    )

    arrived = {}
    for s in (2, 1, 3, 0):
        piece = call(
            lambda *refs, s=s: attend_kernel(s, *refs), [((sub, width), BF16)],
            (queries, near, sums, ctx_all, sinks[None]),
            cost(4 * 4 * sub * 768 * HEAD_DIM, 2 << 20, 4 * sub * 768), 8,
            in_specs=[VMEM] * 4 + [SMEM],
        )
        if s == 0:
            arrived[s] = piece
        else:
            arrived[s] = shifted(piece, "tp", s)

    result = call(
        project_kernel, [((sub, D), BF16)],
        (
            vec, arrived[0], arrived[1], arrived[2], arrived[3], w_out,
            mine[1], mine[2], mine[3], other[1], other[2], other[3], lat,
        ),
        cost(2 * sub * D * D, D * D * 2), 61,
        scratch=[
            pltpu.VMEM((4, D, 512), BF16), pltpu.VMEM((sub, D), BF16),
            pltpu.VMEM((4, sub, 512), BF16), pltpu.SemaphoreType.DMA((21,)),
        ],
        in_specs=[VMEM] * 5 + [HBM] * 8,
        out_specs=HBM,
    )
    return result[None]


def solution(mesh):
    grid = Mesh(mesh.devices.reshape(NZ, NY, NX, 2), ("z", "y", "tp", "dp"))
    in_specs = (
        P("dp", SP, None),
        P("dp", SP, None),
        P("dp", None),
        P(),
        P(),
        P(SP, "tp"),
        P(SP, "tp"),
        P(SP, "tp"),
        P(None, "tp"),
        P(None, "tp"),
        P(None, "tp"),
        P("tp", None),
        P(),
        P(),
        P("tp"),
    )
    out_specs = P("dp", ("z", "y", "tp"), None)

    return jax.shard_map(
        per_device, mesh=grid, in_specs=in_specs, out_specs=out_specs, check_vma=False
    )
```

```python
import math

import jax
import jax.numpy as jnp
from jax import lax
from jax.experimental import pallas as pl
from jax.experimental.pallas import tpu as pltpu
from jax.sharding import Mesh, PartitionSpec as P


HEAD_DIM = 128
WINDOW = 128
GRID_W = 64
NORM_EPSILON = 1e-06
ROPE_BASE = 10000.0
D = 2048
VECS = 20
NZ, NY, NX = 8, 4, 4
SP = ("z", "y")

F32 = jnp.float32
BF16 = jnp.bfloat16
QUERY_SCALE = HEAD_DIM ** (-0.5) * math.log2(math.e)


def sp_index():
    return lax.axis_index("z") * NY + lax.axis_index("y")


def params(vmem_mib):
    return pltpu.CompilerParams(vmem_limit_bytes=vmem_mib * 1024 * 1024)


def cost(flops, nbytes, trans=0):
    return pl.CostEstimate(flops=flops, bytes_accessed=nbytes, transcendentals=trans)


def partial_kernel(cond_in, ctx_in, shift_in, scale_in, gate_in, out_ref,
                   cond_ref, ctx_ref, shift_ref, scale_ref, gate_ref, sems):
    moves = [
        pltpu.make_async_copy(source, to, sems.at[i])
        for i, (source, to) in enumerate(
            (
                (cond_in, cond_ref), (ctx_in, ctx_ref), (shift_in, shift_ref),
                (scale_in, scale_ref), (gate_in, gate_ref),
            )
        )
    ]
    for move in moves:
        move.start()
    for move in moves:
        move.wait()
    sp = sp_index()
    start = pl.multiple_of((sp // 2) * 128, 128)
    row = lax.broadcasted_iota(jnp.int32, (8, 128), 0)
    lane = lax.broadcasted_iota(jnp.int32, (8, 128), 1)
    rows = jnp.where(
        row == 0,
        cond_ref[:, pl.ds(start, 128)],
        jnp.where(row == 1, ctx_ref[:, pl.ds(start, 128)], 0.0),
    )
    active = rows / (1.0 + jnp.exp(-rows))
    active = jnp.where((lane // 64) == (sp % 2), active, 0.0).astype(BF16)

    def times(ref):
        matrix = ref[...]
        return jnp.dot(
            active, jnp.concatenate([matrix, matrix], axis=0), preferred_element_type=F32
        )

    shifts, scales, gates = times(shift_ref), times(scale_ref), times(gate_ref)
    pieces = []
    for values, at in ((shifts, 0), (scales, 0), (shifts, 1), (scales, 1), (gates, 0)):
        for i in range(4):
            pieces.append(values[at : at + 1, i * 128 : (i + 1) * 128])
    pieces.append(jnp.zeros((4, 128), F32))
    stacked = jnp.concatenate(pieces, axis=0).astype(BF16)
    out_ref[...] = jnp.broadcast_to(stacked[None], out_ref.shape)


def resum_kernel(in_ref, out_ref):
    pieces = []
    for t in range(NX):
        rows = None
        for y in range(NY):
            part = in_ref[y * NX + t].astype(F32)
            rows = part if rows is None else rows + part
        pieces.append(rows[:VECS])
    total = jnp.concatenate(pieces, axis=0).astype(BF16)
    out_ref[...] = jnp.broadcast_to(total[None], out_ref.shape)


def vectors_of(mod_ref):
    rows = None
    for z in range(NZ):
        part = mod_ref[z].astype(F32)
        rows = part if rows is None else rows + part
    found = []
    for v in range(5):
        pieces = []
        for t in range(NX):
            for i in range(4):
                at = t * VECS + v * 4 + i
                pieces.append(rows[at : at + 1, :])
        found.append(jnp.concatenate(pieces, axis=1))
    return found


def normed(values):
    values = values.astype(F32)
    return values * lax.rsqrt(jnp.mean(values * values, axis=-1, keepdims=True) + NORM_EPSILON)


def head_norm(v, gain):
    return v * lax.rsqrt(jnp.mean(v * v, axis=-1, keepdims=True) + NORM_EPSILON) * gain


def rotated(v, cosine, sine):
    lane = lax.broadcasted_iota(jnp.int32, v.shape, 1)
    odd = ((lane // 32) % 2) == 1
    swapped = jnp.where(odd, pltpu.roll(v, 32, 1), pltpu.roll(v, 96, 1))
    return v * cosine + swapped * sine


def stage_kernel(w_in, lat_in, half_ref, first_ref, last_ref, own_ref, sems):
    tok = lat_in.shape[0]
    start = pl.multiple_of(lax.axis_index("dp") * (D // 2), D // 2)
    sub = own_ref.shape[0]
    first = pl.multiple_of(lax.axis_index("tp") * sub, sub)
    moves = [
        pltpu.make_async_copy(w_in.at[:, pl.ds(start, D // 2)], half_ref, sems.at[0]),
        pltpu.make_async_copy(lat_in.at[:WINDOW, :], first_ref, sems.at[1]),
        pltpu.make_async_copy(lat_in.at[tok - WINDOW :, :], last_ref, sems.at[2]),
        pltpu.make_async_copy(lat_in.at[pl.ds(first, sub), :], own_ref, sems.at[3]),
    ]
    for move in moves:
        move.start()
    for move in moves:
        move.wait()


def context_kernel(mod_ref, ctx_ref, wk_ref, wv_ref, gain_ref, kgain_ref, kv_ref, vec_ref):
    shift_lat, scale_lat, shift_ctx, scale_ctx, gate = vectors_of(mod_ref)
    gain = gain_ref[...]
    vec_ref[0:1, :] = gain * (1.0 + scale_lat)
    vec_ref[1:2, :] = shift_lat
    vec_ref[2:3, :] = gate
    rows = (normed(ctx_ref[...]) * (gain * (1.0 + scale_ctx)) + shift_ctx).astype(BF16)
    keys = head_norm(jnp.dot(rows, wk_ref[...], preferred_element_type=F32), kgain_ref[...])
    values = jnp.dot(rows, wv_ref[...], preferred_element_type=F32)
    both = jnp.concatenate([keys, values], axis=1).astype(BF16)
    kv_ref[...] = jnp.broadcast_to(both[None], kv_ref.shape)


def qkv_kernel(
    lat_in, before_in, after_in, wq_in, wk_in, wv_in,
    vec_ref, qgain_ref, kgain_ref, rcos_ref, rsin_ref, ccos_ref, csin_ref,
    q_ref, near_ref, sum_ref,
    lat_ref, wq_ref, wk_ref, wv_ref, k_ref, v_ref, even_ref, odd_ref, sems,
):
    step = 256
    tok = lat_in.shape[0]
    steps = tok // step
    qgain = qgain_ref[...] * QUERY_SCALE
    kgain = kgain_ref[...]

    def at(i, size=step):
        return pl.ds(pl.multiple_of(i * step, step), size)

    sources = [(lat_in.at[at(i), :], lat_ref.at[at(i), :]) for i in range(steps)]
    sources += [
        (before_in, lat_ref.at[pl.ds(tok, WINDOW), :]),
        (after_in, lat_ref.at[pl.ds(tok + WINDOW, WINDOW), :]),
        (wk_in, wk_ref), (wv_in, wv_ref), (wq_in, wq_ref),
    ]
    moves = [
        pltpu.make_async_copy(source, to, sems.at[i]) for i, (source, to) in enumerate(sources)
    ]
    for i in (0, steps + 2, steps + 3, steps + 4, *range(1, steps + 2)):
        moves[i].start()

    def tables(groups):
        cosines = [rcos_ref[pl.ds(g, 1), :] + ccos_ref[...] for g in groups]
        sines = [rsin_ref[pl.ds(g, 1), :] + csin_ref[...] for g in groups]
        return jnp.concatenate(cosines), jnp.concatenate(sines)

    def fill(i, to):
        values = lat_ref[at(i), :].astype(F32)
        inverse = lax.rsqrt(jnp.mean(values * values, axis=-1, keepdims=True) + NORM_EPSILON)
        to[...] = (values * inverse * vec_ref[0:1, :] + vec_ref[1:2, :]).astype(BF16)

    def keys_of(rows_ref, cosine, sine):
        keys = jnp.dot(rows_ref[...], wk_ref[...], preferred_element_type=F32)
        keys = rotated(head_norm(keys, kgain), cosine, sine).astype(BF16)
        return keys, jnp.dot(rows_ref[...], wv_ref[...], preferred_element_type=F32).astype(BF16)

    def project(i, rows_ref):
        to = pl.ds(pl.multiple_of(i * step + WINDOW, WINDOW), step)
        first = 2 + i * (step // GRID_W)
        cosine, sine = tables([first + g for g in range(step // GRID_W)])
        queries = jnp.dot(rows_ref[...], wq_ref[...], preferred_element_type=F32)
        k_ref[to, :], v_ref[to, :] = keys_of(rows_ref, cosine, sine)
        for h in range(4):
            head = slice(h * HEAD_DIM, (h + 1) * HEAD_DIM)
            turned = rotated(head_norm(queries[:, head], qgain), cosine, sine).astype(BF16)
            for half in range(2):
                q_ref[i * 2 + half, h * WINDOW : (h + 1) * WINDOW, :] = turned[
                    half * WINDOW : (half + 1) * WINDOW
                ]

    moves[0].wait()
    fill(0, even_ref)
    for i in range(steps + 2, steps + 5):
        moves[i].wait()

    def wait_rows(i):
        pltpu.make_async_copy(lat_in.at[at(0), :], lat_ref.at[at(i), :], sems.at[i]).wait()

    def body(j, carry):
        wait_rows(2 * j + 1)

        @pl.when(j == 0)
        def _():
            wait_rows(2)

        @pl.when(j == 1)
        def _():
            moves[steps].wait()
            moves[steps + 1].wait()

        fill(2 * j + 1, odd_ref)
        project(2 * j, even_ref)
        fill(2 * j + 2, even_ref)
        project(2 * j + 1, odd_ref)
        return carry

    lax.fori_loop(0, steps // 2, body, 0)
    beyond = (tok + WINDOW) // GRID_W
    keys, values = keys_of(even_ref, *tables([0, 1, beyond, beyond + 1]))
    for ref, rows in ((k_ref, keys), (v_ref, values)):
        ref[:WINDOW, :] = rows[:WINDOW]
        ref[tok + WINDOW :, :] = rows[WINDOW:]
    local_pass(q_ref, k_ref, v_ref, near_ref, sum_ref)


def contract_last(a, b):
    return lax.dot_general(a, b, (((1,), (1,)), ((), ())), preferred_element_type=F32)


def lanes_summed(values):
    parts = [values[:, i : i + 128] for i in range(0, values.shape[1], 128)]
    while len(parts) > 1:
        parts = [sum(parts[i : i + 2]) for i in range(0, len(parts), 2)]
    return parts[0]


def local_pass(q_ref, k_ref, v_ref, out_ref, sum_ref):
    sp = sp_index()
    blocks = q_ref.shape[0]
    query_at = lax.broadcasted_iota(jnp.int32, (4 * WINDOW, WINDOW), 0) % WINDOW
    key_at = lax.broadcasted_iota(jnp.int32, (4 * WINDOW, WINDOW), 1)
    in_before, in_after = key_at >= query_at, key_at <= query_at

    sum_ref[...] = jnp.zeros(sum_ref.shape, F32)

    def body(block, carry):
        near = pl.ds(pl.multiple_of(block * WINDOW, WINDOW), 3 * WINDOW)
        no_before = (block == 0) & (sp == 0)
        no_after = (block == blocks - 1) & (sp == NZ * NY - 1)
        local = jnp.exp2(contract_last(q_ref[block], k_ref[near, :]))
        local = jnp.concatenate(
            [
                jnp.where(in_before & jnp.logical_not(no_before), local[:, :WINDOW], 0.0),
                local[:, WINDOW : 2 * WINDOW],
                jnp.where(in_after & jnp.logical_not(no_after), local[:, 2 * WINDOW :], 0.0),
            ],
            axis=1,
        )
        total = jnp.sum(lanes_summed(local), axis=-1, keepdims=True)
        sum_ref[...] = jnp.where(key_at == block, total, sum_ref[...])
        mixed = jnp.dot(local.astype(BF16), v_ref[near, :], preferred_element_type=F32)
        out_ref[block] = mixed.astype(BF16)
        return carry

    lax.fori_loop(0, blocks, body, 0)


def attend_kernel(by, q_ref, near_ref, sum_ref, ctx_ref, sink_ref, out_ref):
    quarter = (lax.axis_index("tp") + by) % NX
    head = HEAD_DIM
    sink = jnp.concatenate(
        [jnp.exp(jnp.full((WINDOW, 1), sink_ref[0, h], F32)) for h in range(4)], axis=0
    )

    lane = lax.broadcasted_iota(jnp.int32, sum_ref.shape, 1)

    def body(i, carry):
        block = quarter * 2 + i
        base = pl.ds(pl.multiple_of(i * WINDOW, WINDOW), WINDOW)
        far = jnp.exp2(contract_last(q_ref[block], ctx_ref[:, :head]))
        near_sum = jnp.where(lane == block, sum_ref[...], 0.0)
        total = jnp.sum(lanes_summed(far) + near_sum, axis=-1, keepdims=True) + sink
        mixed = near_ref[block].astype(F32) + jnp.dot(
            far.astype(BF16), ctx_ref[:, head:], preferred_element_type=F32
        )
        mixed = (mixed * (1.0 / total)).astype(BF16)
        for h in range(4):
            out_ref[base, h * head : (h + 1) * head] = mixed[h * WINDOW : (h + 1) * WINDOW]
        return carry

    lax.fori_loop(0, 2, body, 0)


def project_kernel(
    vec_ref, a0_ref, a1_ref, a2_ref, a3_ref, w0_ref,
    m1_ref, m2_ref, m3_ref, o1_ref, o2_ref, o3_ref, lat_ref, out_ref, done_ref, sems,
):
    dp = lax.axis_index("dp")
    col = 512

    def copy(slot, column):
        return pltpu.make_async_copy(
            done_ref.at[slot], out_ref.at[:, pl.ds(column, col)], sems.at[slot]
        )

    for part, weights in enumerate(((m1_ref, m2_ref, m3_ref), (o1_ref, o2_ref, o3_ref))):
        half = dp if part == 0 else 1 - dp

        def body(j, carry, part=part, weights=weights, half=half):
            column = pl.multiple_of(half * (D // 2) + j * col, col)
            wide = pl.ds(column, col)
            sub = pl.ds(pl.multiple_of(j * col, col), col)
            mixed = jnp.dot(a0_ref[...], w0_ref[:, wide], preferred_element_type=F32)
            for a, w in zip((a1_ref, a2_ref, a3_ref), weights):
                mixed = mixed + jnp.dot(a[...], w[:, sub], preferred_element_type=F32)
            slot = part * 2 + j
            result = lat_ref[:, wide].astype(F32) + vec_ref[2:3, wide] * mixed
            done_ref[slot] = result.astype(BF16)
            copy(slot, column).start()
            return carry

        lax.fori_loop(0, 2, body, 0)
    for slot in range(4):
        copy(slot, 0).wait()


def shifted(array, axis, by):
    peers = lax.axis_size(axis)
    return lax.ppermute(array, axis, [(i, (i + by) % peers) for i in range(peers)])


VMEM = pl.BlockSpec(memory_space=pltpu.VMEM)
SMEM = pl.BlockSpec(memory_space=pltpu.SMEM)
HBM = pl.BlockSpec(memory_space=pltpu.HBM)


def call(kernel, outs, args, estimate, limit, scratch=(), in_specs=None, out_specs=None):
    shapes = [jax.ShapeDtypeStruct(s, t) for s, t in outs]
    single = len(shapes) == 1
    return pl.pallas_call(
        kernel,
        in_specs=in_specs or [VMEM] * len(args),
        out_specs=out_specs or (VMEM if single else [VMEM] * len(shapes)),
        out_shape=shapes[0] if single else shapes,
        scratch_shapes=list(scratch),
        compiler_params=params(limit),
        cost_estimate=estimate,
    )(*args)


def per_device(
    latent, context, cond, ctx_cond, norm_gain, mod_shift, mod_scale, mod_gate,
    w_query, w_key, w_value, w_out, q_gain, k_gain, sinks,
):
    lat = latent[0]
    tok = lat.shape[0]
    sub = tok // NX
    sp = sp_index()
    width = 4 * HEAD_DIM

    part = call(
        partial_kernel, [((NY * NX, 24, 128), BF16)],
        (cond, ctx_cond[None], mod_shift, mod_scale, mod_gate), cost(1 << 20, 1 << 18), 62,
        scratch=[
            pltpu.VMEM((1, D), F32), pltpu.VMEM((1, D), F32), pltpu.VMEM((64, 512), BF16),
            pltpu.VMEM((64, 512), BF16), pltpu.VMEM((64, 512), BF16),
            pltpu.SemaphoreType.DMA((5,)),
        ],
        in_specs=[HBM] * 5,
    )
    part = lax.all_to_all(part, ("y", "tp"), 0, 0, tiled=True)
    part = call(resum_kernel, [((NZ, NX * VECS, 128), BF16)], (part,), cost(1 << 20, 1 << 18), 4)
    mod = lax.all_to_all(part, "z", 0, 0, tiled=True)

    half, first_rows, last_rows, own = call(
        stage_kernel,
        [((width, D // 2), BF16), ((WINDOW, D), BF16), ((WINDOW, D), BF16), ((sub, D), BF16)],
        (w_out, lat), cost(1 << 24, 4 << 20), 60,
        scratch=[pltpu.SemaphoreType.DMA((4,))], in_specs=[HBM] * 2,
    )
    peers = NZ * NY
    up = [(i, i + 1) for i in range(peers - 1)]
    before = lax.ppermute(last_rows, SP, up)
    after = lax.ppermute(first_rows, SP, [(j, i) for i, j in up])

    mine, other = {}, {}
    for s in (1, 3, 2):
        mine[s] = shifted(half, "tp", s)
        other[s] = shifted(mine[s], "dp", 1)

    quarter = HEAD_DIM // 4
    lane = jnp.arange(HEAD_DIM)
    frequency = ROPE_BASE ** (-(lane % quarter).astype(F32) / quarter)
    sign = jnp.where((lane // quarter) % 2 == 0, -1.0, 1.0).astype(F32)
    by_row = lane < HEAD_DIM // 2
    grid_row = (sp * tok - WINDOW) // GRID_W + jnp.arange(24, dtype=jnp.int32)
    row_angle = grid_row.astype(F32)[:, None] * frequency
    col_angle = jnp.arange(GRID_W, dtype=F32)[:, None] * frequency
    row_cos = jnp.where(by_row, jnp.cos(row_angle), 0.0)
    row_sin = jnp.where(by_row, jnp.sin(row_angle) * sign, 0.0)
    col_cos = jnp.where(by_row, 0.0, jnp.cos(col_angle))
    col_sin = jnp.where(by_row, 0.0, jnp.sin(col_angle) * sign)

    rows = tok + 2 * WINDOW
    gain, qgain, kgain = norm_gain[None], q_gain[None], k_gain[None]
    n_ctx = context.shape[1]
    ctx_kv, vec = call(
        context_kernel,
        [((peers, n_ctx, 2 * HEAD_DIM), BF16), ((8, D), F32)],
        (mod, context[0], w_key, w_value, gain, kgain),
        cost(2 * n_ctx * D * 256, D * 512), 63,
    )
    ctx_all = lax.all_to_all(ctx_kv, SP, 0, 0, tiled=True).reshape(-1, 2 * HEAD_DIM)

    queries, near, sums = call(
        qkv_kernel,
        [
            ((tok // WINDOW, 4 * WINDOW, HEAD_DIM), BF16),
            ((tok // WINDOW, 4 * WINDOW, HEAD_DIM), BF16), ((4 * WINDOW, 128), F32),
        ],
        (
            lat, before, after, w_query, w_key, w_value, vec, qgain, kgain,
            row_cos, row_sin, col_cos, col_sin,
        ),
        cost(2 * tok * D * 768 + 16 * tok * 384 * HEAD_DIM, tok * D * 2 + D * 768 * 2), 60,
        scratch=[
            pltpu.VMEM((rows, D), BF16), pltpu.VMEM((D, width), BF16),
            pltpu.VMEM((D, HEAD_DIM), BF16), pltpu.VMEM((D, HEAD_DIM), BF16),
            pltpu.VMEM((rows, HEAD_DIM), BF16), pltpu.VMEM((rows, HEAD_DIM), BF16),
            pltpu.VMEM((256, D), BF16), pltpu.VMEM((256, D), BF16),
            pltpu.SemaphoreType.DMA((tok // 256 + 5,)),
        ],
        in_specs=[HBM] * 6 + [VMEM] * 7,
    )

    arrived = {}
    for s in (2, 1, 3, 0):
        piece = call(
            lambda *refs, s=s: attend_kernel(s, *refs), [((sub, width), BF16)],
            (queries, near, sums, ctx_all, sinks[None]),
            cost(4 * 4 * sub * 768 * HEAD_DIM, 2 << 20, 4 * sub * 768), 8,
            in_specs=[VMEM] * 4 + [SMEM],
        )
        if s == 0:
            arrived[s] = piece
        else:
            arrived[s] = shifted(piece, "tp", s)

    result = call(
        project_kernel, [((sub, D), BF16)],
        (
            vec, arrived[0], arrived[1], arrived[2], arrived[3], w_out,
            mine[1], mine[2], mine[3], other[1], other[2], other[3], own,
        ),
        cost(2 * sub * D * D, D * D * 2), 8,
        scratch=[
            pltpu.VMEM((4, sub, 512), BF16), pltpu.SemaphoreType.DMA((4,)),
        ],
        out_specs=HBM,
    )
    return result[None]


def solution(mesh):
    grid = Mesh(mesh.devices.reshape(NZ, NY, NX, 2), ("z", "y", "tp", "dp"))
    in_specs = (
        P("dp", SP, None),
        P("dp", SP, None),
        P("dp", None),
        P(),
        P(),
        P(SP, "tp"),
        P(SP, "tp"),
        P(SP, "tp"),
        P(None, "tp"),
        P(None, "tp"),
        P(None, "tp"),
        P("tp", None),
        P(),
        P(),
        P("tp"),
    )
    out_specs = P("dp", ("z", "y", "tp"), None)

    return jax.shard_map(
        per_device, mesh=grid, in_specs=in_specs, out_specs=out_specs, check_vma=False
    )
```

```python
import math

import jax
import jax.numpy as jnp
from jax import lax
from jax.experimental import pallas as pl
from jax.experimental.pallas import tpu as pltpu
from jax.sharding import Mesh, PartitionSpec as P


HEAD_DIM = 128
WINDOW = 128
GRID_W = 64
NORM_EPSILON = 1e-06
ROPE_BASE = 10000.0
D = 2048
VECS = 20
NZ, NY, NX = 8, 4, 4
SP = ("z", "y")

F32 = jnp.float32
BF16 = jnp.bfloat16
QUERY_SCALE = HEAD_DIM ** (-0.5) * math.log2(math.e)


def sp_index():
    return lax.axis_index("z") * NY + lax.axis_index("y")


def params(vmem_mib):
    return pltpu.CompilerParams(vmem_limit_bytes=vmem_mib * 1024 * 1024)


def cost(flops, nbytes, trans=0):
    return pl.CostEstimate(flops=flops, bytes_accessed=nbytes, transcendentals=trans)


def partial_kernel(cond_in, ctx_in, shift_in, scale_in, gate_in, out_ref,
                   cond_ref, ctx_ref, shift_ref, scale_ref, gate_ref, sems):
    moves = [
        pltpu.make_async_copy(source, to, sems.at[i])
        for i, (source, to) in enumerate(
            (
                (cond_in, cond_ref), (ctx_in, ctx_ref), (shift_in, shift_ref),
                (scale_in, scale_ref), (gate_in, gate_ref),
            )
        )
    ]
    for move in moves:
        move.start()
    for move in moves:
        move.wait()
    sp = sp_index()
    start = pl.multiple_of((sp // 2) * 128, 128)
    row = lax.broadcasted_iota(jnp.int32, (8, 128), 0)
    lane = lax.broadcasted_iota(jnp.int32, (8, 128), 1)
    rows = jnp.where(
        row == 0,
        cond_ref[:, pl.ds(start, 128)],
        jnp.where(row == 1, ctx_ref[:, pl.ds(start, 128)], 0.0),
    )
    active = rows / (1.0 + jnp.exp(-rows))
    active = jnp.where((lane // 64) == (sp % 2), active, 0.0).astype(BF16)

    def times(ref):
        matrix = ref[...]
        return jnp.dot(
            active, jnp.concatenate([matrix, matrix], axis=0), preferred_element_type=F32
        )

    shifts, scales, gates = times(shift_ref), times(scale_ref), times(gate_ref)
    pieces = []
    for values, at in ((shifts, 0), (scales, 0), (shifts, 1), (scales, 1), (gates, 0)):
        for i in range(4):
            pieces.append(values[at : at + 1, i * 128 : (i + 1) * 128])
    pieces.append(jnp.zeros((4, 128), F32))
    stacked = jnp.concatenate(pieces, axis=0).astype(BF16)
    out_ref[...] = jnp.broadcast_to(stacked[None], out_ref.shape)


def resum_kernel(in_ref, out_ref):
    pieces = []
    for t in range(NX):
        rows = None
        for y in range(NY):
            part = in_ref[y * NX + t].astype(F32)
            rows = part if rows is None else rows + part
        pieces.append(rows[:VECS])
    total = jnp.concatenate(pieces, axis=0).astype(BF16)
    out_ref[...] = jnp.broadcast_to(total[None], out_ref.shape)


def vectors_of(mod_ref):
    rows = None
    for z in range(NZ):
        part = mod_ref[z].astype(F32)
        rows = part if rows is None else rows + part
    found = []
    for v in range(5):
        pieces = []
        for t in range(NX):
            for i in range(4):
                at = t * VECS + v * 4 + i
                pieces.append(rows[at : at + 1, :])
        found.append(jnp.concatenate(pieces, axis=1))
    return found


def normed(values):
    values = values.astype(F32)
    return values * lax.rsqrt(jnp.mean(values * values, axis=-1, keepdims=True) + NORM_EPSILON)


def head_norm(v, gain):
    return v * lax.rsqrt(jnp.mean(v * v, axis=-1, keepdims=True) + NORM_EPSILON) * gain


def rotated(v, cosine, sine):
    lane = lax.broadcasted_iota(jnp.int32, v.shape, 1)
    odd = ((lane // 32) % 2) == 1
    swapped = jnp.where(odd, pltpu.roll(v, 32, 1), pltpu.roll(v, 96, 1))
    return v * cosine + swapped * sine


def stage_kernel(w_in, lat_in, half_ref, first_ref, last_ref, sems):
    tok = lat_in.shape[0]
    start = pl.multiple_of(lax.axis_index("dp") * (D // 2), D // 2)
    moves = [
        pltpu.make_async_copy(w_in.at[:, pl.ds(start, D // 2)], half_ref, sems.at[0]),
        pltpu.make_async_copy(lat_in.at[:WINDOW, :], first_ref, sems.at[1]),
        pltpu.make_async_copy(lat_in.at[tok - WINDOW :, :], last_ref, sems.at[2]),
    ]
    for move in moves:
        move.start()
    for move in moves:
        move.wait()


def own_kernel(lat_in, own_ref, sem):
    sub = own_ref.shape[0]
    first = pl.multiple_of(lax.axis_index("tp") * sub, sub)
    move = pltpu.make_async_copy(lat_in.at[pl.ds(first, sub), :], own_ref, sem)
    move.start()
    move.wait()


def context_kernel(
    mod_ref, ctx_ref, wk_in, wv_in, gain_ref, kgain_ref, kv_ref, vec_ref, wkv_ref, sems
):
    moves = [
        pltpu.make_async_copy(wk_in, wkv_ref.at[:, :HEAD_DIM], sems.at[0]),
        pltpu.make_async_copy(wv_in, wkv_ref.at[:, HEAD_DIM:], sems.at[1]),
    ]
    for move in moves:
        move.start()
    shift_lat, scale_lat, shift_ctx, scale_ctx, gate = vectors_of(mod_ref)
    gain = gain_ref[...]
    vec_ref[0:1, :] = gain * (1.0 + scale_lat)
    vec_ref[1:2, :] = shift_lat
    vec_ref[2:3, :] = gate
    rows = (normed(ctx_ref[...]) * (gain * (1.0 + scale_ctx)) + shift_ctx).astype(BF16)
    for move in moves:
        move.wait()
    both = jnp.dot(rows, wkv_ref[...], preferred_element_type=F32)
    keys = head_norm(both[:, :HEAD_DIM], kgain_ref[...])
    both = jnp.concatenate([keys, both[:, HEAD_DIM:]], axis=1).astype(BF16)
    kv_ref[...] = jnp.broadcast_to(both[None], kv_ref.shape)


def qkv_kernel(
    lat_in, before_in, after_in, wq_in, wk_in, wv_in,
    vec_ref, qgain_ref, kgain_ref, rcos_ref, rsin_ref, ccos_ref, csin_ref,
    out_ref, lat_ref, wq_ref, wkv_ref, k_ref, v_ref, even_ref, odd_ref, sum_ref, sems,
):
    step = 256
    tok = lat_in.shape[0]
    steps = tok // step
    qgain = qgain_ref[...] * QUERY_SCALE
    kgain = kgain_ref[...]

    def at(i, size=step):
        return pl.ds(pl.multiple_of(i * step, step), size)

    sources = [(lat_in.at[at(i), :], lat_ref.at[at(i), :]) for i in range(steps)]
    sources += [
        (before_in, lat_ref.at[pl.ds(tok, WINDOW), :]),
        (after_in, lat_ref.at[pl.ds(tok + WINDOW, WINDOW), :]),
        (wk_in, wkv_ref.at[:, :HEAD_DIM]), (wv_in, wkv_ref.at[:, HEAD_DIM:]), (wq_in, wq_ref),
    ]
    moves = [
        pltpu.make_async_copy(source, to, sems.at[i]) for i, (source, to) in enumerate(sources)
    ]
    for i in (0, steps + 2, steps + 3, steps + 4, *range(1, steps + 2)):
        moves[i].start()

    def tables(groups):
        cosines = [rcos_ref[pl.ds(g, 1), :] + ccos_ref[...] for g in groups]
        sines = [rsin_ref[pl.ds(g, 1), :] + csin_ref[...] for g in groups]
        return jnp.concatenate(cosines), jnp.concatenate(sines)

    def fill(i, to):
        values = lat_ref[at(i), :].astype(F32)
        inverse = lax.rsqrt(jnp.mean(values * values, axis=-1, keepdims=True) + NORM_EPSILON)
        to[...] = (values * inverse * vec_ref[0:1, :] + vec_ref[1:2, :]).astype(BF16)

    def keys_of(rows_ref, cosine, sine):
        both = jnp.dot(rows_ref[...], wkv_ref[...], preferred_element_type=F32)
        keys = rotated(head_norm(both[:, :HEAD_DIM], kgain), cosine, sine).astype(BF16)
        return keys, both[:, HEAD_DIM:].astype(BF16)

    def project(i, rows_ref):
        to = pl.ds(pl.multiple_of(i * step + WINDOW, WINDOW), step)
        first = 2 + i * (step // GRID_W)
        cosine, sine = tables([first + g for g in range(step // GRID_W)])
        queries = jnp.dot(rows_ref[...], wq_ref[...], preferred_element_type=F32)
        k_ref[to, :], v_ref[to, :] = keys_of(rows_ref, cosine, sine)
        for h in range(4):
            head = slice(h * HEAD_DIM, (h + 1) * HEAD_DIM)
            turned = rotated(head_norm(queries[:, head], qgain), cosine, sine).astype(BF16)
            for half in range(2):
                out_ref[i * 2 + half, h * WINDOW : (h + 1) * WINDOW, :HEAD_DIM] = turned[
                    half * WINDOW : (half + 1) * WINDOW
                ]

    moves[0].wait()
    fill(0, even_ref)
    for i in range(steps + 2, steps + 5):
        moves[i].wait()

    def wait_rows(i):
        pltpu.make_async_copy(lat_in.at[at(0), :], lat_ref.at[at(i), :], sems.at[i]).wait()

    def body(j, carry):
        wait_rows(2 * j + 1)

        @pl.when(j == 0)
        def _():
            wait_rows(2)

        @pl.when(j == 1)
        def _():
            moves[steps].wait()
            moves[steps + 1].wait()

        fill(2 * j + 1, odd_ref)
        project(2 * j, even_ref)
        fill(2 * j + 2, even_ref)
        project(2 * j + 1, odd_ref)
        return carry

    lax.fori_loop(0, steps // 2, body, 0)
    beyond = (tok + WINDOW) // GRID_W
    keys, values = keys_of(even_ref, *tables([0, 1, beyond, beyond + 1]))
    for ref, rows in ((k_ref, keys), (v_ref, values)):
        ref[:WINDOW, :] = rows[:WINDOW]
        ref[tok + WINDOW :, :] = rows[WINDOW:]
    local_pass(out_ref, k_ref, v_ref, sum_ref)


def contract_last(a, b):
    return lax.dot_general(a, b, (((1,), (1,)), ((), ())), preferred_element_type=F32)


def lanes_summed(values):
    parts = [values[:, i : i + 128] for i in range(0, values.shape[1], 128)]
    while len(parts) > 1:
        parts = [sum(parts[i : i + 2]) for i in range(0, len(parts), 2)]
    return parts[0]


def local_pass(out_ref, k_ref, v_ref, sum_ref):
    sp = sp_index()
    blocks = out_ref.shape[0] - 1
    query_at = lax.broadcasted_iota(jnp.int32, (4 * WINDOW, WINDOW), 0) % WINDOW
    key_at = lax.broadcasted_iota(jnp.int32, (4 * WINDOW, WINDOW), 1)
    in_before, in_after = key_at >= query_at, key_at <= query_at

    sum_ref[...] = jnp.zeros(sum_ref.shape, F32)

    def body(block, carry):
        near = pl.ds(pl.multiple_of(block * WINDOW, WINDOW), 3 * WINDOW)
        no_before = (block == 0) & (sp == 0)
        no_after = (block == blocks - 1) & (sp == NZ * NY - 1)
        local = jnp.exp2(contract_last(out_ref[block, :, :HEAD_DIM], k_ref[near, :]))
        local = jnp.concatenate(
            [
                jnp.where(in_before & jnp.logical_not(no_before), local[:, :WINDOW], 0.0),
                local[:, WINDOW : 2 * WINDOW],
                jnp.where(in_after & jnp.logical_not(no_after), local[:, 2 * WINDOW :], 0.0),
            ],
            axis=1,
        )
        total = jnp.sum(lanes_summed(local), axis=-1, keepdims=True)
        sum_ref[...] = jnp.where(key_at == block, total, sum_ref[...])
        mixed = jnp.dot(local.astype(BF16), v_ref[near, :], preferred_element_type=F32)
        out_ref[block, :, HEAD_DIM:] = mixed.astype(BF16)
        return carry

    lax.fori_loop(0, blocks, body, 0)
    high = sum_ref[...].astype(BF16)
    out_ref[blocks, :, :HEAD_DIM] = high
    out_ref[blocks, :, HEAD_DIM:] = (sum_ref[...] - high.astype(F32)).astype(BF16)


def attend_kernel(shifts, packed_ref, ctx_ref, sink_ref, *out_refs):
    head = HEAD_DIM
    last = packed_ref.shape[0] - 1
    tp = lax.axis_index("tp")
    sink = jnp.concatenate(
        [jnp.exp(jnp.full((WINDOW, 1), sink_ref[0, h], F32)) for h in range(4)], axis=0
    )
    lane = lax.broadcasted_iota(jnp.int32, (4 * WINDOW, 128), 1)
    sums = packed_ref[last, :, :head].astype(F32) + packed_ref[last, :, head:].astype(F32)

    for by, out_ref in zip(shifts, out_refs):
        quarter = (tp + by) % NX

        def body(i, carry, quarter=quarter, out_ref=out_ref):
            block = quarter * 2 + i
            base = pl.ds(pl.multiple_of(i * WINDOW, WINDOW), WINDOW)
            far = jnp.exp2(contract_last(packed_ref[block, :, :head], ctx_ref[:, :head]))
            near_sum = jnp.where(lane == block, sums, 0.0)
            total = jnp.sum(lanes_summed(far) + near_sum, axis=-1, keepdims=True) + sink
            mixed = packed_ref[block, :, head:].astype(F32) + jnp.dot(
                far.astype(BF16), ctx_ref[:, head:], preferred_element_type=F32
            )
            mixed = (mixed * (1.0 / total)).astype(BF16)
            for h in range(4):
                out_ref[base, h * head : (h + 1) * head] = mixed[h * WINDOW : (h + 1) * WINDOW]
            return carry

        lax.fori_loop(0, 2, body, 0)


def project_kernel(
    vec_ref, a0_ref, a1_ref, a2_ref, a3_ref, w0_ref,
    m1_in, m2_in, m3_in, o1_ref, o2_ref, o3_ref, lat_ref, out_ref,
    m1_ref, m2_ref, m3_ref, done_ref, sems,
):
    dp = lax.axis_index("dp")
    col = 512
    moves = [
        pltpu.make_async_copy(source, to, sems.at[4 + i])
        for i, (source, to) in enumerate(((m1_in, m1_ref), (m2_in, m2_ref), (m3_in, m3_ref)))
    ]
    for move in moves:
        move.start()

    def copy(slot, column):
        return pltpu.make_async_copy(
            done_ref.at[slot], out_ref.at[:, pl.ds(column, col)], sems.at[slot]
        )

    for part, weights in enumerate(((o1_ref, o2_ref, o3_ref), (m1_ref, m2_ref, m3_ref))):
        half = 1 - dp if part == 0 else dp
        if part == 1:
            for move in moves:
                move.wait()

        def body(j, carry, part=part, weights=weights, half=half):
            column = pl.multiple_of(half * (D // 2) + j * col, col)
            wide = pl.ds(column, col)
            sub = pl.ds(pl.multiple_of(j * col, col), col)
            mixed = jnp.dot(a0_ref[...], w0_ref[:, wide], preferred_element_type=F32)
            for a, w in zip((a1_ref, a2_ref, a3_ref), weights):
                mixed = mixed + jnp.dot(a[...], w[:, sub], preferred_element_type=F32)
            slot = part * 2 + j
            result = lat_ref[:, wide].astype(F32) + vec_ref[2:3, wide] * mixed
            done_ref[slot] = result.astype(BF16)
            copy(slot, column).start()
            return carry

        lax.fori_loop(0, 2, body, 0)
    for slot in range(4):
        copy(slot, 0).wait()


def shifted(array, axis, by):
    peers = lax.axis_size(axis)
    return lax.ppermute(array, axis, [(i, (i + by) % peers) for i in range(peers)])


VMEM = pl.BlockSpec(memory_space=pltpu.VMEM)
SMEM = pl.BlockSpec(memory_space=pltpu.SMEM)
HBM = pl.BlockSpec(memory_space=pltpu.HBM)


def call(kernel, outs, args, estimate, limit, scratch=(), in_specs=None, out_specs=None):
    shapes = [jax.ShapeDtypeStruct(s, t) for s, t in outs]
    single = len(shapes) == 1
    return pl.pallas_call(
        kernel,
        in_specs=in_specs or [VMEM] * len(args),
        out_specs=out_specs or (VMEM if single else [VMEM] * len(shapes)),
        out_shape=shapes[0] if single else shapes,
        scratch_shapes=list(scratch),
        compiler_params=params(limit),
        cost_estimate=estimate,
    )(*args)


def per_device(
    latent, context, cond, ctx_cond, norm_gain, mod_shift, mod_scale, mod_gate,
    w_query, w_key, w_value, w_out, q_gain, k_gain, sinks,
):
    lat = latent[0]
    tok = lat.shape[0]
    sub = tok // NX
    sp = sp_index()
    width = 4 * HEAD_DIM

    part = call(
        partial_kernel, [((NY * NX, 24, 128), BF16)],
        (cond, ctx_cond[None], mod_shift, mod_scale, mod_gate), cost(1 << 20, 1 << 18), 62,
        scratch=[
            pltpu.VMEM((1, D), F32), pltpu.VMEM((1, D), F32), pltpu.VMEM((64, 512), BF16),
            pltpu.VMEM((64, 512), BF16), pltpu.VMEM((64, 512), BF16),
            pltpu.SemaphoreType.DMA((5,)),
        ],
        in_specs=[HBM] * 5,
    )
    part = lax.all_to_all(part, ("y", "tp"), 0, 0, tiled=True)
    part = call(resum_kernel, [((NZ, NX * VECS, 128), BF16)], (part,), cost(1 << 20, 1 << 18), 4)
    mod = lax.all_to_all(part, "z", 0, 0, tiled=True)

    half, first_rows, last_rows = call(
        stage_kernel,
        [((width, D // 2), BF16), ((WINDOW, D), BF16), ((WINDOW, D), BF16)],
        (w_out, lat), cost(1 << 24, 4 << 20), 60,
        scratch=[pltpu.SemaphoreType.DMA((3,))], in_specs=[HBM] * 2,
    )
    own = call(
        own_kernel, [((sub, D), BF16)], (lat,), cost(1 << 24, 2 << 20), 62,
        scratch=[pltpu.SemaphoreType.DMA], in_specs=[HBM],
    )
    peers = NZ * NY
    up = [(i, i + 1) for i in range(peers - 1)]
    before = lax.ppermute(last_rows, SP, up)
    after = lax.ppermute(first_rows, SP, [(j, i) for i, j in up])

    mine, other = {}, {}
    for s in (1, 3, 2):
        mine[s] = shifted(half, "tp", s)
        other[s] = shifted(mine[s], "dp", 1)

    quarter = HEAD_DIM // 4
    lane = jnp.arange(HEAD_DIM)
    frequency = ROPE_BASE ** (-(lane % quarter).astype(F32) / quarter)
    sign = jnp.where((lane // quarter) % 2 == 0, -1.0, 1.0).astype(F32)
    by_row = lane < HEAD_DIM // 2
    grid_row = (sp * tok - WINDOW) // GRID_W + jnp.arange(24, dtype=jnp.int32)
    row_angle = grid_row.astype(F32)[:, None] * frequency
    col_angle = jnp.arange(GRID_W, dtype=F32)[:, None] * frequency
    row_cos = jnp.where(by_row, jnp.cos(row_angle), 0.0)
    row_sin = jnp.where(by_row, jnp.sin(row_angle) * sign, 0.0)
    col_cos = jnp.where(by_row, 0.0, jnp.cos(col_angle))
    col_sin = jnp.where(by_row, 0.0, jnp.sin(col_angle) * sign)

    rows = tok + 2 * WINDOW
    gain, qgain, kgain = norm_gain[None], q_gain[None], k_gain[None]
    n_ctx = context.shape[1]
    ctx_kv, vec = call(
        context_kernel,
        [((peers, n_ctx, 2 * HEAD_DIM), BF16), ((8, D), F32)],
        (mod, context[0], w_key, w_value, gain, kgain),
        cost(2 * n_ctx * D * 256, D * 512), 63,
        scratch=[pltpu.VMEM((D, 2 * HEAD_DIM), BF16), pltpu.SemaphoreType.DMA((2,))],
        in_specs=[VMEM, VMEM, HBM, HBM, VMEM, VMEM],
    )
    ctx_all = lax.all_to_all(ctx_kv, SP, 0, 0, tiled=True).reshape(-1, 2 * HEAD_DIM)

    packed = call(
        qkv_kernel, [((tok // WINDOW + 1, 4 * WINDOW, 2 * HEAD_DIM), BF16)],
        (
            lat, before, after, w_query, w_key, w_value, vec, qgain, kgain,
            row_cos, row_sin, col_cos, col_sin,
        ),
        cost(2 * tok * D * 768 + 16 * tok * 384 * HEAD_DIM, tok * D * 2 + D * 768 * 2), 60,
        scratch=[
            pltpu.VMEM((rows, D), BF16), pltpu.VMEM((D, width), BF16),
            pltpu.VMEM((D, 2 * HEAD_DIM), BF16),
            pltpu.VMEM((rows, HEAD_DIM), BF16), pltpu.VMEM((rows, HEAD_DIM), BF16),
            pltpu.VMEM((256, D), BF16), pltpu.VMEM((256, D), BF16),
            pltpu.VMEM((4 * WINDOW, 128), F32),
            pltpu.SemaphoreType.DMA((tok // 256 + 5,)),
        ],
        in_specs=[HBM] * 6 + [VMEM] * 7,
    )

    arrived = {}
    for shifts in ((2,), (1, 3), (0,)):
        pieces = call(
            lambda *refs, shifts=shifts: attend_kernel(shifts, *refs),
            [((sub, width), BF16)] * len(shifts), (packed, ctx_all, sinks[None]),
            cost(16 * len(shifts) * sub * 768 * HEAD_DIM, 2 << 20, 4 * len(shifts) * sub * 768), 8,
            in_specs=[VMEM] * 2 + [SMEM],
        )
        for s, piece in zip(shifts, pieces if len(shifts) > 1 else [pieces]):
            if s == 0:
                arrived[s] = piece
            else:
                arrived[s] = shifted(piece, "tp", s)

    result = call(
        project_kernel, [((sub, D), BF16)],
        (
            vec, arrived[0], arrived[1], arrived[2], arrived[3], w_out,
            mine[1], mine[2], mine[3], other[1], other[2], other[3], own,
        ),
        cost(2 * sub * D * D, D * D * 2), 24,
        scratch=[
            *[pltpu.VMEM((width, D // 2), BF16)] * 3,
            pltpu.VMEM((4, sub, 512), BF16), pltpu.SemaphoreType.DMA((7,)),
        ],
        in_specs=[VMEM] * 6 + [HBM] * 3 + [VMEM] * 4,
        out_specs=HBM,
    )
    return result[None]


def solution(mesh):
    grid = Mesh(mesh.devices.reshape(NZ, NY, NX, 2), ("z", "y", "tp", "dp"))
    in_specs = (
        P("dp", SP, None),
        P("dp", SP, None),
        P("dp", None),
        P(),
        P(),
        P(SP, "tp"),
        P(SP, "tp"),
        P(SP, "tp"),
        P(None, "tp"),
        P(None, "tp"),
        P(None, "tp"),
        P("tp", None),
        P(),
        P(),
        P("tp"),
    )
    out_specs = P("dp", ("z", "y", "tp"), None)

    return jax.shard_map(
        per_device, mesh=grid, in_specs=in_specs, out_specs=out_specs, check_vma=False
    )
```

```python
import math

import jax
import jax.numpy as jnp
from jax import lax
from jax.experimental import pallas as pl
from jax.experimental.pallas import tpu as pltpu
from jax.sharding import Mesh, PartitionSpec as P


HEAD_DIM = 128
WINDOW = 128
GRID_W = 64
NORM_EPSILON = 1e-06
ROPE_BASE = 10000.0
D = 2048
NZ, NY, NX = 8, 4, 4
SP = ("z", "y")

F32 = jnp.float32
BF16 = jnp.bfloat16
QUERY_SCALE = HEAD_DIM ** (-0.5) * math.log2(math.e)


def sp_index():
    return lax.axis_index("z") * NY + lax.axis_index("y")


def params(vmem_mib):
    return pltpu.CompilerParams(vmem_limit_bytes=vmem_mib * 1024 * 1024)


def cost(flops, nbytes, trans=0):
    return pl.CostEstimate(flops=flops, bytes_accessed=nbytes, transcendentals=trans)


def partial_kernel(
    cond_in, ctx_in, shift_in, scale_in, gate_in, w_in, lat_in,
    out_ref, half_out, first_out, last_out,
    cond_ref, ctx_ref, shift_ref, scale_ref, gate_ref, half_ref, first_ref, last_ref, sems,
):
    tok = lat_in.shape[0]
    column = pl.multiple_of(lax.axis_index("dp") * (D // 2), D // 2)

    def moves_of(pairs, base):
        return [
            pltpu.make_async_copy(source, to, sems.at[base + i])
            for i, (source, to) in enumerate(pairs)
        ]

    moves = moves_of(
        (
            (cond_in, cond_ref), (ctx_in, ctx_ref), (shift_in, shift_ref),
            (scale_in, scale_ref), (gate_in, gate_ref),
        ),
        0,
    )
    stage_in = moves_of(
        (
            (w_in.at[:, pl.ds(column, D // 2)], half_ref),
            (lat_in.at[:WINDOW, :], first_ref), (lat_in.at[tok - WINDOW :, :], last_ref),
        ),
        5,
    )
    stage_out = moves_of(
        ((half_ref, half_out), (first_ref, first_out), (last_ref, last_out)), 8
    )
    for move in moves + stage_in:
        move.start()
    for move in moves:
        move.wait()
    sp = sp_index()
    start = pl.multiple_of((sp // 2) * 128, 128)
    row = lax.broadcasted_iota(jnp.int32, (8, 128), 0)
    lane = lax.broadcasted_iota(jnp.int32, (8, 128), 1)
    rows = jnp.where(
        row == 0,
        cond_ref[:, pl.ds(start, 128)],
        jnp.where(row == 1, ctx_ref[:, pl.ds(start, 128)], 0.0),
    )
    active = rows / (1.0 + jnp.exp(-rows))
    active = jnp.where((lane // 64) == (sp % 2), active, 0.0).astype(BF16)

    def times(ref):
        matrix = ref[...]
        return jnp.dot(
            active, jnp.concatenate([matrix, matrix], axis=0), preferred_element_type=F32
        )

    shifts, scales, gates = times(shift_ref), times(scale_ref), times(gate_ref)
    pieces = []
    for values, at in ((shifts, 0), (scales, 0), (shifts, 1), (scales, 1), (gates, 0)):
        for i in range(4):
            pieces.append(values[at : at + 1, i * 128 : (i + 1) * 128])
    pieces.append(jnp.zeros((4, 128), F32))
    stacked = jnp.concatenate(pieces, axis=0).astype(BF16)
    out_ref[...] = jnp.broadcast_to(stacked[None], out_ref.shape)
    for arrived, move in zip(stage_in, stage_out):
        arrived.wait()
        move.start()
    for move in stage_out:
        move.wait()


def vectors_of(mod_ref):
    totals = []
    for t in range(NX):
        rows = None
        for p in range(NZ * NY):
            part = mod_ref[p * NX + t].astype(F32)
            rows = part if rows is None else rows + part
        totals.append(rows)
    found = []
    for v in range(5):
        pieces = []
        for t in range(NX):
            for i in range(4):
                pieces.append(totals[t][v * 4 + i : v * 4 + i + 1, :])
        found.append(jnp.concatenate(pieces, axis=1))
    return found


def normed(values):
    values = values.astype(F32)
    return values * lax.rsqrt(jnp.mean(values * values, axis=-1, keepdims=True) + NORM_EPSILON)


def head_norm(v, gain):
    return v * lax.rsqrt(jnp.mean(v * v, axis=-1, keepdims=True) + NORM_EPSILON) * gain


def rotated(v, cosine, sine):
    lane = lax.broadcasted_iota(jnp.int32, v.shape, 1)
    odd = ((lane // 32) % 2) == 1
    swapped = jnp.where(odd, pltpu.roll(v, 32, 1), pltpu.roll(v, 96, 1))
    return v * cosine + swapped * sine


def context_kernel(
    mod_ref, ctx_ref, wk_ref, wv_ref, gain_ref, kgain_ref, kv_ref, vec_ref
):
    shift_lat, scale_lat, shift_ctx, scale_ctx, gate = vectors_of(mod_ref)
    gain = gain_ref[...]
    vec_ref[0:1, :] = gain * (1.0 + scale_lat)
    vec_ref[1:2, :] = shift_lat
    vec_ref[2:3, :] = gate
    rows = (normed(ctx_ref[...]) * (gain * (1.0 + scale_ctx)) + shift_ctx).astype(BF16)
    keys = head_norm(jnp.dot(rows, wk_ref[...], preferred_element_type=F32), kgain_ref[...])
    values = jnp.dot(rows, wv_ref[...], preferred_element_type=F32)
    both = jnp.concatenate([keys, values], axis=1).astype(BF16)
    kv_ref[...] = jnp.broadcast_to(both[None], kv_ref.shape)


def qkv_kernel(
    lat_in, before_in, after_in, wq_in, wk_in, wv_in,
    vec_ref, qgain_ref, kgain_ref, rcos_ref, rsin_ref, ccos_ref, csin_ref,
    out_ref, own_ref, lat_ref, wq_ref, wkv_ref, k_ref, v_ref, even_ref, odd_ref, sum_ref, sems,
):
    step = 256
    tok = lat_in.shape[0]
    steps = tok // step
    qgain = qgain_ref[...] * QUERY_SCALE
    kgain = kgain_ref[...]

    def at(i, size=step):
        return pl.ds(pl.multiple_of(i * step, step), size)

    sources = [(lat_in.at[at(i), :], lat_ref.at[at(i), :]) for i in range(steps)]
    sources += [
        (before_in, lat_ref.at[pl.ds(tok, WINDOW), :]),
        (after_in, lat_ref.at[pl.ds(tok + WINDOW, WINDOW), :]),
        (wk_in, wkv_ref.at[:, :HEAD_DIM]), (wv_in, wkv_ref.at[:, HEAD_DIM:]), (wq_in, wq_ref),
    ]
    moves = [
        pltpu.make_async_copy(source, to, sems.at[i]) for i, (source, to) in enumerate(sources)
    ]
    for i in (0, steps + 2, steps + 3, steps + 4, *range(1, steps + 2)):
        moves[i].start()

    def tables(groups):
        cosines = [rcos_ref[pl.ds(g, 1), :] + ccos_ref[...] for g in groups]
        sines = [rsin_ref[pl.ds(g, 1), :] + csin_ref[...] for g in groups]
        return jnp.concatenate(cosines), jnp.concatenate(sines)

    def fill(i, to):
        values = lat_ref[at(i), :].astype(F32)
        inverse = lax.rsqrt(jnp.mean(values * values, axis=-1, keepdims=True) + NORM_EPSILON)
        to[...] = (values * inverse * vec_ref[0:1, :] + vec_ref[1:2, :]).astype(BF16)

    def keys_of(rows_ref, cosine, sine):
        both = jnp.dot(rows_ref[...], wkv_ref[...], preferred_element_type=F32)
        keys = rotated(head_norm(both[:, :HEAD_DIM], kgain), cosine, sine).astype(BF16)
        return keys, both[:, HEAD_DIM:].astype(BF16)

    def project(i, rows_ref):
        to = pl.ds(pl.multiple_of(i * step + WINDOW, WINDOW), step)
        first = 2 + i * (step // GRID_W)
        cosine, sine = tables([first + g for g in range(step // GRID_W)])
        queries = jnp.dot(rows_ref[...], wq_ref[...], preferred_element_type=F32)
        k_ref[to, :], v_ref[to, :] = keys_of(rows_ref, cosine, sine)
        for h in range(4):
            head = slice(h * HEAD_DIM, (h + 1) * HEAD_DIM)
            turned = rotated(head_norm(queries[:, head], qgain), cosine, sine).astype(BF16)
            for half in range(2):
                out_ref[i * 2 + half, h * WINDOW : (h + 1) * WINDOW, :HEAD_DIM] = turned[
                    half * WINDOW : (half + 1) * WINDOW
                ]

    moves[0].wait()
    fill(0, even_ref)
    for i in range(steps + 2, steps + 5):
        moves[i].wait()

    def wait_rows(i):
        pltpu.make_async_copy(lat_in.at[at(0), :], lat_ref.at[at(i), :], sems.at[i]).wait()

    def body(j, carry):
        wait_rows(2 * j + 1)

        @pl.when(j == 0)
        def _():
            wait_rows(2)

        @pl.when(j == 1)
        def _():
            moves[steps].wait()
            moves[steps + 1].wait()

        fill(2 * j + 1, odd_ref)
        project(2 * j, even_ref)
        fill(2 * j + 2, even_ref)
        project(2 * j + 1, odd_ref)
        return carry

    lax.fori_loop(0, steps // 2, body, 0)
    own_move = pltpu.make_async_copy(
        lat_ref.at[at(lax.axis_index("tp"), own_ref.shape[0]), :], own_ref, sems.at[steps + 5]
    )
    own_move.start()
    beyond = (tok + WINDOW) // GRID_W
    keys, values = keys_of(even_ref, *tables([0, 1, beyond, beyond + 1]))
    for ref, rows in ((k_ref, keys), (v_ref, values)):
        ref[:WINDOW, :] = rows[:WINDOW]
        ref[tok + WINDOW :, :] = rows[WINDOW:]
    local_pass(out_ref, k_ref, v_ref, sum_ref)
    own_move.wait()


def contract_last(a, b):
    return lax.dot_general(a, b, (((1,), (1,)), ((), ())), preferred_element_type=F32)


def lanes_summed(values):
    parts = [values[:, i : i + 128] for i in range(0, values.shape[1], 128)]
    while len(parts) > 1:
        parts = [sum(parts[i : i + 2]) for i in range(0, len(parts), 2)]
    return parts[0]


def local_pass(out_ref, k_ref, v_ref, sum_ref):
    sp = sp_index()
    blocks = out_ref.shape[0] - 1
    query_at = lax.broadcasted_iota(jnp.int32, (4 * WINDOW, WINDOW), 0) % WINDOW
    key_at = lax.broadcasted_iota(jnp.int32, (4 * WINDOW, WINDOW), 1)
    in_before, in_after = key_at >= query_at, key_at <= query_at

    sum_ref[...] = jnp.zeros(sum_ref.shape, F32)

    def body(block, carry):
        near = pl.ds(pl.multiple_of(block * WINDOW, WINDOW), 3 * WINDOW)
        no_before = (block == 0) & (sp == 0)
        no_after = (block == blocks - 1) & (sp == NZ * NY - 1)
        local = jnp.exp2(contract_last(out_ref[block, :, :HEAD_DIM], k_ref[near, :]))
        local = jnp.concatenate(
            [
                jnp.where(in_before & jnp.logical_not(no_before), local[:, :WINDOW], 0.0),
                local[:, WINDOW : 2 * WINDOW],
                jnp.where(in_after & jnp.logical_not(no_after), local[:, 2 * WINDOW :], 0.0),
            ],
            axis=1,
        )
        total = jnp.sum(lanes_summed(local), axis=-1, keepdims=True)
        sum_ref[...] = jnp.where(key_at == block, total, sum_ref[...])
        mixed = jnp.dot(local.astype(BF16), v_ref[near, :], preferred_element_type=F32)
        out_ref[block, :, HEAD_DIM:] = mixed.astype(BF16)
        return carry

    lax.fori_loop(0, blocks, body, 0)
    high = sum_ref[...].astype(BF16)
    out_ref[blocks, :, :HEAD_DIM] = high
    out_ref[blocks, :, HEAD_DIM:] = (sum_ref[...] - high.astype(F32)).astype(BF16)


def attend_kernel(shifts, packed_ref, ctx_ref, sink_ref, *out_refs):
    head = HEAD_DIM
    last = packed_ref.shape[0] - 1
    tp = lax.axis_index("tp")
    sink = jnp.concatenate(
        [jnp.exp(jnp.full((WINDOW, 1), sink_ref[0, h], F32)) for h in range(4)], axis=0
    )
    lane = lax.broadcasted_iota(jnp.int32, (4 * WINDOW, 128), 1)
    sums = packed_ref[last, :, :head].astype(F32) + packed_ref[last, :, head:].astype(F32)

    for by, out_ref in zip(shifts, out_refs):
        quarter = (tp + by) % NX

        def body(i, carry, quarter=quarter, out_ref=out_ref):
            block = quarter * 2 + i
            base = pl.ds(pl.multiple_of(i * WINDOW, WINDOW), WINDOW)
            far = jnp.exp2(contract_last(packed_ref[block, :, :head], ctx_ref[:, :head]))
            near_sum = jnp.where(lane == block, sums, 0.0)
            total = jnp.sum(lanes_summed(far) + near_sum, axis=-1, keepdims=True) + sink
            mixed = packed_ref[block, :, head:].astype(F32) + jnp.dot(
                far.astype(BF16), ctx_ref[:, head:], preferred_element_type=F32
            )
            mixed = (mixed * (1.0 / total)).astype(BF16)
            for h in range(4):
                out_ref[base, h * head : (h + 1) * head] = mixed[h * WINDOW : (h + 1) * WINDOW]
            return carry

        lax.fori_loop(0, 2, body, 0)


def project_kernel(
    vec_ref, a0_ref, a1_ref, a2_ref, a3_ref, w0_ref,
    m1_in, m2_in, m3_in, o1_ref, o2_ref, o3_ref, lat_ref, out_ref,
    m1_ref, m2_ref, m3_ref, done_ref, sems,
):
    dp = lax.axis_index("dp")
    col = 512
    moves = [
        pltpu.make_async_copy(source, to, sems.at[4 + i])
        for i, (source, to) in enumerate(((m1_in, m1_ref), (m2_in, m2_ref), (m3_in, m3_ref)))
    ]
    for move in moves:
        move.start()

    def copy(slot, column):
        return pltpu.make_async_copy(
            done_ref.at[slot], out_ref.at[:, pl.ds(column, col)], sems.at[slot]
        )

    for part, weights in enumerate(((o1_ref, o2_ref, o3_ref), (m1_ref, m2_ref, m3_ref))):
        half = 1 - dp if part == 0 else dp
        if part == 1:
            for move in moves:
                move.wait()

        def body(j, carry, part=part, weights=weights, half=half):
            column = pl.multiple_of(half * (D // 2) + j * col, col)
            wide = pl.ds(column, col)
            sub = pl.ds(pl.multiple_of(j * col, col), col)
            mixed = jnp.dot(a0_ref[...], w0_ref[:, wide], preferred_element_type=F32)
            for a, w in zip((a1_ref, a2_ref, a3_ref), weights):
                mixed = mixed + jnp.dot(a[...], w[:, sub], preferred_element_type=F32)
            slot = part * 2 + j
            result = lat_ref[:, wide].astype(F32) + vec_ref[2:3, wide] * mixed
            done_ref[slot] = result.astype(BF16)
            copy(slot, column).start()
            return carry

        lax.fori_loop(0, 2, body, 0)
    for slot in range(4):
        copy(slot, 0).wait()


def shifted(array, axis, by):
    peers = lax.axis_size(axis)
    return lax.ppermute(array, axis, [(i, (i + by) % peers) for i in range(peers)])


VMEM = pl.BlockSpec(memory_space=pltpu.VMEM)
SMEM = pl.BlockSpec(memory_space=pltpu.SMEM)
HBM = pl.BlockSpec(memory_space=pltpu.HBM)


def call(kernel, outs, args, estimate, limit, scratch=(), in_specs=None, out_specs=None):
    shapes = [jax.ShapeDtypeStruct(s, t) for s, t in outs]
    single = len(shapes) == 1
    return pl.pallas_call(
        kernel,
        in_specs=in_specs or [VMEM] * len(args),
        out_specs=out_specs or (VMEM if single else [VMEM] * len(shapes)),
        out_shape=shapes[0] if single else shapes,
        scratch_shapes=list(scratch),
        compiler_params=params(limit),
        cost_estimate=estimate,
    )(*args)


def per_device(
    latent, context, cond, ctx_cond, norm_gain, mod_shift, mod_scale, mod_gate,
    w_query, w_key, w_value, w_out, q_gain, k_gain, sinks,
):
    lat = latent[0]
    tok = lat.shape[0]
    sub = tok // NX
    sp = sp_index()
    width = 4 * HEAD_DIM

    peers = NZ * NY
    small = pltpu.VMEM((64, 512), BF16)
    edge_rows = ((WINDOW, D), BF16)
    part, half, first_rows, last_rows = call(
        partial_kernel,
        [((peers * NX, 24, 128), BF16), ((width, D // 2), BF16), edge_rows, edge_rows],
        (cond, ctx_cond[None], mod_shift, mod_scale, mod_gate, w_out, lat),
        cost(1 << 20, 1 << 18), 62,
        scratch=[
            pltpu.VMEM((1, D), F32), pltpu.VMEM((1, D), F32), small, small, small,
            pltpu.VMEM((width, D // 2), BF16), pltpu.VMEM((WINDOW, D), BF16),
            pltpu.VMEM((WINDOW, D), BF16), pltpu.SemaphoreType.DMA((11,)),
        ],
        in_specs=[HBM] * 7,
        out_specs=[VMEM, HBM, HBM, HBM],
    )
    mod = lax.all_to_all(part, ("z", "y", "tp"), 0, 0, tiled=True)

    up = [(i, i + 1) for i in range(peers - 1)]
    before = lax.ppermute(last_rows, SP, up)
    after = lax.ppermute(first_rows, SP, [(j, i) for i, j in up])

    mine, other = {}, {}
    for s in (1, 3, 2):
        mine[s] = shifted(half, "tp", s)
        other[s] = shifted(mine[s], "dp", 1)

    quarter = HEAD_DIM // 4
    lane = jnp.arange(HEAD_DIM)
    frequency = ROPE_BASE ** (-(lane % quarter).astype(F32) / quarter)
    sign = jnp.where((lane // quarter) % 2 == 0, -1.0, 1.0).astype(F32)
    by_row = lane < HEAD_DIM // 2
    grid_row = (sp * tok - WINDOW) // GRID_W + jnp.arange(24, dtype=jnp.int32)
    row_angle = grid_row.astype(F32)[:, None] * frequency
    col_angle = jnp.arange(GRID_W, dtype=F32)[:, None] * frequency
    row_cos = jnp.where(by_row, jnp.cos(row_angle), 0.0)
    row_sin = jnp.where(by_row, jnp.sin(row_angle) * sign, 0.0)
    col_cos = jnp.where(by_row, 0.0, jnp.cos(col_angle))
    col_sin = jnp.where(by_row, 0.0, jnp.sin(col_angle) * sign)

    rows = tok + 2 * WINDOW
    gain, qgain, kgain = norm_gain[None], q_gain[None], k_gain[None]
    n_ctx = context.shape[1]
    ctx_kv, vec = call(
        context_kernel,
        [((peers, n_ctx, 2 * HEAD_DIM), BF16), ((8, D), F32)],
        (mod, context[0], w_key, w_value, gain, kgain),
        cost(2 * n_ctx * D * 256, D * 512), 58,
    )
    ctx_all = lax.all_to_all(ctx_kv, SP, 0, 0, tiled=True).reshape(-1, 2 * HEAD_DIM)

    packed, own = call(
        qkv_kernel,
        [((tok // WINDOW + 1, 4 * WINDOW, 2 * HEAD_DIM), BF16), ((sub, D), BF16)],
        (
            lat, before, after, w_query, w_key, w_value, vec, qgain, kgain,
            row_cos, row_sin, col_cos, col_sin,
        ),
        cost(2 * tok * D * 768 + 16 * tok * 384 * HEAD_DIM, tok * D * 2 + D * 768 * 2), 60,
        scratch=[
            pltpu.VMEM((rows, D), BF16), pltpu.VMEM((D, width), BF16),
            pltpu.VMEM((D, 2 * HEAD_DIM), BF16),
            pltpu.VMEM((rows, HEAD_DIM), BF16), pltpu.VMEM((rows, HEAD_DIM), BF16),
            pltpu.VMEM((256, D), BF16), pltpu.VMEM((256, D), BF16),
            pltpu.VMEM((4 * WINDOW, 128), F32),
            pltpu.SemaphoreType.DMA((tok // 256 + 6,)),
        ],
        in_specs=[HBM] * 6 + [VMEM] * 7,
        out_specs=[VMEM, HBM],
    )

    arrived = {}
    for shifts in ((2,), (1, 3), (0,)):
        pieces = call(
            lambda *refs, shifts=shifts: attend_kernel(shifts, *refs),
            [((sub, width), BF16)] * len(shifts), (packed, ctx_all, sinks[None]),
            cost(16 * len(shifts) * sub * 768 * HEAD_DIM, 2 << 20, 4 * len(shifts) * sub * 768), 8,
            in_specs=[VMEM] * 2 + [SMEM],
        )
        for s, piece in zip(shifts, pieces if len(shifts) > 1 else [pieces]):
            if s == 0:
                arrived[s] = piece
            else:
                arrived[s] = shifted(piece, "tp", s)

    result = call(
        project_kernel, [((sub, D), BF16)],
        (
            vec, arrived[0], arrived[1], arrived[2], arrived[3], w_out,
            mine[1], mine[2], mine[3], other[1], other[2], other[3], own,
        ),
        cost(2 * sub * D * D, D * D * 2), 24,
        scratch=[
            *[pltpu.VMEM((width, D // 2), BF16)] * 3,
            pltpu.VMEM((4, sub, 512), BF16), pltpu.SemaphoreType.DMA((7,)),
        ],
        in_specs=[VMEM] * 6 + [HBM] * 3 + [VMEM] * 4,
        out_specs=HBM,
    )
    return result[None]


def solution(mesh):
    grid = Mesh(mesh.devices.reshape(NZ, NY, NX, 2), ("z", "y", "tp", "dp"))
    in_specs = (
        P("dp", SP, None),
        P("dp", SP, None),
        P("dp", None),
        P(),
        P(),
        P(SP, "tp"),
        P(SP, "tp"),
        P(SP, "tp"),
        P(None, "tp"),
        P(None, "tp"),
        P(None, "tp"),
        P("tp", None),
        P(),
        P(),
        P("tp"),
    )
    out_specs = P("dp", ("z", "y", "tp"), None)

    return jax.shard_map(
        per_device, mesh=grid, in_specs=in_specs, out_specs=out_specs, check_vma=False
    )
```

```python
import math

import jax
import jax.numpy as jnp
from jax import lax
from jax.experimental import pallas as pl
from jax.experimental.pallas import tpu as pltpu
from jax.sharding import Mesh, PartitionSpec as P


HEAD_DIM = 128
WINDOW = 128
GRID_W = 64
NORM_EPSILON = 1e-06
ROPE_BASE = 10000.0
D = 2048
VECS = 20
NZ, NY, NX = 8, 4, 4
SP = ("z", "y")

F32 = jnp.float32
BF16 = jnp.bfloat16
QUERY_SCALE = HEAD_DIM ** (-0.5) * math.log2(math.e)


def sp_index():
    return lax.axis_index("z") * NY + lax.axis_index("y")


def params(vmem_mib):
    return pltpu.CompilerParams(vmem_limit_bytes=vmem_mib * 1024 * 1024)


def cost(flops, nbytes, trans=0):
    return pl.CostEstimate(flops=flops, bytes_accessed=nbytes, transcendentals=trans)


def partial_kernel(cond_in, ctx_in, shift_in, scale_in, gate_in, out_ref,
                   cond_ref, ctx_ref, shift_ref, scale_ref, gate_ref, sems):
    moves = [
        pltpu.make_async_copy(source, to, sems.at[i])
        for i, (source, to) in enumerate(
            (
                (cond_in, cond_ref), (ctx_in, ctx_ref), (shift_in, shift_ref),
                (scale_in, scale_ref), (gate_in, gate_ref),
            )
        )
    ]
    for move in moves:
        move.start()
    for move in moves:
        move.wait()
    sp = sp_index()
    start = pl.multiple_of((sp // 2) * 128, 128)
    row = lax.broadcasted_iota(jnp.int32, (8, 128), 0)
    lane = lax.broadcasted_iota(jnp.int32, (8, 128), 1)
    rows = jnp.where(
        row == 0,
        cond_ref[:, pl.ds(start, 128)],
        jnp.where(row == 1, ctx_ref[:, pl.ds(start, 128)], 0.0),
    )
    active = rows / (1.0 + jnp.exp(-rows))
    active = jnp.where((lane // 64) == (sp % 2), active, 0.0).astype(BF16)

    def times(ref):
        matrix = ref[...]
        return jnp.dot(
            active, jnp.concatenate([matrix, matrix], axis=0), preferred_element_type=F32
        )

    shifts, scales, gates = times(shift_ref), times(scale_ref), times(gate_ref)
    pieces = []
    for values, at in ((shifts, 0), (scales, 0), (shifts, 1), (scales, 1), (gates, 0)):
        for i in range(4):
            pieces.append(values[at : at + 1, i * 128 : (i + 1) * 128])
    pieces.append(jnp.zeros((4, 128), F32))
    stacked = jnp.concatenate(pieces, axis=0).astype(BF16)
    out_ref[...] = jnp.broadcast_to(stacked[None], out_ref.shape)


def resum_kernel(in_ref, out_ref):
    pieces = []
    for t in range(NX):
        rows = None
        for y in range(NY):
            part = in_ref[y * NX + t].astype(F32)
            rows = part if rows is None else rows + part
        pieces.append(rows[:VECS])
    total = jnp.concatenate(pieces, axis=0).astype(BF16)
    out_ref[...] = jnp.broadcast_to(total[None], out_ref.shape)


def vectors_of(mod_ref):
    rows = None
    for z in range(NZ):
        part = mod_ref[z].astype(F32)
        rows = part if rows is None else rows + part
    found = []
    for v in range(5):
        pieces = []
        for t in range(NX):
            for i in range(4):
                at = t * VECS + v * 4 + i
                pieces.append(rows[at : at + 1, :])
        found.append(jnp.concatenate(pieces, axis=1))
    return found


def normed(values):
    values = values.astype(F32)
    return values * lax.rsqrt(jnp.mean(values * values, axis=-1, keepdims=True) + NORM_EPSILON)


def head_norm(v, gain):
    return v * lax.rsqrt(jnp.mean(v * v, axis=-1, keepdims=True) + NORM_EPSILON) * gain


def rotated(v, cosine, sine):
    lane = lax.broadcasted_iota(jnp.int32, v.shape, 1)
    odd = ((lane // 32) % 2) == 1
    swapped = jnp.where(odd, pltpu.roll(v, 32, 1), pltpu.roll(v, 96, 1))
    return v * cosine + swapped * sine


def stage_weight_kernel(w_in, half_ref, sem):
    start = pl.multiple_of(lax.axis_index("dp") * (D // 2), D // 2)
    move = pltpu.make_async_copy(w_in.at[:, pl.ds(start, D // 2)], half_ref, sem)
    move.start()
    move.wait()


def stage_rows_kernel(lat_in, first_ref, last_ref, sems):
    tok = lat_in.shape[0]
    moves = [
        pltpu.make_async_copy(lat_in.at[:WINDOW, :], first_ref, sems.at[0]),
        pltpu.make_async_copy(lat_in.at[tok - WINDOW :, :], last_ref, sems.at[1]),
    ]
    for move in moves:
        move.start()
    for move in moves:
        move.wait()


def context_kernel(
    mod_ref, ctx_ref, wk_ref, wv_ref, gain_ref, kgain_ref, kv_ref, vec_ref
):
    shift_lat, scale_lat, shift_ctx, scale_ctx, gate = vectors_of(mod_ref)
    gain = gain_ref[...]
    vec_ref[0:1, :] = gain * (1.0 + scale_lat)
    vec_ref[1:2, :] = shift_lat
    vec_ref[2:3, :] = gate
    rows = (normed(ctx_ref[...]) * (gain * (1.0 + scale_ctx)) + shift_ctx).astype(BF16)
    keys = head_norm(jnp.dot(rows, wk_ref[...], preferred_element_type=F32), kgain_ref[...])
    values = jnp.dot(rows, wv_ref[...], preferred_element_type=F32)
    both = jnp.concatenate([keys, values], axis=1).astype(BF16)
    kv_ref[...] = jnp.broadcast_to(both[None], kv_ref.shape)


def qkv_kernel(
    lat_in, before_in, after_in, wq_in, wk_in, wv_in,
    vec_ref, qgain_ref, kgain_ref, rcos_ref, rsin_ref, ccos_ref, csin_ref,
    packed_out, own_ref, out_ref, lat_ref, wq_ref, wkv_ref, k_ref, v_ref, even_ref, odd_ref,
    sum_ref, sems,
):
    step = 256
    tok = lat_in.shape[0]
    steps = tok // step
    qgain = qgain_ref[...] * QUERY_SCALE
    kgain = kgain_ref[...]

    def at(i, size=step):
        return pl.ds(pl.multiple_of(i * step, step), size)

    sources = [(lat_in.at[at(i), :], lat_ref.at[at(i), :]) for i in range(steps)]
    sources += [
        (before_in, lat_ref.at[pl.ds(tok, WINDOW), :]),
        (after_in, lat_ref.at[pl.ds(tok + WINDOW, WINDOW), :]),
        (wk_in, wkv_ref.at[:, :HEAD_DIM]), (wv_in, wkv_ref.at[:, HEAD_DIM:]), (wq_in, wq_ref),
    ]
    moves = [
        pltpu.make_async_copy(source, to, sems.at[i]) for i, (source, to) in enumerate(sources)
    ]
    for i in (0, steps + 2, steps + 3, steps + 4, *range(1, steps + 2)):
        moves[i].start()

    def tables(groups):
        cosines = [rcos_ref[pl.ds(g, 1), :] + ccos_ref[...] for g in groups]
        sines = [rsin_ref[pl.ds(g, 1), :] + csin_ref[...] for g in groups]
        return jnp.concatenate(cosines), jnp.concatenate(sines)

    def fill(i, to):
        values = lat_ref[at(i), :].astype(F32)
        inverse = lax.rsqrt(jnp.mean(values * values, axis=-1, keepdims=True) + NORM_EPSILON)
        to[...] = (values * inverse * vec_ref[0:1, :] + vec_ref[1:2, :]).astype(BF16)

    def keys_of(rows_ref, cosine, sine):
        both = jnp.dot(rows_ref[...], wkv_ref[...], preferred_element_type=F32)
        keys = rotated(head_norm(both[:, :HEAD_DIM], kgain), cosine, sine).astype(BF16)
        return keys, both[:, HEAD_DIM:].astype(BF16)

    def project(i, rows_ref):
        to = pl.ds(pl.multiple_of(i * step + WINDOW, WINDOW), step)
        first = 2 + i * (step // GRID_W)
        cosine, sine = tables([first + g for g in range(step // GRID_W)])
        queries = jnp.dot(rows_ref[...], wq_ref[...], preferred_element_type=F32)
        k_ref[to, :], v_ref[to, :] = keys_of(rows_ref, cosine, sine)
        for h in range(4):
            head = slice(h * HEAD_DIM, (h + 1) * HEAD_DIM)
            turned = rotated(head_norm(queries[:, head], qgain), cosine, sine).astype(BF16)
            for half in range(2):
                out_ref[i * 2 + half, h * WINDOW : (h + 1) * WINDOW, :HEAD_DIM] = turned[
                    half * WINDOW : (half + 1) * WINDOW
                ]

    moves[0].wait()
    fill(0, even_ref)
    for i in range(steps + 2, steps + 5):
        moves[i].wait()

    def wait_rows(i):
        pltpu.make_async_copy(lat_in.at[at(0), :], lat_ref.at[at(i), :], sems.at[i]).wait()

    def body(j, carry):
        wait_rows(2 * j + 1)

        @pl.when(j == 0)
        def _():
            wait_rows(2)

        @pl.when(j == 1)
        def _():
            moves[steps].wait()
            moves[steps + 1].wait()

        fill(2 * j + 1, odd_ref)
        project(2 * j, even_ref)
        fill(2 * j + 2, even_ref)
        project(2 * j + 1, odd_ref)
        return carry

    lax.fori_loop(0, steps // 2, body, 0)
    own_move = pltpu.make_async_copy(
        lat_ref.at[at(lax.axis_index("tp"), own_ref.shape[0]), :], own_ref, sems.at[steps + 5]
    )
    own_move.start()
    beyond = (tok + WINDOW) // GRID_W
    keys, values = keys_of(even_ref, *tables([0, 1, beyond, beyond + 1]))
    for ref, rows in ((k_ref, keys), (v_ref, values)):
        ref[:WINDOW, :] = rows[:WINDOW]
        ref[tok + WINDOW :, :] = rows[WINDOW:]

    def block_move(block):
        return pltpu.make_async_copy(
            out_ref.at[block], packed_out.at[block], sems.at[steps + 6 + block]
        )

    local_pass(out_ref, k_ref, v_ref, sum_ref, block_move)
    for block in range(packed_out.shape[0]):
        block_move(block).wait()
    own_move.wait()


def contract_last(a, b):
    return lax.dot_general(a, b, (((1,), (1,)), ((), ())), preferred_element_type=F32)


def lanes_summed(values):
    parts = [values[:, i : i + 128] for i in range(0, values.shape[1], 128)]
    while len(parts) > 1:
        parts = [sum(parts[i : i + 2]) for i in range(0, len(parts), 2)]
    return parts[0]


def local_pass(out_ref, k_ref, v_ref, sum_ref, block_move):
    sp = sp_index()
    blocks = out_ref.shape[0] - 1
    query_at = lax.broadcasted_iota(jnp.int32, (4 * WINDOW, WINDOW), 0) % WINDOW
    key_at = lax.broadcasted_iota(jnp.int32, (4 * WINDOW, WINDOW), 1)
    in_before, in_after = key_at >= query_at, key_at <= query_at

    sum_ref[...] = jnp.zeros(sum_ref.shape, F32)

    def body(block, carry):
        near = pl.ds(pl.multiple_of(block * WINDOW, WINDOW), 3 * WINDOW)
        no_before = (block == 0) & (sp == 0)
        no_after = (block == blocks - 1) & (sp == NZ * NY - 1)
        local = jnp.exp2(contract_last(out_ref[block, :, :HEAD_DIM], k_ref[near, :]))
        local = jnp.concatenate(
            [
                jnp.where(in_before & jnp.logical_not(no_before), local[:, :WINDOW], 0.0),
                local[:, WINDOW : 2 * WINDOW],
                jnp.where(in_after & jnp.logical_not(no_after), local[:, 2 * WINDOW :], 0.0),
            ],
            axis=1,
        )
        total = jnp.sum(lanes_summed(local), axis=-1, keepdims=True)
        sum_ref[...] = jnp.where(key_at == block, total, sum_ref[...])
        mixed = jnp.dot(local.astype(BF16), v_ref[near, :], preferred_element_type=F32)
        out_ref[block, :, HEAD_DIM:] = mixed.astype(BF16)
        block_move(block).start()
        return carry

    lax.fori_loop(0, blocks, body, 0)
    high = sum_ref[...].astype(BF16)
    out_ref[blocks, :, :HEAD_DIM] = high
    out_ref[blocks, :, HEAD_DIM:] = (sum_ref[...] - high.astype(F32)).astype(BF16)
    block_move(blocks).start()


def attend_kernel(shifts, packed_ref, ctx_ref, sink_ref, *out_refs):
    head = HEAD_DIM
    last = packed_ref.shape[0] - 1
    tp = lax.axis_index("tp")
    sink = jnp.concatenate(
        [jnp.exp(jnp.full((WINDOW, 1), sink_ref[0, h], F32)) for h in range(4)], axis=0
    )
    lane = lax.broadcasted_iota(jnp.int32, (4 * WINDOW, 128), 1)
    sums = packed_ref[last, :, :head].astype(F32) + packed_ref[last, :, head:].astype(F32)

    for by, out_ref in zip(shifts, out_refs):
        quarter = (tp + by) % NX

        def body(i, carry, quarter=quarter, out_ref=out_ref):
            block = quarter * 2 + i
            base = pl.ds(pl.multiple_of(i * WINDOW, WINDOW), WINDOW)
            far = jnp.exp2(contract_last(packed_ref[block, :, :head], ctx_ref[:, :head]))
            near_sum = jnp.where(lane == block, sums, 0.0)
            total = jnp.sum(lanes_summed(far) + near_sum, axis=-1, keepdims=True) + sink
            mixed = packed_ref[block, :, head:].astype(F32) + jnp.dot(
                far.astype(BF16), ctx_ref[:, head:], preferred_element_type=F32
            )
            mixed = (mixed * (1.0 / total)).astype(BF16)
            for h in range(4):
                out_ref[base, h * head : (h + 1) * head] = mixed[h * WINDOW : (h + 1) * WINDOW]
            return carry

        lax.fori_loop(0, 2, body, 0)


def project_kernel(
    vec_ref, a0_ref, a1_ref, a2_ref, a3_ref, w0_ref,
    m1_in, m2_in, m3_in, o1_ref, o2_ref, o3_ref, lat_ref, out_ref,
    m1_ref, m2_ref, m3_ref, done_ref, sems,
):
    dp = lax.axis_index("dp")
    col = 512
    moves = [
        pltpu.make_async_copy(source, to, sems.at[4 + i])
        for i, (source, to) in enumerate(((m1_in, m1_ref), (m2_in, m2_ref), (m3_in, m3_ref)))
    ]
    for move in moves:
        move.start()

    def copy(slot, column):
        return pltpu.make_async_copy(
            done_ref.at[slot], out_ref.at[:, pl.ds(column, col)], sems.at[slot]
        )

    for part, weights in enumerate(((o1_ref, o2_ref, o3_ref), (m1_ref, m2_ref, m3_ref))):
        half = 1 - dp if part == 0 else dp
        if part == 1:
            for move in moves:
                move.wait()

        def body(j, carry, part=part, weights=weights, half=half):
            column = pl.multiple_of(half * (D // 2) + j * col, col)
            wide = pl.ds(column, col)
            sub = pl.ds(pl.multiple_of(j * col, col), col)
            mixed = jnp.dot(a0_ref[...], w0_ref[:, wide], preferred_element_type=F32)
            for a, w in zip((a1_ref, a2_ref, a3_ref), weights):
                mixed = mixed + jnp.dot(a[...], w[:, sub], preferred_element_type=F32)
            slot = part * 2 + j
            result = lat_ref[:, wide].astype(F32) + vec_ref[2:3, wide] * mixed
            done_ref[slot] = result.astype(BF16)
            copy(slot, column).start()
            return carry

        lax.fori_loop(0, 2, body, 0)
    for slot in range(4):
        copy(slot, 0).wait()


def shifted(array, axis, by):
    peers = lax.axis_size(axis)
    return lax.ppermute(array, axis, [(i, (i + by) % peers) for i in range(peers)])


VMEM = pl.BlockSpec(memory_space=pltpu.VMEM)
SMEM = pl.BlockSpec(memory_space=pltpu.SMEM)
HBM = pl.BlockSpec(memory_space=pltpu.HBM)


def call(kernel, outs, args, estimate, limit, scratch=(), in_specs=None, out_specs=None):
    shapes = [jax.ShapeDtypeStruct(s, t) for s, t in outs]
    single = len(shapes) == 1
    return pl.pallas_call(
        kernel,
        in_specs=in_specs or [VMEM] * len(args),
        out_specs=out_specs or (VMEM if single else [VMEM] * len(shapes)),
        out_shape=shapes[0] if single else shapes,
        scratch_shapes=list(scratch),
        compiler_params=params(limit),
        cost_estimate=estimate,
    )(*args)


def per_device(
    latent, context, cond, ctx_cond, norm_gain, mod_shift, mod_scale, mod_gate,
    w_query, w_key, w_value, w_out, q_gain, k_gain, sinks,
):
    lat = latent[0]
    tok = lat.shape[0]
    sub = tok // NX
    sp = sp_index()
    width = 4 * HEAD_DIM

    part = call(
        partial_kernel, [((NY * NX, 24, 128), BF16)],
        (cond, ctx_cond[None], mod_shift, mod_scale, mod_gate), cost(1 << 20, 1 << 18), 62,
        scratch=[
            pltpu.VMEM((1, D), F32), pltpu.VMEM((1, D), F32), pltpu.VMEM((64, 512), BF16),
            pltpu.VMEM((64, 512), BF16), pltpu.VMEM((64, 512), BF16),
            pltpu.SemaphoreType.DMA((5,)),
        ],
        in_specs=[HBM] * 5,
    )
    part = lax.all_to_all(part, ("y", "tp"), 0, 0, tiled=True)
    part = call(resum_kernel, [((NZ, NX * VECS, 128), BF16)], (part,), cost(1 << 20, 1 << 18), 4)
    mod = lax.all_to_all(part, "z", 0, 0, tiled=True)

    half = call(
        stage_weight_kernel, [((width, D // 2), BF16)], (w_out,),
        cost(1 << 24, 2 << 20), 60, scratch=[pltpu.SemaphoreType.DMA], in_specs=[HBM],
    )
    first_rows, last_rows = call(
        stage_rows_kernel, [((WINDOW, D), BF16)] * 2, (lat,),
        cost(1 << 24, 2 << 20), 60, scratch=[pltpu.SemaphoreType.DMA((2,))], in_specs=[HBM],
    )
    peers = NZ * NY
    up = [(i, i + 1) for i in range(peers - 1)]
    before = lax.ppermute(last_rows, SP, up)
    after = lax.ppermute(first_rows, SP, [(j, i) for i, j in up])

    mine, other = {}, {}
    for s in (1, 3, 2):
        mine[s] = shifted(half, "tp", s)
        other[s] = shifted(mine[s], "dp", 1)

    quarter = HEAD_DIM // 4
    lane = jnp.arange(HEAD_DIM)
    frequency = ROPE_BASE ** (-(lane % quarter).astype(F32) / quarter)
    sign = jnp.where((lane // quarter) % 2 == 0, -1.0, 1.0).astype(F32)
    by_row = lane < HEAD_DIM // 2
    grid_row = (sp * tok - WINDOW) // GRID_W + jnp.arange(24, dtype=jnp.int32)
    row_angle = grid_row.astype(F32)[:, None] * frequency
    col_angle = jnp.arange(GRID_W, dtype=F32)[:, None] * frequency
    row_cos = jnp.where(by_row, jnp.cos(row_angle), 0.0)
    row_sin = jnp.where(by_row, jnp.sin(row_angle) * sign, 0.0)
    col_cos = jnp.where(by_row, 0.0, jnp.cos(col_angle))
    col_sin = jnp.where(by_row, 0.0, jnp.sin(col_angle) * sign)

    rows = tok + 2 * WINDOW
    gain, qgain, kgain = norm_gain[None], q_gain[None], k_gain[None]
    n_ctx = context.shape[1]
    ctx_kv, vec = call(
        context_kernel,
        [((peers, n_ctx, 2 * HEAD_DIM), BF16), ((8, D), F32)],
        (mod, context[0], w_key, w_value, gain, kgain),
        cost(2 * n_ctx * D * 256, D * 512), 63,
    )
    ctx_all = lax.all_to_all(ctx_kv, SP, 0, 0, tiled=True).reshape(-1, 2 * HEAD_DIM)

    packed_shape = (tok // WINDOW + 1, 4 * WINDOW, 2 * HEAD_DIM)
    packed, own = call(
        qkv_kernel, [(packed_shape, BF16), ((sub, D), BF16)],
        (
            lat, before, after, w_query, w_key, w_value, vec, qgain, kgain,
            row_cos, row_sin, col_cos, col_sin,
        ),
        cost(2 * tok * D * 768 + 16 * tok * 384 * HEAD_DIM, tok * D * 2 + D * 768 * 2), 60,
        scratch=[
            pltpu.VMEM(packed_shape, BF16),
            pltpu.VMEM((rows, D), BF16), pltpu.VMEM((D, width), BF16),
            pltpu.VMEM((D, 2 * HEAD_DIM), BF16),
            pltpu.VMEM((rows, HEAD_DIM), BF16), pltpu.VMEM((rows, HEAD_DIM), BF16),
            pltpu.VMEM((256, D), BF16), pltpu.VMEM((256, D), BF16),
            pltpu.VMEM((4 * WINDOW, 128), F32),
            pltpu.SemaphoreType.DMA((tok // 256 + 6 + packed_shape[0],)),
        ],
        in_specs=[HBM] * 6 + [VMEM] * 7,
        out_specs=[HBM, HBM],
    )

    arrived = {}
    for shifts in ((2,), (1, 3), (0,)):
        pieces = call(
            lambda *refs, shifts=shifts: attend_kernel(shifts, *refs),
            [((sub, width), BF16)] * len(shifts), (packed, ctx_all, sinks[None]),
            cost(16 * len(shifts) * sub * 768 * HEAD_DIM, 2 << 20, 4 * len(shifts) * sub * 768), 8,
            in_specs=[VMEM] * 2 + [SMEM],
        )
        for s, piece in zip(shifts, pieces if len(shifts) > 1 else [pieces]):
            if s == 0:
                arrived[s] = piece
            else:
                arrived[s] = shifted(piece, "tp", s)

    result = call(
        project_kernel, [((sub, D), BF16)],
        (
            vec, arrived[0], arrived[1], arrived[2], arrived[3], w_out,
            mine[1], mine[2], mine[3], other[1], other[2], other[3], own,
        ),
        cost(2 * sub * D * D, D * D * 2), 24,
        scratch=[
            *[pltpu.VMEM((width, D // 2), BF16)] * 3,
            pltpu.VMEM((4, sub, 512), BF16), pltpu.SemaphoreType.DMA((7,)),
        ],
        in_specs=[VMEM] * 6 + [HBM] * 3 + [VMEM] * 4,
        out_specs=HBM,
    )
    return result[None]


def solution(mesh):
    grid = Mesh(mesh.devices.reshape(NZ, NY, NX, 2), ("z", "y", "tp", "dp"))
    in_specs = (
        P("dp", SP, None),
        P("dp", SP, None),
        P("dp", None),
        P(),
        P(),
        P(SP, "tp"),
        P(SP, "tp"),
        P(SP, "tp"),
        P(None, "tp"),
        P(None, "tp"),
        P(None, "tp"),
        P("tp", None),
        P(),
        P(),
        P("tp"),
    )
    out_specs = P("dp", ("z", "y", "tp"), None)

    return jax.shard_map(
        per_device, mesh=grid, in_specs=in_specs, out_specs=out_specs, check_vma=False
    )
```

```python
import math

import jax
import jax.numpy as jnp
from jax import lax
from jax.experimental import pallas as pl
from jax.experimental.pallas import tpu as pltpu
from jax.sharding import Mesh, PartitionSpec as P


HEAD_DIM = 128
WINDOW = 128
GRID_W = 64
NORM_EPSILON = 1e-06
ROPE_BASE = 10000.0
D = 2048
VECS = 20
NZ, NY, NX = 8, 4, 4
SP = ("z", "y")

F32 = jnp.float32
BF16 = jnp.bfloat16
QUERY_SCALE = HEAD_DIM ** (-0.5) * math.log2(math.e)


def sp_index():
    return lax.axis_index("z") * NY + lax.axis_index("y")


def params(vmem_mib):
    return pltpu.CompilerParams(vmem_limit_bytes=vmem_mib * 1024 * 1024)


def cost(flops, nbytes, trans=0):
    return pl.CostEstimate(flops=flops, bytes_accessed=nbytes, transcendentals=trans)


def partial_kernel(cond_in, ctx_in, shift_in, scale_in, gate_in, out_ref,
                   cond_ref, ctx_ref, shift_ref, scale_ref, gate_ref, sems):
    moves = [
        pltpu.make_async_copy(source, to, sems.at[i])
        for i, (source, to) in enumerate(
            (
                (cond_in, cond_ref), (ctx_in, ctx_ref), (shift_in, shift_ref),
                (scale_in, scale_ref), (gate_in, gate_ref),
            )
        )
    ]
    for move in moves:
        move.start()
    for move in moves:
        move.wait()
    sp = sp_index()
    start = pl.multiple_of((sp // 2) * 128, 128)
    row = lax.broadcasted_iota(jnp.int32, (8, 128), 0)
    lane = lax.broadcasted_iota(jnp.int32, (8, 128), 1)
    rows = jnp.where(
        row == 0,
        cond_ref[:, pl.ds(start, 128)],
        jnp.where(row == 1, ctx_ref[:, pl.ds(start, 128)], 0.0),
    )
    active = rows / (1.0 + jnp.exp(-rows))
    active = jnp.where((lane // 64) == (sp % 2), active, 0.0).astype(BF16)

    def times(ref):
        matrix = ref[...]
        return jnp.dot(
            active, jnp.concatenate([matrix, matrix], axis=0), preferred_element_type=F32
        )

    shifts, scales, gates = times(shift_ref), times(scale_ref), times(gate_ref)
    pieces = []
    for values, at in ((shifts, 0), (scales, 0), (shifts, 1), (scales, 1), (gates, 0)):
        for i in range(4):
            pieces.append(values[at : at + 1, i * 128 : (i + 1) * 128])
    pieces.append(jnp.zeros((4, 128), F32))
    stacked = jnp.concatenate(pieces, axis=0).astype(BF16)
    out_ref[...] = jnp.broadcast_to(stacked[None], out_ref.shape)


def resum_kernel(in_ref, out_ref):
    pieces = []
    for t in range(NX):
        rows = None
        for y in range(NY):
            part = in_ref[y * NX + t].astype(F32)
            rows = part if rows is None else rows + part
        pieces.append(rows[:VECS])
    total = jnp.concatenate(pieces, axis=0).astype(BF16)
    out_ref[...] = jnp.broadcast_to(total[None], out_ref.shape)


def vectors_of(mod_ref):
    rows = None
    for z in range(NZ):
        part = mod_ref[z].astype(F32)
        rows = part if rows is None else rows + part
    found = []
    for v in range(5):
        pieces = []
        for t in range(NX):
            for i in range(4):
                at = t * VECS + v * 4 + i
                pieces.append(rows[at : at + 1, :])
        found.append(jnp.concatenate(pieces, axis=1))
    return found


def normed(values):
    values = values.astype(F32)
    return values * lax.rsqrt(jnp.mean(values * values, axis=-1, keepdims=True) + NORM_EPSILON)


def head_norm(v, gain):
    return v * lax.rsqrt(jnp.mean(v * v, axis=-1, keepdims=True) + NORM_EPSILON) * gain


def rotated(v, cosine, sine):
    lane = lax.broadcasted_iota(jnp.int32, v.shape, 1)
    odd = ((lane // 32) % 2) == 1
    swapped = jnp.where(odd, pltpu.roll(v, 32, 1), pltpu.roll(v, 96, 1))
    return v * cosine + swapped * sine


def stage_weight_kernel(w_in, half_ref, sem):
    start = pl.multiple_of(lax.axis_index("dp") * (D // 2), D // 2)
    move = pltpu.make_async_copy(w_in.at[:, pl.ds(start, D // 2)], half_ref, sem)
    move.start()
    move.wait()


def rotation(refs, groups):
    row_cos, row_sin, col_cos, col_sin = refs
    cosines = [row_cos[pl.ds(g, 1), :] + col_cos[...] for g in groups]
    sines = [row_sin[pl.ds(g, 1), :] + col_sin[...] for g in groups]
    return jnp.concatenate(cosines), jnp.concatenate(sines)


def context_kernel(
    mod_ref, ctx_ref, wk_ref, wv_ref, gain_ref, kgain_ref, rcos_ref, rsin_ref, ccos_ref, csin_ref,
    lat_in, kv_ref, vec_ref, first_ref, last_ref, edge_ref, rows_ref, sems,
):
    tok = lat_in.shape[0]
    moves = [
        pltpu.make_async_copy(lat_in.at[:WINDOW, :], edge_ref.at[:WINDOW], sems.at[0]),
        pltpu.make_async_copy(lat_in.at[tok - WINDOW :, :], edge_ref.at[WINDOW:], sems.at[1]),
    ]
    for move in moves:
        move.start()
    shift_lat, scale_lat, shift_ctx, scale_ctx, gate = vectors_of(mod_ref)
    gain = gain_ref[...]
    vec_ref[0:1, :] = gain * (1.0 + scale_lat)
    vec_ref[1:2, :] = shift_lat
    vec_ref[2:3, :] = gate
    rows_ref[2 * WINDOW :, :] = (
        normed(ctx_ref[...]) * (gain * (1.0 + scale_ctx)) + shift_ctx
    ).astype(BF16)
    for move in moves:
        move.wait()
    step = 64

    def body(i, carry):
        at = pl.ds(pl.multiple_of(i * step, step), step)
        rows_ref[at, :] = (normed(edge_ref[at, :]) * vec_ref[0:1, :] + vec_ref[1:2, :]).astype(BF16)
        return carry

    lax.fori_loop(0, 2 * WINDOW // step, body, 0)
    keys = head_norm(
        jnp.dot(rows_ref[...], wk_ref[...], preferred_element_type=F32), kgain_ref[...]
    )
    values = jnp.dot(rows_ref[...], wv_ref[...], preferred_element_type=F32).astype(BF16)
    refs = (rcos_ref, rsin_ref, ccos_ref, csin_ref)
    final = tok // GRID_W
    for ref, base, groups in ((first_ref, 0, (2, 3)), (last_ref, WINDOW, (final, final + 1))):
        at = slice(base, base + WINDOW)
        ref[:, :HEAD_DIM] = rotated(keys[at], *rotation(refs, groups)).astype(BF16)
        ref[:, HEAD_DIM:] = values[at]
    both = jnp.concatenate([keys[2 * WINDOW :].astype(BF16), values[2 * WINDOW :]], axis=1)
    kv_ref[...] = jnp.broadcast_to(both[None], kv_ref.shape)


def qkv_kernel(
    lat_in, wq_in, wk_in, wv_in, before_ref, after_ref,
    vec_ref, qgain_ref, kgain_ref, rcos_ref, rsin_ref, ccos_ref, csin_ref,
    packed_out, own_ref, out_ref, lat_ref, wq_ref, wkv_ref, k_ref, v_ref, even_ref, odd_ref,
    sum_ref, sems,
):
    step = 256
    tok = lat_in.shape[0]
    steps = tok // step
    qgain = qgain_ref[...] * QUERY_SCALE
    kgain = kgain_ref[...]

    def at(i, size=step):
        return pl.ds(pl.multiple_of(i * step, step), size)

    sources = [(lat_in.at[at(i), :], lat_ref.at[at(i), :]) for i in range(steps)]
    sources += [
        (wk_in, wkv_ref.at[:, :HEAD_DIM]), (wv_in, wkv_ref.at[:, HEAD_DIM:]), (wq_in, wq_ref),
    ]
    moves = [
        pltpu.make_async_copy(source, to, sems.at[i]) for i, (source, to) in enumerate(sources)
    ]
    for i in (0, steps, steps + 1, steps + 2, *range(1, steps)):
        moves[i].start()
    for ref, edge in ((k_ref, slice(0, HEAD_DIM)), (v_ref, slice(HEAD_DIM, 2 * HEAD_DIM))):
        ref[:WINDOW, :] = before_ref[:, edge]
        ref[tok + WINDOW :, :] = after_ref[:, edge]
    refs = (rcos_ref, rsin_ref, ccos_ref, csin_ref)

    def fill(i, to):
        values = lat_ref[at(i), :].astype(F32)
        inverse = lax.rsqrt(jnp.mean(values * values, axis=-1, keepdims=True) + NORM_EPSILON)
        to[...] = (values * inverse * vec_ref[0:1, :] + vec_ref[1:2, :]).astype(BF16)

    def keys_of(rows_ref, cosine, sine):
        both = jnp.dot(rows_ref[...], wkv_ref[...], preferred_element_type=F32)
        keys = rotated(head_norm(both[:, :HEAD_DIM], kgain), cosine, sine).astype(BF16)
        return keys, both[:, HEAD_DIM:].astype(BF16)

    def project(i, rows_ref):
        to = pl.ds(pl.multiple_of(i * step + WINDOW, WINDOW), step)
        first = 2 + i * (step // GRID_W)
        cosine, sine = rotation(refs, [first + g for g in range(step // GRID_W)])
        queries = jnp.dot(rows_ref[...], wq_ref[...], preferred_element_type=F32)
        k_ref[to, :], v_ref[to, :] = keys_of(rows_ref, cosine, sine)
        for h in range(4):
            head = slice(h * HEAD_DIM, (h + 1) * HEAD_DIM)
            turned = rotated(head_norm(queries[:, head], qgain), cosine, sine).astype(BF16)
            for half in range(2):
                out_ref[i * 2 + half, h * WINDOW : (h + 1) * WINDOW, :HEAD_DIM] = turned[
                    half * WINDOW : (half + 1) * WINDOW
                ]

    moves[0].wait()
    fill(0, even_ref)
    for i in range(steps, steps + 3):
        moves[i].wait()

    def wait_rows(i):
        pltpu.make_async_copy(lat_in.at[at(0), :], lat_ref.at[at(i), :], sems.at[i]).wait()

    def body(j, carry):
        wait_rows(2 * j + 1)

        @pl.when(j == 0)
        def _():
            wait_rows(2)

        fill(2 * j + 1, odd_ref)
        project(2 * j, even_ref)
        fill(jnp.minimum(2 * j + 2, steps - 1), even_ref)
        project(2 * j + 1, odd_ref)
        return carry

    lax.fori_loop(0, steps // 2, body, 0)
    own_move = pltpu.make_async_copy(
        lat_ref.at[at(lax.axis_index("tp"), own_ref.shape[0]), :], own_ref, sems.at[steps + 3]
    )
    own_move.start()

    def block_move(block):
        return pltpu.make_async_copy(
            out_ref.at[block], packed_out.at[block], sems.at[steps + 4 + block]
        )

    local_pass(out_ref, k_ref, v_ref, sum_ref, block_move)
    for block in range(packed_out.shape[0]):
        block_move(block).wait()
    own_move.wait()


def contract_last(a, b):
    return lax.dot_general(a, b, (((1,), (1,)), ((), ())), preferred_element_type=F32)


def lanes_summed(values):
    parts = [values[:, i : i + 128] for i in range(0, values.shape[1], 128)]
    while len(parts) > 1:
        parts = [sum(parts[i : i + 2]) for i in range(0, len(parts), 2)]
    return parts[0]


def local_pass(out_ref, k_ref, v_ref, sum_ref, block_move):
    sp = sp_index()
    blocks = out_ref.shape[0] - 1
    query_at = lax.broadcasted_iota(jnp.int32, (4 * WINDOW, WINDOW), 0) % WINDOW
    key_at = lax.broadcasted_iota(jnp.int32, (4 * WINDOW, WINDOW), 1)
    in_before, in_after = key_at >= query_at, key_at <= query_at

    sum_ref[...] = jnp.zeros(sum_ref.shape, F32)

    def body(block, carry):
        near = pl.ds(pl.multiple_of(block * WINDOW, WINDOW), 3 * WINDOW)
        no_before = (block == 0) & (sp == 0)
        no_after = (block == blocks - 1) & (sp == NZ * NY - 1)
        local = jnp.exp2(contract_last(out_ref[block, :, :HEAD_DIM], k_ref[near, :]))
        local = jnp.concatenate(
            [
                jnp.where(in_before & jnp.logical_not(no_before), local[:, :WINDOW], 0.0),
                local[:, WINDOW : 2 * WINDOW],
                jnp.where(in_after & jnp.logical_not(no_after), local[:, 2 * WINDOW :], 0.0),
            ],
            axis=1,
        )
        total = jnp.sum(lanes_summed(local), axis=-1, keepdims=True)
        sum_ref[...] = jnp.where(key_at == block, total, sum_ref[...])
        mixed = jnp.dot(local.astype(BF16), v_ref[near, :], preferred_element_type=F32)
        out_ref[block, :, HEAD_DIM:] = mixed.astype(BF16)
        block_move(block).start()
        return carry

    lax.fori_loop(0, blocks, body, 0)
    high = sum_ref[...].astype(BF16)
    out_ref[blocks, :, :HEAD_DIM] = high
    out_ref[blocks, :, HEAD_DIM:] = (sum_ref[...] - high.astype(F32)).astype(BF16)
    block_move(blocks).start()


def attend_kernel(shifts, packed_ref, ctx_ref, sink_ref, *out_refs):
    head = HEAD_DIM
    last = packed_ref.shape[0] - 1
    tp = lax.axis_index("tp")
    sink = jnp.concatenate(
        [jnp.exp(jnp.full((WINDOW, 1), sink_ref[0, h], F32)) for h in range(4)], axis=0
    )
    lane = lax.broadcasted_iota(jnp.int32, (4 * WINDOW, 128), 1)
    sums = packed_ref[last, :, :head].astype(F32) + packed_ref[last, :, head:].astype(F32)

    for by, out_ref in zip(shifts, out_refs):
        quarter = (tp + by) % NX

        def body(i, carry, quarter=quarter, out_ref=out_ref):
            block = quarter * 2 + i
            base = pl.ds(pl.multiple_of(i * WINDOW, WINDOW), WINDOW)
            far = jnp.exp2(contract_last(packed_ref[block, :, :head], ctx_ref[:, :head]))
            near_sum = jnp.where(lane == block, sums, 0.0)
            total = jnp.sum(lanes_summed(far) + near_sum, axis=-1, keepdims=True) + sink
            mixed = packed_ref[block, :, head:].astype(F32) + jnp.dot(
                far.astype(BF16), ctx_ref[:, head:], preferred_element_type=F32
            )
            mixed = (mixed * (1.0 / total)).astype(BF16)
            for h in range(4):
                out_ref[base, h * head : (h + 1) * head] = mixed[h * WINDOW : (h + 1) * WINDOW]
            return carry

        lax.fori_loop(0, 2, body, 0)


def project_kernel(
    vec_ref, a0_ref, a1_ref, a2_ref, a3_ref, w0_ref,
    m1_in, m2_in, m3_in, o1_ref, o2_ref, o3_ref, lat_ref, out_ref,
    m1_ref, m2_ref, m3_ref, done_ref, sems,
):
    dp = lax.axis_index("dp")
    col = 512
    moves = [
        pltpu.make_async_copy(source, to, sems.at[4 + i])
        for i, (source, to) in enumerate(((m1_in, m1_ref), (m2_in, m2_ref), (m3_in, m3_ref)))
    ]
    for move in moves:
        move.start()

    def copy(slot, column):
        return pltpu.make_async_copy(
            done_ref.at[slot], out_ref.at[:, pl.ds(column, col)], sems.at[slot]
        )

    for part, weights in enumerate(((o1_ref, o2_ref, o3_ref), (m1_ref, m2_ref, m3_ref))):
        half = 1 - dp if part == 0 else dp
        if part == 1:
            for move in moves:
                move.wait()

        def body(j, carry, part=part, weights=weights, half=half):
            column = pl.multiple_of(half * (D // 2) + j * col, col)
            wide = pl.ds(column, col)
            sub = pl.ds(pl.multiple_of(j * col, col), col)
            mixed = jnp.dot(a0_ref[...], w0_ref[:, wide], preferred_element_type=F32)
            for a, w in zip((a1_ref, a2_ref, a3_ref), weights):
                mixed = mixed + jnp.dot(a[...], w[:, sub], preferred_element_type=F32)
            slot = part * 2 + j
            result = lat_ref[:, wide].astype(F32) + vec_ref[2:3, wide] * mixed
            done_ref[slot] = result.astype(BF16)
            copy(slot, column).start()
            return carry

        lax.fori_loop(0, 2, body, 0)
    for slot in range(4):
        copy(slot, 0).wait()


def shifted(array, axis, by):
    peers = lax.axis_size(axis)
    return lax.ppermute(array, axis, [(i, (i + by) % peers) for i in range(peers)])


VMEM = pl.BlockSpec(memory_space=pltpu.VMEM)
SMEM = pl.BlockSpec(memory_space=pltpu.SMEM)
HBM = pl.BlockSpec(memory_space=pltpu.HBM)


def call(kernel, outs, args, estimate, limit, scratch=(), in_specs=None, out_specs=None):
    shapes = [jax.ShapeDtypeStruct(s, t) for s, t in outs]
    single = len(shapes) == 1
    return pl.pallas_call(
        kernel,
        in_specs=in_specs or [VMEM] * len(args),
        out_specs=out_specs or (VMEM if single else [VMEM] * len(shapes)),
        out_shape=shapes[0] if single else shapes,
        scratch_shapes=list(scratch),
        compiler_params=params(limit),
        cost_estimate=estimate,
    )(*args)


def per_device(
    latent, context, cond, ctx_cond, norm_gain, mod_shift, mod_scale, mod_gate,
    w_query, w_key, w_value, w_out, q_gain, k_gain, sinks,
):
    lat = latent[0]
    tok = lat.shape[0]
    sub = tok // NX
    sp = sp_index()
    width = 4 * HEAD_DIM

    peers = NZ * NY
    part = call(
        partial_kernel, [((NY * NX, 24, 128), BF16)],
        (cond, ctx_cond[None], mod_shift, mod_scale, mod_gate), cost(1 << 20, 1 << 18), 62,
        scratch=[
            pltpu.VMEM((1, D), F32), pltpu.VMEM((1, D), F32), pltpu.VMEM((64, 512), BF16),
            pltpu.VMEM((64, 512), BF16), pltpu.VMEM((64, 512), BF16),
            pltpu.SemaphoreType.DMA((5,)),
        ],
        in_specs=[HBM] * 5,
    )
    part = lax.all_to_all(part, ("y", "tp"), 0, 0, tiled=True)
    part = call(resum_kernel, [((NZ, NX * VECS, 128), BF16)], (part,), cost(1 << 20, 1 << 18), 4)
    mod = lax.all_to_all(part, "z", 0, 0, tiled=True)

    half = call(
        stage_weight_kernel, [((width, D // 2), BF16)], (w_out,),
        cost(1 << 24, 2 << 20), 60, scratch=[pltpu.SemaphoreType.DMA], in_specs=[HBM],
    )
    mine, other = {}, {}
    for s in (1, 3, 2):
        mine[s] = shifted(half, "tp", s)
        other[s] = shifted(mine[s], "dp", 1)

    quarter = HEAD_DIM // 4
    lane = jnp.arange(HEAD_DIM)
    frequency = ROPE_BASE ** (-(lane % quarter).astype(F32) / quarter)
    sign = jnp.where((lane // quarter) % 2 == 0, -1.0, 1.0).astype(F32)
    by_row = lane < HEAD_DIM // 2
    grid_row = (sp * tok - WINDOW) // GRID_W + jnp.arange(24, dtype=jnp.int32)
    row_angle = grid_row.astype(F32)[:, None] * frequency
    col_angle = jnp.arange(GRID_W, dtype=F32)[:, None] * frequency
    row_cos = jnp.where(by_row, jnp.cos(row_angle), 0.0)
    row_sin = jnp.where(by_row, jnp.sin(row_angle) * sign, 0.0)
    col_cos = jnp.where(by_row, 0.0, jnp.cos(col_angle))
    col_sin = jnp.where(by_row, 0.0, jnp.sin(col_angle) * sign)

    rows = tok + 2 * WINDOW
    gain, qgain, kgain = norm_gain[None], q_gain[None], k_gain[None]
    n_ctx = context.shape[1]
    edge = ((WINDOW, 2 * HEAD_DIM), BF16)
    ctx_kv, vec, first_kv, last_kv = call(
        context_kernel,
        [((peers, n_ctx, 2 * HEAD_DIM), BF16), ((8, D), F32), edge, edge],
        (
            mod, context[0], w_key, w_value, gain, kgain,
            row_cos, row_sin, col_cos, col_sin, lat,
        ),
        cost(2 * (n_ctx + 2 * WINDOW) * D * 256, D * 512), 63,
        scratch=[
            pltpu.VMEM((2 * WINDOW, D), BF16), pltpu.VMEM((2 * WINDOW + n_ctx, D), BF16),
            pltpu.SemaphoreType.DMA((2,)),
        ],
        in_specs=[VMEM] * 10 + [HBM],
    )
    up = [(i, i + 1) for i in range(peers - 1)]
    before = lax.ppermute(last_kv, SP, up)
    after = lax.ppermute(first_kv, SP, [(j, i) for i, j in up])
    ctx_all = lax.all_to_all(ctx_kv, SP, 0, 0, tiled=True).reshape(-1, 2 * HEAD_DIM)

    packed_shape = (tok // WINDOW + 1, 4 * WINDOW, 2 * HEAD_DIM)
    packed, own = call(
        qkv_kernel, [(packed_shape, BF16), ((sub, D), BF16)],
        (
            lat, w_query, w_key, w_value, before, after, vec, qgain, kgain,
            row_cos, row_sin, col_cos, col_sin,
        ),
        cost(2 * tok * D * 768 + 16 * tok * 384 * HEAD_DIM, tok * D * 2 + D * 768 * 2), 60,
        scratch=[
            pltpu.VMEM(packed_shape, BF16),
            pltpu.VMEM((tok, D), BF16), pltpu.VMEM((D, width), BF16),
            pltpu.VMEM((D, 2 * HEAD_DIM), BF16),
            pltpu.VMEM((rows, HEAD_DIM), BF16), pltpu.VMEM((rows, HEAD_DIM), BF16),
            pltpu.VMEM((256, D), BF16), pltpu.VMEM((256, D), BF16),
            pltpu.VMEM((4 * WINDOW, 128), F32),
            pltpu.SemaphoreType.DMA((tok // 256 + 4 + packed_shape[0],)),
        ],
        in_specs=[HBM] * 4 + [VMEM] * 9,
        out_specs=[HBM, HBM],
    )

    arrived = {}
    for shifts in ((2,), (1, 3), (0,)):
        pieces = call(
            lambda *refs, shifts=shifts: attend_kernel(shifts, *refs),
            [((sub, width), BF16)] * len(shifts), (packed, ctx_all, sinks[None]),
            cost(16 * len(shifts) * sub * 768 * HEAD_DIM, 2 << 20, 4 * len(shifts) * sub * 768), 8,
            in_specs=[VMEM] * 2 + [SMEM],
        )
        for s, piece in zip(shifts, pieces if len(shifts) > 1 else [pieces]):
            if s == 0:
                arrived[s] = piece
            else:
                arrived[s] = shifted(piece, "tp", s)

    result = call(
        project_kernel, [((sub, D), BF16)],
        (
            vec, arrived[0], arrived[1], arrived[2], arrived[3], w_out,
            mine[1], mine[2], mine[3], other[1], other[2], other[3], own,
        ),
        cost(2 * sub * D * D, D * D * 2), 24,
        scratch=[
            *[pltpu.VMEM((width, D // 2), BF16)] * 3,
            pltpu.VMEM((4, sub, 512), BF16), pltpu.SemaphoreType.DMA((7,)),
        ],
        in_specs=[VMEM] * 6 + [HBM] * 3 + [VMEM] * 4,
        out_specs=HBM,
    )
    return result[None]


def solution(mesh):
    grid = Mesh(mesh.devices.reshape(NZ, NY, NX, 2), ("z", "y", "tp", "dp"))
    in_specs = (
        P("dp", SP, None),
        P("dp", SP, None),
        P("dp", None),
        P(),
        P(),
        P(SP, "tp"),
        P(SP, "tp"),
        P(SP, "tp"),
        P(None, "tp"),
        P(None, "tp"),
        P(None, "tp"),
        P("tp", None),
        P(),
        P(),
        P("tp"),
    )
    out_specs = P("dp", ("z", "y", "tp"), None)

    return jax.shard_map(
        per_device, mesh=grid, in_specs=in_specs, out_specs=out_specs, check_vma=False
    )
```

```python
import math

import jax
import jax.numpy as jnp
from jax import lax
from jax.experimental import pallas as pl
from jax.experimental.pallas import tpu as pltpu
from jax.sharding import Mesh, PartitionSpec as P


HEAD_DIM = 128
WINDOW = 128
GRID_W = 64
NORM_EPSILON = 1e-06
ROPE_BASE = 10000.0
D = 2048
VECS = 20
NZ, NY, NX = 8, 4, 4
SP = ("z", "y")

F32 = jnp.float32
BF16 = jnp.bfloat16
QUERY_SCALE = HEAD_DIM ** (-0.5) * math.log2(math.e)


def sp_index():
    return lax.axis_index("z") * NY + lax.axis_index("y")


def params(vmem_mib):
    return pltpu.CompilerParams(vmem_limit_bytes=vmem_mib * 1024 * 1024)


def cost(flops, nbytes, trans=0):
    return pl.CostEstimate(flops=flops, bytes_accessed=nbytes, transcendentals=trans)


def partial_kernel(cond_in, ctx_in, shift_in, scale_in, gate_in, out_ref,
                   cond_ref, ctx_ref, shift_ref, scale_ref, gate_ref, sems):
    moves = [
        pltpu.make_async_copy(source, to, sems.at[i])
        for i, (source, to) in enumerate(
            (
                (cond_in, cond_ref), (ctx_in, ctx_ref), (shift_in, shift_ref),
                (scale_in, scale_ref), (gate_in, gate_ref),
            )
        )
    ]
    for move in moves:
        move.start()
    for move in moves:
        move.wait()
    sp = sp_index()
    start = pl.multiple_of((sp // 2) * 128, 128)
    row = lax.broadcasted_iota(jnp.int32, (8, 128), 0)
    lane = lax.broadcasted_iota(jnp.int32, (8, 128), 1)
    rows = jnp.where(
        row == 0,
        cond_ref[:, pl.ds(start, 128)],
        jnp.where(row == 1, ctx_ref[:, pl.ds(start, 128)], 0.0),
    )
    active = rows / (1.0 + jnp.exp(-rows))
    active = jnp.where((lane // 64) == (sp % 2), active, 0.0).astype(BF16)

    def times(ref):
        matrix = ref[...]
        return jnp.dot(
            active, jnp.concatenate([matrix, matrix], axis=0), preferred_element_type=F32
        )

    shifts, scales, gates = times(shift_ref), times(scale_ref), times(gate_ref)
    pieces = []
    for values, at in ((shifts, 0), (scales, 0), (shifts, 1), (scales, 1), (gates, 0)):
        for i in range(4):
            pieces.append(values[at : at + 1, i * 128 : (i + 1) * 128])
    pieces.append(jnp.zeros((4, 128), F32))
    stacked = jnp.concatenate(pieces, axis=0).astype(BF16)
    out_ref[...] = jnp.broadcast_to(stacked[None], out_ref.shape)


def resum_kernel(in_ref, out_ref):
    pieces = []
    for t in range(NX):
        rows = None
        for y in range(NY):
            part = in_ref[y * NX + t].astype(F32)
            rows = part if rows is None else rows + part
        pieces.append(rows[:VECS])
    total = jnp.concatenate(pieces, axis=0).astype(BF16)
    out_ref[...] = jnp.broadcast_to(total[None], out_ref.shape)


def vectors_of(mod_ref):
    rows = None
    for z in range(NZ):
        part = mod_ref[z].astype(F32)
        rows = part if rows is None else rows + part
    found = []
    for v in range(5):
        pieces = []
        for t in range(NX):
            for i in range(4):
                at = t * VECS + v * 4 + i
                pieces.append(rows[at : at + 1, :])
        found.append(jnp.concatenate(pieces, axis=1))
    return found


def normed(values):
    values = values.astype(F32)
    return values * lax.rsqrt(jnp.mean(values * values, axis=-1, keepdims=True) + NORM_EPSILON)


def head_norm(v, gain):
    return v * lax.rsqrt(jnp.mean(v * v, axis=-1, keepdims=True) + NORM_EPSILON) * gain


def rotated(v, cosine, sine):
    lane = lax.broadcasted_iota(jnp.int32, v.shape, 1)
    odd = ((lane // 32) % 2) == 1
    swapped = jnp.where(odd, pltpu.roll(v, 32, 1), pltpu.roll(v, 96, 1))
    return v * cosine + swapped * sine


def stage_weight_kernel(w_in, half_ref, sem):
    start = pl.multiple_of(lax.axis_index("dp") * (D // 2), D // 2)
    move = pltpu.make_async_copy(w_in.at[:, pl.ds(start, D // 2)], half_ref, sem)
    move.start()
    move.wait()


def rotation(refs, groups):
    row_cos, row_sin, col_cos, col_sin = refs
    cosines = [row_cos[pl.ds(g, 1), :] + col_cos[...] for g in groups]
    sines = [row_sin[pl.ds(g, 1), :] + col_sin[...] for g in groups]
    return jnp.concatenate(cosines), jnp.concatenate(sines)


def prepare_kernel(lat_in, ctx_in, wk_in, wv_in, rows_ref, wkv_ref, edge_ref, ctx_ref, sems):
    tok = lat_in.shape[0]
    moves = [
        pltpu.make_async_copy(source, to, sems.at[i])
        for i, (source, to) in enumerate(
            (
                (lat_in.at[:WINDOW, :], edge_ref.at[:WINDOW]),
                (lat_in.at[tok - WINDOW :, :], edge_ref.at[WINDOW:]),
                (ctx_in, ctx_ref),
                (wk_in, wkv_ref.at[:, :HEAD_DIM]),
                (wv_in, wkv_ref.at[:, HEAD_DIM:]),
            )
        )
    ]
    for move in moves:
        move.start()
    for move in moves[:3]:
        move.wait()
    step = 64

    def body(i, carry):
        at = pl.ds(pl.multiple_of(i * step, step), step)
        rows_ref[at, :] = normed(edge_ref[at, :]).astype(BF16)
        return carry

    lax.fori_loop(0, 2 * WINDOW // step, body, 0)
    rows_ref[2 * WINDOW :, :] = normed(ctx_ref[...]).astype(BF16)
    for move in moves[3:]:
        move.wait()


def context_kernel(
    mod_ref, rows_in, wkv_ref, gain_ref, kgain_ref, rcos_ref, rsin_ref, ccos_ref, csin_ref,
    kv_ref, vec_ref, first_ref, last_ref, rows_ref,
):
    shift_lat, scale_lat, shift_ctx, scale_ctx, gate = vectors_of(mod_ref)
    gain = gain_ref[...]
    vec_ref[0:1, :] = gain * (1.0 + scale_lat)
    vec_ref[1:2, :] = shift_lat
    vec_ref[2:3, :] = gate
    rows_ref[2 * WINDOW :, :] = (
        rows_in[2 * WINDOW :, :].astype(F32) * (gain * (1.0 + scale_ctx)) + shift_ctx
    ).astype(BF16)
    step = 64

    def body(i, carry):
        at = pl.ds(pl.multiple_of(i * step, step), step)
        rows = rows_in[at, :].astype(F32) * vec_ref[0:1, :] + vec_ref[1:2, :]
        rows_ref[at, :] = rows.astype(BF16)
        return carry

    lax.fori_loop(0, 2 * WINDOW // step, body, 0)
    both = jnp.dot(rows_ref[...], wkv_ref[...], preferred_element_type=F32)
    keys = head_norm(both[:, :HEAD_DIM], kgain_ref[...])
    values = both[:, HEAD_DIM:].astype(BF16)
    refs = (rcos_ref, rsin_ref, ccos_ref, csin_ref)
    final = 1024 // GRID_W
    for ref, base, groups in ((first_ref, 0, (2, 3)), (last_ref, WINDOW, (final, final + 1))):
        at = slice(base, base + WINDOW)
        ref[:, :HEAD_DIM] = rotated(keys[at], *rotation(refs, groups)).astype(BF16)
        ref[:, HEAD_DIM:] = values[at]
    both = jnp.concatenate([keys[2 * WINDOW :].astype(BF16), values[2 * WINDOW :]], axis=1)
    kv_ref[...] = jnp.broadcast_to(both[None], kv_ref.shape)


def qkv_kernel(
    lat_in, wq_in, wkv_in, before_ref, after_ref,
    vec_ref, qgain_ref, kgain_ref, rcos_ref, rsin_ref, ccos_ref, csin_ref,
    packed_out, own_ref, out_ref, lat_ref, wq_ref, wkv_ref, k_ref, v_ref, even_ref, odd_ref,
    sum_ref, sems,
):
    step = 256
    tok = lat_in.shape[0]
    steps = tok // step
    qgain = qgain_ref[...] * QUERY_SCALE
    kgain = kgain_ref[...]

    def at(i, size=step):
        return pl.ds(pl.multiple_of(i * step, step), size)

    sources = [(lat_in.at[at(i), :], lat_ref.at[at(i), :]) for i in range(steps)]
    sources += [
        (wkv_in, wkv_ref), (wq_in, wq_ref),
    ]
    moves = [
        pltpu.make_async_copy(source, to, sems.at[i]) for i, (source, to) in enumerate(sources)
    ]
    for i in (0, steps, steps + 1, *range(1, steps)):
        moves[i].start()
    for ref, edge in ((k_ref, slice(0, HEAD_DIM)), (v_ref, slice(HEAD_DIM, 2 * HEAD_DIM))):
        ref[:WINDOW, :] = before_ref[:, edge]
        ref[tok + WINDOW :, :] = after_ref[:, edge]
    refs = (rcos_ref, rsin_ref, ccos_ref, csin_ref)

    def fill(i, to):
        values = lat_ref[at(i), :].astype(F32)
        inverse = lax.rsqrt(jnp.mean(values * values, axis=-1, keepdims=True) + NORM_EPSILON)
        to[...] = (values * inverse * vec_ref[0:1, :] + vec_ref[1:2, :]).astype(BF16)

    def keys_of(rows_ref, cosine, sine):
        both = jnp.dot(rows_ref[...], wkv_ref[...], preferred_element_type=F32)
        keys = rotated(head_norm(both[:, :HEAD_DIM], kgain), cosine, sine).astype(BF16)
        return keys, both[:, HEAD_DIM:].astype(BF16)

    def project(i, rows_ref):
        to = pl.ds(pl.multiple_of(i * step + WINDOW, WINDOW), step)
        first = 2 + i * (step // GRID_W)
        cosine, sine = rotation(refs, [first + g for g in range(step // GRID_W)])
        queries = jnp.dot(rows_ref[...], wq_ref[...], preferred_element_type=F32)
        k_ref[to, :], v_ref[to, :] = keys_of(rows_ref, cosine, sine)
        for h in range(4):
            head = slice(h * HEAD_DIM, (h + 1) * HEAD_DIM)
            turned = rotated(head_norm(queries[:, head], qgain), cosine, sine).astype(BF16)
            for half in range(2):
                out_ref[i * 2 + half, h * WINDOW : (h + 1) * WINDOW, :HEAD_DIM] = turned[
                    half * WINDOW : (half + 1) * WINDOW
                ]

    moves[0].wait()
    fill(0, even_ref)
    for i in range(steps, steps + 2):
        moves[i].wait()

    def wait_rows(i):
        pltpu.make_async_copy(lat_in.at[at(0), :], lat_ref.at[at(i), :], sems.at[i]).wait()

    def body(j, carry):
        wait_rows(2 * j + 1)

        @pl.when(j == 0)
        def _():
            wait_rows(2)

        fill(2 * j + 1, odd_ref)
        project(2 * j, even_ref)
        fill(jnp.minimum(2 * j + 2, steps - 1), even_ref)
        project(2 * j + 1, odd_ref)
        return carry

    lax.fori_loop(0, steps // 2, body, 0)
    own_move = pltpu.make_async_copy(
        lat_ref.at[at(lax.axis_index("tp"), own_ref.shape[0]), :], own_ref, sems.at[steps + 3]
    )
    own_move.start()

    def block_move(block):
        return pltpu.make_async_copy(
            out_ref.at[block], packed_out.at[block], sems.at[steps + 4 + block]
        )

    local_pass(out_ref, k_ref, v_ref, sum_ref, block_move)
    for block in range(packed_out.shape[0]):
        block_move(block).wait()
    own_move.wait()


def contract_last(a, b):
    return lax.dot_general(a, b, (((1,), (1,)), ((), ())), preferred_element_type=F32)


def lanes_summed(values):
    parts = [values[:, i : i + 128] for i in range(0, values.shape[1], 128)]
    while len(parts) > 1:
        parts = [sum(parts[i : i + 2]) for i in range(0, len(parts), 2)]
    return parts[0]


def local_pass(out_ref, k_ref, v_ref, sum_ref, block_move):
    sp = sp_index()
    blocks = out_ref.shape[0] - 1
    query_at = lax.broadcasted_iota(jnp.int32, (4 * WINDOW, WINDOW), 0) % WINDOW
    key_at = lax.broadcasted_iota(jnp.int32, (4 * WINDOW, WINDOW), 1)
    in_before, in_after = key_at >= query_at, key_at <= query_at

    sum_ref[...] = jnp.zeros(sum_ref.shape, F32)

    def one(block):
        near = pl.ds(pl.multiple_of(block * WINDOW, WINDOW), 3 * WINDOW)
        no_before = (block == 0) & (sp == 0)
        no_after = (block == blocks - 1) & (sp == NZ * NY - 1)
        local = jnp.exp2(contract_last(out_ref[block, :, :HEAD_DIM], k_ref[near, :]))
        local = jnp.concatenate(
            [
                jnp.where(in_before & jnp.logical_not(no_before), local[:, :WINDOW], 0.0),
                local[:, WINDOW : 2 * WINDOW],
                jnp.where(in_after & jnp.logical_not(no_after), local[:, 2 * WINDOW :], 0.0),
            ],
            axis=1,
        )
        total = jnp.sum(lanes_summed(local), axis=-1, keepdims=True)
        mixed = jnp.dot(local.astype(BF16), v_ref[near, :], preferred_element_type=F32)
        return total, mixed.astype(BF16)

    def body(i, carry):
        pair = (2 * i, 2 * i + 1)
        found = [one(block) for block in pair]
        sums = sum_ref[...]
        for block, (total, mixed) in zip(pair, found):
            sums = jnp.where(key_at == block, total, sums)
            out_ref[block, :, HEAD_DIM:] = mixed
        sum_ref[...] = sums
        for block in pair:
            block_move(block).start()
        return carry

    lax.fori_loop(0, blocks // 2, body, 0)
    high = sum_ref[...].astype(BF16)
    out_ref[blocks, :, :HEAD_DIM] = high
    out_ref[blocks, :, HEAD_DIM:] = (sum_ref[...] - high.astype(F32)).astype(BF16)
    block_move(blocks).start()


def attend_kernel(shifts, packed_ref, ctx_ref, sink_ref, *out_refs):
    head = HEAD_DIM
    last = packed_ref.shape[0] - 1
    tp = lax.axis_index("tp")
    sink = jnp.concatenate(
        [jnp.exp(jnp.full((WINDOW, 1), sink_ref[0, h], F32)) for h in range(4)], axis=0
    )
    lane = lax.broadcasted_iota(jnp.int32, (4 * WINDOW, 128), 1)
    sums = packed_ref[last, :, :head].astype(F32) + packed_ref[last, :, head:].astype(F32)

    for by, out_ref in zip(shifts, out_refs):
        quarter = (tp + by) % NX

        def body(i, carry, quarter=quarter, out_ref=out_ref):
            block = quarter * 2 + i
            base = pl.ds(pl.multiple_of(i * WINDOW, WINDOW), WINDOW)
            far = jnp.exp2(contract_last(packed_ref[block, :, :head], ctx_ref[:, :head]))
            near_sum = jnp.where(lane == block, sums, 0.0)
            total = jnp.sum(lanes_summed(far) + near_sum, axis=-1, keepdims=True) + sink
            mixed = packed_ref[block, :, head:].astype(F32) + jnp.dot(
                far.astype(BF16), ctx_ref[:, head:], preferred_element_type=F32
            )
            mixed = (mixed * (1.0 / total)).astype(BF16)
            for h in range(4):
                out_ref[base, h * head : (h + 1) * head] = mixed[h * WINDOW : (h + 1) * WINDOW]
            return carry

        lax.fori_loop(0, 2, body, 0)


def early_kernel(a0_ref, a2_ref, w0_ref, m2_in, o2_ref, sum_ref, m2_ref, sem):
    dp = lax.axis_index("dp")
    col = 512
    move = pltpu.make_async_copy(m2_in, m2_ref, sem)
    move.start()
    for part, weight in enumerate((o2_ref, m2_ref)):
        half = 1 - dp if part == 0 else dp
        if part == 1:
            move.wait()

        def body(j, carry, weight=weight, half=half):
            wide = pl.ds(pl.multiple_of(half * (D // 2) + j * col, col), col)
            sub = pl.ds(pl.multiple_of(j * col, col), col)
            sum_ref[:, wide] = jnp.dot(
                a0_ref[...], w0_ref[:, wide], preferred_element_type=F32
            ) + jnp.dot(a2_ref[...], weight[:, sub], preferred_element_type=F32)
            return carry

        lax.fori_loop(0, 2, body, 0)


def project_kernel(
    vec_ref, sum_ref, a1_ref, a3_ref, m1_in, m3_in, o1_ref, o3_ref, lat_ref, out_ref,
    m1_ref, m3_ref, done_ref, sems,
):
    dp = lax.axis_index("dp")
    col = 512
    moves = [
        pltpu.make_async_copy(source, to, sems.at[4 + i])
        for i, (source, to) in enumerate(((m1_in, m1_ref), (m3_in, m3_ref)))
    ]
    for move in moves:
        move.start()

    def copy(slot, column):
        return pltpu.make_async_copy(
            done_ref.at[slot], out_ref.at[:, pl.ds(column, col)], sems.at[slot]
        )

    for part, weights in enumerate(((o1_ref, o3_ref), (m1_ref, m3_ref))):
        half = 1 - dp if part == 0 else dp
        if part == 1:
            for move in moves:
                move.wait()

        def body(j, carry, part=part, weights=weights, half=half):
            column = pl.multiple_of(half * (D // 2) + j * col, col)
            wide = pl.ds(column, col)
            sub = pl.ds(pl.multiple_of(j * col, col), col)
            mixed = sum_ref[:, wide]
            for a, w in zip((a1_ref, a3_ref), weights):
                mixed = mixed + jnp.dot(a[...], w[:, sub], preferred_element_type=F32)
            slot = part * 2 + j
            result = lat_ref[:, wide].astype(F32) + vec_ref[2:3, wide] * mixed
            done_ref[slot] = result.astype(BF16)
            copy(slot, column).start()
            return carry

        lax.fori_loop(0, 2, body, 0)
    for slot in range(4):
        copy(slot, 0).wait()


def shifted(array, axis, by):
    peers = lax.axis_size(axis)
    return lax.ppermute(array, axis, [(i, (i + by) % peers) for i in range(peers)])


VMEM = pl.BlockSpec(memory_space=pltpu.VMEM)
SMEM = pl.BlockSpec(memory_space=pltpu.SMEM)
HBM = pl.BlockSpec(memory_space=pltpu.HBM)


def call(kernel, outs, args, estimate, limit, scratch=(), in_specs=None, out_specs=None):
    shapes = [jax.ShapeDtypeStruct(s, t) for s, t in outs]
    single = len(shapes) == 1
    return pl.pallas_call(
        kernel,
        in_specs=in_specs or [VMEM] * len(args),
        out_specs=out_specs or (VMEM if single else [VMEM] * len(shapes)),
        out_shape=shapes[0] if single else shapes,
        scratch_shapes=list(scratch),
        compiler_params=params(limit),
        cost_estimate=estimate,
    )(*args)


def per_device(
    latent, context, cond, ctx_cond, norm_gain, mod_shift, mod_scale, mod_gate,
    w_query, w_key, w_value, w_out, q_gain, k_gain, sinks,
):
    lat = latent[0]
    tok = lat.shape[0]
    sub = tok // NX
    sp = sp_index()
    width = 4 * HEAD_DIM

    peers = NZ * NY
    part = call(
        partial_kernel, [((NY * NX, 24, 128), BF16)],
        (cond, ctx_cond[None], mod_shift, mod_scale, mod_gate), cost(1 << 20, 1 << 18), 62,
        scratch=[
            pltpu.VMEM((1, D), F32), pltpu.VMEM((1, D), F32), pltpu.VMEM((64, 512), BF16),
            pltpu.VMEM((64, 512), BF16), pltpu.VMEM((64, 512), BF16),
            pltpu.SemaphoreType.DMA((5,)),
        ],
        in_specs=[HBM] * 5,
    )
    part = lax.all_to_all(part, ("y", "tp"), 0, 0, tiled=True)
    part = call(resum_kernel, [((NZ, NX * VECS, 128), BF16)], (part,), cost(1 << 20, 1 << 18), 4)
    mod = lax.all_to_all(part, "z", 0, 0, tiled=True)

    half = call(
        stage_weight_kernel, [((width, D // 2), BF16)], (w_out,),
        cost(1 << 24, 2 << 20), 60, scratch=[pltpu.SemaphoreType.DMA], in_specs=[HBM],
    )
    mine, other = {}, {}
    for s in (1, 3, 2):
        mine[s] = shifted(half, "tp", s)
        other[s] = shifted(mine[s], "dp", 1)

    quarter = HEAD_DIM // 4
    lane = jnp.arange(HEAD_DIM)
    frequency = ROPE_BASE ** (-(lane % quarter).astype(F32) / quarter)
    sign = jnp.where((lane // quarter) % 2 == 0, -1.0, 1.0).astype(F32)
    by_row = lane < HEAD_DIM // 2
    grid_row = (sp * tok - WINDOW) // GRID_W + jnp.arange(24, dtype=jnp.int32)
    row_angle = grid_row.astype(F32)[:, None] * frequency
    col_angle = jnp.arange(GRID_W, dtype=F32)[:, None] * frequency
    row_cos = jnp.where(by_row, jnp.cos(row_angle), 0.0)
    row_sin = jnp.where(by_row, jnp.sin(row_angle) * sign, 0.0)
    col_cos = jnp.where(by_row, 0.0, jnp.cos(col_angle))
    col_sin = jnp.where(by_row, 0.0, jnp.sin(col_angle) * sign)

    rows = tok + 2 * WINDOW
    gain, qgain, kgain = norm_gain[None], q_gain[None], k_gain[None]
    n_ctx = context.shape[1]
    prepared, w_kv = call(
        prepare_kernel,
        [((2 * WINDOW + n_ctx, D), BF16), ((D, 2 * HEAD_DIM), BF16)],
        (lat, context[0], w_key, w_value), cost(1 << 24, 4 << 20), 60,
        scratch=[
            pltpu.VMEM((2 * WINDOW, D), BF16), pltpu.VMEM((n_ctx, D), BF16),
            pltpu.SemaphoreType.DMA((5,)),
        ],
        in_specs=[HBM] * 4,
    )
    edge = ((WINDOW, 2 * HEAD_DIM), BF16)
    ctx_kv, vec, first_kv, last_kv = call(
        context_kernel,
        [((peers, n_ctx, 2 * HEAD_DIM), BF16), ((8, D), F32), edge, edge],
        (mod, prepared, w_kv, gain, kgain, row_cos, row_sin, col_cos, col_sin),
        cost(2 * (n_ctx + 2 * WINDOW) * D * 256, D * 512), 63,
        scratch=[pltpu.VMEM((2 * WINDOW + n_ctx, D), BF16)],
    )
    up = [(i, i + 1) for i in range(peers - 1)]
    before = lax.ppermute(last_kv, SP, up)
    after = lax.ppermute(first_kv, SP, [(j, i) for i, j in up])
    ctx_all = lax.all_to_all(ctx_kv, SP, 0, 0, tiled=True).reshape(-1, 2 * HEAD_DIM)

    packed_shape = (tok // WINDOW + 1, 4 * WINDOW, 2 * HEAD_DIM)
    packed, own = call(
        qkv_kernel, [(packed_shape, BF16), ((sub, D), BF16)],
        (
            lat, w_query, w_kv, before, after, vec, qgain, kgain,
            row_cos, row_sin, col_cos, col_sin,
        ),
        cost(2 * tok * D * 768 + 16 * tok * 384 * HEAD_DIM, tok * D * 2 + D * 768 * 2), 60,
        scratch=[
            pltpu.VMEM(packed_shape, BF16),
            pltpu.VMEM((tok, D), BF16), pltpu.VMEM((D, width), BF16),
            pltpu.VMEM((D, 2 * HEAD_DIM), BF16),
            pltpu.VMEM((rows, HEAD_DIM), BF16), pltpu.VMEM((rows, HEAD_DIM), BF16),
            pltpu.VMEM((256, D), BF16), pltpu.VMEM((256, D), BF16),
            pltpu.VMEM((4 * WINDOW, 128), F32),
            pltpu.SemaphoreType.DMA((tok // 256 + 4 + packed_shape[0],)),
        ],
        in_specs=[HBM] * 3 + [VMEM] * 9,
        out_specs=[HBM, HBM],
    )

    arrived = {}
    for shifts in ((2,), (1, 3), (0,)):
        pieces = call(
            lambda *refs, shifts=shifts: attend_kernel(shifts, *refs),
            [((sub, width), BF16)] * len(shifts), (packed, ctx_all, sinks[None]),
            cost(16 * len(shifts) * sub * 768 * HEAD_DIM, 2 << 20, 4 * len(shifts) * sub * 768), 8,
            in_specs=[VMEM] * 2 + [SMEM],
        )
        for s, piece in zip(shifts, pieces if len(shifts) > 1 else [pieces]):
            if s == 0:
                arrived[s] = piece
            else:
                arrived[s] = shifted(piece, "tp", s)

    matrix = pltpu.VMEM((width, D // 2), BF16)
    early = call(
        early_kernel, [((sub, D), F32)],
        (arrived[0], arrived[2], w_out, mine[2], other[2]),
        cost(sub * D * D, D * D), 24,
        scratch=[matrix, pltpu.SemaphoreType.DMA], in_specs=[VMEM] * 3 + [HBM, VMEM],
    )
    result = call(
        project_kernel, [((sub, D), BF16)],
        (
            vec, early, arrived[1], arrived[3], mine[1], mine[3], other[1], other[3], own,
        ),
        cost(sub * D * D, D * D), 24,
        scratch=[
            matrix, matrix, pltpu.VMEM((4, sub, 512), BF16), pltpu.SemaphoreType.DMA((6,)),
        ],
        in_specs=[VMEM] * 4 + [HBM] * 2 + [VMEM] * 3,
        out_specs=HBM,
    )
    return result[None]


def solution(mesh):
    grid = Mesh(mesh.devices.reshape(NZ, NY, NX, 2), ("z", "y", "tp", "dp"))
    in_specs = (
        P("dp", SP, None),
        P("dp", SP, None),
        P("dp", None),
        P(),
        P(),
        P(SP, "tp"),
        P(SP, "tp"),
        P(SP, "tp"),
        P(None, "tp"),
        P(None, "tp"),
        P(None, "tp"),
        P("tp", None),
        P(),
        P(),
        P("tp"),
    )
    out_specs = P("dp", ("z", "y", "tp"), None)

    return jax.shard_map(
        per_device, mesh=grid, in_specs=in_specs, out_specs=out_specs, check_vma=False
    )
```

```python
import math

import jax
import jax.numpy as jnp
from jax import lax
from jax.experimental import pallas as pl
from jax.experimental.pallas import tpu as pltpu
from jax.sharding import Mesh, PartitionSpec as P


HEAD_DIM = 128
WINDOW = 128
GRID_W = 64
NORM_EPSILON = 1e-06
ROPE_BASE = 10000.0
D = 2048
VECS = 20
NZ, NY, NX = 8, 4, 4
SP = ("z", "y")

F32 = jnp.float32
BF16 = jnp.bfloat16
QUERY_SCALE = HEAD_DIM ** (-0.5) * math.log2(math.e)


def sp_index():
    return lax.axis_index("z") * NY + lax.axis_index("y")


def params(vmem_mib):
    return pltpu.CompilerParams(vmem_limit_bytes=vmem_mib * 1024 * 1024)


def cost(flops, nbytes, trans=0):
    return pl.CostEstimate(flops=flops, bytes_accessed=nbytes, transcendentals=trans)


def partial_kernel(cond_in, ctx_in, shift_in, scale_in, gate_in, out_ref,
                   cond_ref, ctx_ref, shift_ref, scale_ref, gate_ref, sems):
    moves = [
        pltpu.make_async_copy(source, to, sems.at[i])
        for i, (source, to) in enumerate(
            (
                (cond_in, cond_ref), (ctx_in, ctx_ref), (shift_in, shift_ref),
                (scale_in, scale_ref), (gate_in, gate_ref),
            )
        )
    ]
    for move in moves:
        move.start()
    for move in moves:
        move.wait()
    sp = sp_index()
    start = pl.multiple_of((sp // 2) * 128, 128)
    row = lax.broadcasted_iota(jnp.int32, (8, 128), 0)
    lane = lax.broadcasted_iota(jnp.int32, (8, 128), 1)
    rows = jnp.where(
        row == 0,
        cond_ref[:, pl.ds(start, 128)],
        jnp.where(row == 1, ctx_ref[:, pl.ds(start, 128)], 0.0),
    )
    active = rows / (1.0 + jnp.exp(-rows))
    active = jnp.where((lane // 64) == (sp % 2), active, 0.0).astype(BF16)

    def times(ref):
        matrix = ref[...]
        return jnp.dot(
            active, jnp.concatenate([matrix, matrix], axis=0), preferred_element_type=F32
        )

    shifts, scales, gates = times(shift_ref), times(scale_ref), times(gate_ref)
    pieces = []
    for values, at in ((shifts, 0), (scales, 0), (shifts, 1), (scales, 1), (gates, 0)):
        for i in range(4):
            pieces.append(values[at : at + 1, i * 128 : (i + 1) * 128])
    pieces.append(jnp.zeros((4, 128), F32))
    stacked = jnp.concatenate(pieces, axis=0).astype(BF16)
    out_ref[...] = jnp.broadcast_to(stacked[None], out_ref.shape)


def resum_kernel(in_ref, out_ref):
    pieces = []
    for t in range(NX):
        rows = None
        for y in range(NY):
            part = in_ref[y * NX + t].astype(F32)
            rows = part if rows is None else rows + part
        pieces.append(rows[:VECS])
    total = jnp.concatenate(pieces, axis=0).astype(BF16)
    out_ref[...] = jnp.broadcast_to(total[None], out_ref.shape)


def vectors_of(mod_ref):
    rows = None
    for z in range(NZ):
        part = mod_ref[z].astype(F32)
        rows = part if rows is None else rows + part
    found = []
    for v in range(5):
        pieces = []
        for t in range(NX):
            for i in range(4):
                at = t * VECS + v * 4 + i
                pieces.append(rows[at : at + 1, :])
        found.append(jnp.concatenate(pieces, axis=1))
    return found


def normed(values):
    values = values.astype(F32)
    return values * lax.rsqrt(jnp.mean(values * values, axis=-1, keepdims=True) + NORM_EPSILON)


def head_norm(v, gain):
    return v * lax.rsqrt(jnp.mean(v * v, axis=-1, keepdims=True) + NORM_EPSILON) * gain


def rotated(v, cosine, sine):
    lane = lax.broadcasted_iota(jnp.int32, v.shape, 1)
    odd = ((lane // 32) % 2) == 1
    swapped = jnp.where(odd, pltpu.roll(v, 32, 1), pltpu.roll(v, 96, 1))
    return v * cosine + swapped * sine


def stage_weight_kernel(w_in, half_ref, sem):
    start = pl.multiple_of(lax.axis_index("dp") * (D // 2), D // 2)
    move = pltpu.make_async_copy(w_in.at[:, pl.ds(start, D // 2)], half_ref, sem)
    move.start()
    move.wait()


def rotation(refs, groups):
    row_cos, row_sin, col_cos, col_sin = refs
    cosines = [row_cos[pl.ds(g, 1), :] + col_cos[...] for g in groups]
    sines = [row_sin[pl.ds(g, 1), :] + col_sin[...] for g in groups]
    return jnp.concatenate(cosines), jnp.concatenate(sines)


def fill_tables(first_row, cos_ref, sin_ref, rows):
    shape = cos_ref.shape
    quarter = HEAD_DIM // 4
    at = lax.broadcasted_iota(jnp.int32, shape, 0) + first_row
    lane = lax.broadcasted_iota(jnp.int32, shape, 1)
    frequency = jnp.exp((lane % quarter).astype(F32) * (-math.log(ROPE_BASE) / quarter))
    angle = at.astype(F32) * frequency
    wanted = (lane < HEAD_DIM // 2) == rows
    sign = jnp.where((lane // quarter) % 2 == 0, -1.0, 1.0)
    cos_ref[...] = jnp.where(wanted, jnp.cos(angle), 0.0)
    sin_ref[...] = jnp.where(wanted, jnp.sin(angle) * sign, 0.0)


def prepare_kernel(
    lat_in, ctx_in, wk_in, wv_in,
    rows_ref, wkv_ref, rcos_ref, rsin_ref, ccos_ref, csin_ref, edge_ref, ctx_ref, sems,
):
    tok = lat_in.shape[0]
    moves = [
        pltpu.make_async_copy(source, to, sems.at[i])
        for i, (source, to) in enumerate(
            (
                (lat_in.at[:WINDOW, :], edge_ref.at[:WINDOW]),
                (lat_in.at[tok - WINDOW :, :], edge_ref.at[WINDOW:]),
                (ctx_in, ctx_ref),
                (wk_in, wkv_ref.at[:, :HEAD_DIM]),
                (wv_in, wkv_ref.at[:, HEAD_DIM:]),
            )
        )
    ]
    for move in moves:
        move.start()
    fill_tables((sp_index() * tok - WINDOW) // GRID_W, rcos_ref, rsin_ref, True)
    fill_tables(0, ccos_ref, csin_ref, False)
    for move in moves[:3]:
        move.wait()
    step = 64

    def body(i, carry):
        at = pl.ds(pl.multiple_of(i * step, step), step)
        rows_ref[at, :] = normed(edge_ref[at, :]).astype(BF16)
        return carry

    lax.fori_loop(0, 2 * WINDOW // step, body, 0)
    rows_ref[2 * WINDOW :, :] = normed(ctx_ref[...]).astype(BF16)
    for move in moves[3:]:
        move.wait()


def context_kernel(
    mod_ref, rows_in, wkv_ref, gain_ref, kgain_ref, rcos_ref, rsin_ref, ccos_ref, csin_ref,
    kv_ref, vec_ref, first_ref, last_ref, rows_ref,
):
    shift_lat, scale_lat, shift_ctx, scale_ctx, gate = vectors_of(mod_ref)
    gain = gain_ref[...]
    vec_ref[0:1, :] = gain * (1.0 + scale_lat)
    vec_ref[1:2, :] = shift_lat
    vec_ref[2:3, :] = gate
    rows_ref[2 * WINDOW :, :] = (
        rows_in[2 * WINDOW :, :].astype(F32) * (gain * (1.0 + scale_ctx)) + shift_ctx
    ).astype(BF16)
    step = 64

    def body(i, carry):
        at = pl.ds(pl.multiple_of(i * step, step), step)
        rows = rows_in[at, :].astype(F32) * vec_ref[0:1, :] + vec_ref[1:2, :]
        rows_ref[at, :] = rows.astype(BF16)
        return carry

    lax.fori_loop(0, 2 * WINDOW // step, body, 0)
    both = jnp.dot(rows_ref[...], wkv_ref[...], preferred_element_type=F32)
    keys = head_norm(both[:, :HEAD_DIM], kgain_ref[...])
    values = both[:, HEAD_DIM:].astype(BF16)
    refs = (rcos_ref, rsin_ref, ccos_ref, csin_ref)
    final = 1024 // GRID_W
    for ref, base, groups in ((first_ref, 0, (2, 3)), (last_ref, WINDOW, (final, final + 1))):
        at = slice(base, base + WINDOW)
        ref[:, :HEAD_DIM] = rotated(keys[at], *rotation(refs, groups)).astype(BF16)
        ref[:, HEAD_DIM:] = values[at]
    both = jnp.concatenate([keys[2 * WINDOW :].astype(BF16), values[2 * WINDOW :]], axis=1)
    kv_ref[...] = jnp.broadcast_to(both[None], kv_ref.shape)


def qkv_kernel(
    lat_in, wq_in, wkv_in, before_ref, after_ref,
    vec_ref, qgain_ref, kgain_ref, rcos_ref, rsin_ref, ccos_ref, csin_ref,
    packed_out, own_ref, out_ref, lat_ref, wq_ref, wkv_ref, k_ref, v_ref, even_ref, odd_ref,
    sum_ref, sems,
):
    step = 256
    tok = lat_in.shape[0]
    steps = tok // step
    qgain = qgain_ref[...] * QUERY_SCALE
    kgain = kgain_ref[...]

    def at(i, size=step):
        return pl.ds(pl.multiple_of(i * step, step), size)

    sources = [(lat_in.at[at(i), :], lat_ref.at[at(i), :]) for i in range(steps)]
    sources += [
        (wkv_in, wkv_ref), (wq_in, wq_ref),
    ]
    moves = [
        pltpu.make_async_copy(source, to, sems.at[i]) for i, (source, to) in enumerate(sources)
    ]
    for i in (0, steps, steps + 1, *range(1, steps)):
        moves[i].start()
    for ref, edge in ((k_ref, slice(0, HEAD_DIM)), (v_ref, slice(HEAD_DIM, 2 * HEAD_DIM))):
        ref[:WINDOW, :] = before_ref[:, edge]
        ref[tok + WINDOW :, :] = after_ref[:, edge]
    refs = (rcos_ref, rsin_ref, ccos_ref, csin_ref)

    def fill(i, to):
        values = lat_ref[at(i), :].astype(F32)
        inverse = lax.rsqrt(jnp.mean(values * values, axis=-1, keepdims=True) + NORM_EPSILON)
        to[...] = (values * inverse * vec_ref[0:1, :] + vec_ref[1:2, :]).astype(BF16)

    def keys_of(rows_ref, cosine, sine):
        both = jnp.dot(rows_ref[...], wkv_ref[...], preferred_element_type=F32)
        keys = rotated(head_norm(both[:, :HEAD_DIM], kgain), cosine, sine).astype(BF16)
        return keys, both[:, HEAD_DIM:].astype(BF16)

    def project(i, rows_ref):
        to = pl.ds(pl.multiple_of(i * step + WINDOW, WINDOW), step)
        first = 2 + i * (step // GRID_W)
        cosine, sine = rotation(refs, [first + g for g in range(step // GRID_W)])
        queries = jnp.dot(rows_ref[...], wq_ref[...], preferred_element_type=F32)
        k_ref[to, :], v_ref[to, :] = keys_of(rows_ref, cosine, sine)
        for h in range(4):
            head = slice(h * HEAD_DIM, (h + 1) * HEAD_DIM)
            turned = rotated(head_norm(queries[:, head], qgain), cosine, sine).astype(BF16)
            for half in range(2):
                out_ref[i * 2 + half, h * WINDOW : (h + 1) * WINDOW, :HEAD_DIM] = turned[
                    half * WINDOW : (half + 1) * WINDOW
                ]

    moves[0].wait()
    fill(0, even_ref)
    for i in range(steps, steps + 2):
        moves[i].wait()

    def wait_rows(i):
        pltpu.make_async_copy(lat_in.at[at(0), :], lat_ref.at[at(i), :], sems.at[i]).wait()

    def body(j, carry):
        wait_rows(2 * j + 1)

        @pl.when(j == 0)
        def _():
            wait_rows(2)

        fill(2 * j + 1, odd_ref)
        project(2 * j, even_ref)
        fill(jnp.minimum(2 * j + 2, steps - 1), even_ref)
        project(2 * j + 1, odd_ref)
        return carry

    lax.fori_loop(0, steps // 2, body, 0)
    own_move = pltpu.make_async_copy(
        lat_ref.at[at(lax.axis_index("tp"), own_ref.shape[0]), :], own_ref, sems.at[steps + 3]
    )
    own_move.start()

    def block_move(block):
        return pltpu.make_async_copy(
            out_ref.at[block], packed_out.at[block], sems.at[steps + 4 + block]
        )

    local_pass(out_ref, k_ref, v_ref, sum_ref, block_move)
    for block in range(packed_out.shape[0]):
        block_move(block).wait()
    own_move.wait()


def contract_last(a, b):
    return lax.dot_general(a, b, (((1,), (1,)), ((), ())), preferred_element_type=F32)


def lanes_summed(values):
    parts = [values[:, i : i + 128] for i in range(0, values.shape[1], 128)]
    while len(parts) > 1:
        parts = [sum(parts[i : i + 2]) for i in range(0, len(parts), 2)]
    return parts[0]


def local_pass(out_ref, k_ref, v_ref, sum_ref, block_move):
    sp = sp_index()
    blocks = out_ref.shape[0] - 1
    query_at = lax.broadcasted_iota(jnp.int32, (4 * WINDOW, WINDOW), 0) % WINDOW
    key_at = lax.broadcasted_iota(jnp.int32, (4 * WINDOW, WINDOW), 1)
    in_before, in_after = key_at >= query_at, key_at <= query_at

    sum_ref[...] = jnp.zeros(sum_ref.shape, F32)

    def one(block):
        near = pl.ds(pl.multiple_of(block * WINDOW, WINDOW), 3 * WINDOW)
        no_before = (block == 0) & (sp == 0)
        no_after = (block == blocks - 1) & (sp == NZ * NY - 1)
        local = jnp.exp2(contract_last(out_ref[block, :, :HEAD_DIM], k_ref[near, :]))
        local = jnp.concatenate(
            [
                jnp.where(in_before & jnp.logical_not(no_before), local[:, :WINDOW], 0.0),
                local[:, WINDOW : 2 * WINDOW],
                jnp.where(in_after & jnp.logical_not(no_after), local[:, 2 * WINDOW :], 0.0),
            ],
            axis=1,
        )
        total = jnp.sum(lanes_summed(local), axis=-1, keepdims=True)
        mixed = jnp.dot(local.astype(BF16), v_ref[near, :], preferred_element_type=F32)
        return total, mixed.astype(BF16)

    def body(i, carry):
        pair = (2 * i, 2 * i + 1)
        found = [one(block) for block in pair]
        sums = sum_ref[...]
        for block, (total, mixed) in zip(pair, found):
            sums = jnp.where(key_at == block, total, sums)
            out_ref[block, :, HEAD_DIM:] = mixed
        sum_ref[...] = sums
        for block in pair:
            block_move(block).start()
        return carry

    lax.fori_loop(0, blocks // 2, body, 0)
    high = sum_ref[...].astype(BF16)
    out_ref[blocks, :, :HEAD_DIM] = high
    out_ref[blocks, :, HEAD_DIM:] = (sum_ref[...] - high.astype(F32)).astype(BF16)
    block_move(blocks).start()


def attend_kernel(shifts, packed_ref, ctx_ref, sink_ref, *out_refs):
    head = HEAD_DIM
    last = packed_ref.shape[0] - 1
    tp = lax.axis_index("tp")
    sink = jnp.concatenate(
        [jnp.exp(jnp.full((WINDOW, 1), sink_ref[0, h], F32)) for h in range(4)], axis=0
    )
    lane = lax.broadcasted_iota(jnp.int32, (4 * WINDOW, 128), 1)
    sums = packed_ref[last, :, :head].astype(F32) + packed_ref[last, :, head:].astype(F32)

    for by, out_ref in zip(shifts, out_refs):
        quarter = (tp + by) % NX

        def body(i, carry, quarter=quarter, out_ref=out_ref):
            block = quarter * 2 + i
            base = pl.ds(pl.multiple_of(i * WINDOW, WINDOW), WINDOW)
            far = jnp.exp2(contract_last(packed_ref[block, :, :head], ctx_ref[:, :head]))
            near_sum = jnp.where(lane == block, sums, 0.0)
            total = jnp.sum(lanes_summed(far) + near_sum, axis=-1, keepdims=True) + sink
            mixed = packed_ref[block, :, head:].astype(F32) + jnp.dot(
                far.astype(BF16), ctx_ref[:, head:], preferred_element_type=F32
            )
            mixed = (mixed * (1.0 / total)).astype(BF16)
            for h in range(4):
                out_ref[base, h * head : (h + 1) * head] = mixed[h * WINDOW : (h + 1) * WINDOW]
            return carry

        lax.fori_loop(0, 2, body, 0)


def early_kernel(a0_ref, a2_ref, w0_ref, m2_in, o2_ref, sum_ref, m2_ref, sem):
    dp = lax.axis_index("dp")
    col = 512
    move = pltpu.make_async_copy(m2_in, m2_ref, sem)
    move.start()
    for part, weight in enumerate((o2_ref, m2_ref)):
        half = 1 - dp if part == 0 else dp
        if part == 1:
            move.wait()

        def body(j, carry, weight=weight, half=half):
            wide = pl.ds(pl.multiple_of(half * (D // 2) + j * col, col), col)
            sub = pl.ds(pl.multiple_of(j * col, col), col)
            sum_ref[:, wide] = jnp.dot(
                a0_ref[...], w0_ref[:, wide], preferred_element_type=F32
            ) + jnp.dot(a2_ref[...], weight[:, sub], preferred_element_type=F32)
            return carry

        lax.fori_loop(0, 2, body, 0)


def project_kernel(
    vec_ref, sum_ref, a1_ref, a3_ref, m1_in, m3_in, o1_ref, o3_ref, lat_ref, out_ref,
    m1_ref, m3_ref, done_ref, sems,
):
    dp = lax.axis_index("dp")
    col = 512
    moves = [
        pltpu.make_async_copy(source, to, sems.at[4 + i])
        for i, (source, to) in enumerate(((m1_in, m1_ref), (m3_in, m3_ref)))
    ]
    for move in moves:
        move.start()

    def copy(slot, column):
        return pltpu.make_async_copy(
            done_ref.at[slot], out_ref.at[:, pl.ds(column, col)], sems.at[slot]
        )

    for part, weights in enumerate(((o1_ref, o3_ref), (m1_ref, m3_ref))):
        half = 1 - dp if part == 0 else dp
        if part == 1:
            for move in moves:
                move.wait()

        def body(j, carry, part=part, weights=weights, half=half):
            column = pl.multiple_of(half * (D // 2) + j * col, col)
            wide = pl.ds(column, col)
            sub = pl.ds(pl.multiple_of(j * col, col), col)
            mixed = sum_ref[:, wide]
            for a, w in zip((a1_ref, a3_ref), weights):
                mixed = mixed + jnp.dot(a[...], w[:, sub], preferred_element_type=F32)
            slot = part * 2 + j
            result = lat_ref[:, wide].astype(F32) + vec_ref[2:3, wide] * mixed
            done_ref[slot] = result.astype(BF16)
            copy(slot, column).start()
            return carry

        lax.fori_loop(0, 2, body, 0)
    for slot in range(4):
        copy(slot, 0).wait()


def shifted(array, axis, by):
    peers = lax.axis_size(axis)
    return lax.ppermute(array, axis, [(i, (i + by) % peers) for i in range(peers)])


VMEM = pl.BlockSpec(memory_space=pltpu.VMEM)
SMEM = pl.BlockSpec(memory_space=pltpu.SMEM)
HBM = pl.BlockSpec(memory_space=pltpu.HBM)


def call(kernel, outs, args, estimate, limit, scratch=(), in_specs=None, out_specs=None):
    shapes = [jax.ShapeDtypeStruct(s, t) for s, t in outs]
    single = len(shapes) == 1
    return pl.pallas_call(
        kernel,
        in_specs=in_specs or [VMEM] * len(args),
        out_specs=out_specs or (VMEM if single else [VMEM] * len(shapes)),
        out_shape=shapes[0] if single else shapes,
        scratch_shapes=list(scratch),
        compiler_params=params(limit),
        cost_estimate=estimate,
    )(*args)


def per_device(
    latent, context, cond, ctx_cond, norm_gain, mod_shift, mod_scale, mod_gate,
    w_query, w_key, w_value, w_out, q_gain, k_gain, sinks,
):
    lat = latent[0]
    tok = lat.shape[0]
    sub = tok // NX
    width = 4 * HEAD_DIM

    peers = NZ * NY
    part = call(
        partial_kernel, [((NY * NX, 24, 128), BF16)],
        (cond, ctx_cond[None], mod_shift, mod_scale, mod_gate), cost(1 << 20, 1 << 18), 62,
        scratch=[
            pltpu.VMEM((1, D), F32), pltpu.VMEM((1, D), F32), pltpu.VMEM((64, 512), BF16),
            pltpu.VMEM((64, 512), BF16), pltpu.VMEM((64, 512), BF16),
            pltpu.SemaphoreType.DMA((5,)),
        ],
        in_specs=[HBM] * 5,
    )
    part = lax.all_to_all(part, ("y", "tp"), 0, 0, tiled=True)
    part = call(resum_kernel, [((NZ, NX * VECS, 128), BF16)], (part,), cost(1 << 20, 1 << 18), 4)
    mod = lax.all_to_all(part, "z", 0, 0, tiled=True)

    half = call(
        stage_weight_kernel, [((width, D // 2), BF16)], (w_out,),
        cost(1 << 24, 2 << 20), 60, scratch=[pltpu.SemaphoreType.DMA], in_specs=[HBM],
    )
    mine, other = {}, {}
    for s in (1, 3, 2):
        mine[s] = shifted(half, "tp", s)
        other[s] = shifted(mine[s], "dp", 1)

    rows = tok + 2 * WINDOW
    gain, qgain, kgain = norm_gain[None], q_gain[None], k_gain[None]
    n_ctx = context.shape[1]
    table, column_table = ((24, HEAD_DIM), F32), ((GRID_W, HEAD_DIM), F32)
    prepared, w_kv, row_cos, row_sin, col_cos, col_sin = call(
        prepare_kernel,
        [
            ((2 * WINDOW + n_ctx, D), BF16), ((D, 2 * HEAD_DIM), BF16),
            table, table, column_table, column_table,
        ],
        (lat, context[0], w_key, w_value), cost(1 << 24, 4 << 20), 60,
        scratch=[
            pltpu.VMEM((2 * WINDOW, D), BF16), pltpu.VMEM((n_ctx, D), BF16),
            pltpu.SemaphoreType.DMA((5,)),
        ],
        in_specs=[HBM] * 4,
    )
    edge = ((WINDOW, 2 * HEAD_DIM), BF16)
    ctx_kv, vec, first_kv, last_kv = call(
        context_kernel,
        [((peers, n_ctx, 2 * HEAD_DIM), BF16), ((8, D), F32), edge, edge],
        (mod, prepared, w_kv, gain, kgain, row_cos, row_sin, col_cos, col_sin),
        cost(2 * (n_ctx + 2 * WINDOW) * D * 256, D * 512), 63,
        scratch=[pltpu.VMEM((2 * WINDOW + n_ctx, D), BF16)],
    )
    up = [(i, i + 1) for i in range(peers - 1)]
    before = lax.ppermute(last_kv, SP, up)
    after = lax.ppermute(first_kv, SP, [(j, i) for i, j in up])
    ctx_all = lax.all_to_all(ctx_kv, SP, 0, 0, tiled=True).reshape(-1, 2 * HEAD_DIM)

    packed_shape = (tok // WINDOW + 1, 4 * WINDOW, 2 * HEAD_DIM)
    packed, own = call(
        qkv_kernel, [(packed_shape, BF16), ((sub, D), BF16)],
        (
            lat, w_query, w_kv, before, after, vec, qgain, kgain,
            row_cos, row_sin, col_cos, col_sin,
        ),
        cost(2 * tok * D * 768 + 16 * tok * 384 * HEAD_DIM, tok * D * 2 + D * 768 * 2), 60,
        scratch=[
            pltpu.VMEM(packed_shape, BF16),
            pltpu.VMEM((tok, D), BF16), pltpu.VMEM((D, width), BF16),
            pltpu.VMEM((D, 2 * HEAD_DIM), BF16),
            pltpu.VMEM((rows, HEAD_DIM), BF16), pltpu.VMEM((rows, HEAD_DIM), BF16),
            pltpu.VMEM((256, D), BF16), pltpu.VMEM((256, D), BF16),
            pltpu.VMEM((4 * WINDOW, 128), F32),
            pltpu.SemaphoreType.DMA((tok // 256 + 4 + packed_shape[0],)),
        ],
        in_specs=[HBM] * 3 + [VMEM] * 9,
        out_specs=[HBM, HBM],
    )

    arrived = {}
    for shifts in ((2,), (1, 3), (0,)):
        pieces = call(
            lambda *refs, shifts=shifts: attend_kernel(shifts, *refs),
            [((sub, width), BF16)] * len(shifts), (packed, ctx_all, sinks[None]),
            cost(16 * len(shifts) * sub * 768 * HEAD_DIM, 2 << 20, 4 * len(shifts) * sub * 768), 8,
            in_specs=[VMEM] * 2 + [SMEM],
        )
        for s, piece in zip(shifts, pieces if len(shifts) > 1 else [pieces]):
            if s == 0:
                arrived[s] = piece
            else:
                arrived[s] = shifted(piece, "tp", s)

    matrix = pltpu.VMEM((width, D // 2), BF16)
    early = call(
        early_kernel, [((sub, D), F32)],
        (arrived[0], arrived[2], w_out, mine[2], other[2]),
        cost(sub * D * D, D * D), 24,
        scratch=[matrix, pltpu.SemaphoreType.DMA], in_specs=[VMEM] * 3 + [HBM, VMEM],
    )
    result = call(
        project_kernel, [((sub, D), BF16)],
        (
            vec, early, arrived[1], arrived[3], mine[1], mine[3], other[1], other[3], own,
        ),
        cost(sub * D * D, D * D), 24,
        scratch=[
            matrix, matrix, pltpu.VMEM((4, sub, 512), BF16), pltpu.SemaphoreType.DMA((6,)),
        ],
        in_specs=[VMEM] * 4 + [HBM] * 2 + [VMEM] * 3,
        out_specs=HBM,
    )
    return result[None]


def solution(mesh):
    grid = Mesh(mesh.devices.reshape(NZ, NY, NX, 2), ("z", "y", "tp", "dp"))
    in_specs = (
        P("dp", SP, None),
        P("dp", SP, None),
        P("dp", None),
        P(),
        P(),
        P(SP, "tp"),
        P(SP, "tp"),
        P(SP, "tp"),
        P(None, "tp"),
        P(None, "tp"),
        P(None, "tp"),
        P("tp", None),
        P(),
        P(),
        P("tp"),
    )
    out_specs = P("dp", ("z", "y", "tp"), None)

    return jax.shard_map(
        per_device, mesh=grid, in_specs=in_specs, out_specs=out_specs, check_vma=False
    )
```

```python
import math

import jax
import jax.numpy as jnp
from jax import lax
from jax.experimental import pallas as pl
from jax.experimental.pallas import tpu as pltpu
from jax.sharding import Mesh, PartitionSpec as P


HEAD_DIM = 128
WINDOW = 128
GRID_W = 64
NORM_EPSILON = 1e-06
ROPE_BASE = 10000.0
D = 2048
VECS = 20
NZ, NY, NX = 8, 4, 4
SP = ("z", "y")

F32 = jnp.float32
BF16 = jnp.bfloat16
QUERY_SCALE = HEAD_DIM ** (-0.5) * math.log2(math.e)


def sp_index():
    return lax.axis_index("z") * NY + lax.axis_index("y")


def params(vmem_mib):
    return pltpu.CompilerParams(vmem_limit_bytes=vmem_mib * 1024 * 1024)


def cost(flops, nbytes, trans=0):
    return pl.CostEstimate(flops=flops, bytes_accessed=nbytes, transcendentals=trans)


def partial_kernel(cond_in, ctx_in, shift_in, scale_in, gate_in, out_ref,
                   cond_ref, ctx_ref, shift_ref, scale_ref, gate_ref, sems):
    moves = [
        pltpu.make_async_copy(source, to, sems.at[i])
        for i, (source, to) in enumerate(
            (
                (cond_in, cond_ref), (ctx_in, ctx_ref), (shift_in, shift_ref),
                (scale_in, scale_ref), (gate_in, gate_ref),
            )
        )
    ]
    for move in moves:
        move.start()
    for move in moves:
        move.wait()
    sp = sp_index()
    start = pl.multiple_of((sp // 2) * 128, 128)
    row = lax.broadcasted_iota(jnp.int32, (8, 128), 0)
    lane = lax.broadcasted_iota(jnp.int32, (8, 128), 1)
    rows = jnp.where(
        row == 0,
        cond_ref[:, pl.ds(start, 128)],
        jnp.where(row == 1, ctx_ref[:, pl.ds(start, 128)], 0.0),
    )
    active = rows / (1.0 + jnp.exp(-rows))
    active = jnp.where((lane // 64) == (sp % 2), active, 0.0).astype(BF16)

    def times(ref):
        matrix = ref[...]
        return jnp.dot(
            active, jnp.concatenate([matrix, matrix], axis=0), preferred_element_type=F32
        )

    shifts, scales, gates = times(shift_ref), times(scale_ref), times(gate_ref)
    pieces = []
    for values, at in ((shifts, 0), (scales, 0), (shifts, 1), (scales, 1), (gates, 0)):
        for i in range(4):
            pieces.append(values[at : at + 1, i * 128 : (i + 1) * 128])
    pieces.append(jnp.zeros((4, 128), F32))
    stacked = jnp.concatenate(pieces, axis=0).astype(BF16)
    out_ref[...] = jnp.broadcast_to(stacked[None], out_ref.shape)


def resum_kernel(in_ref, out_ref):
    pieces = []
    for t in range(NX):
        rows = None
        for y in range(NY):
            part = in_ref[y * NX + t].astype(F32)
            rows = part if rows is None else rows + part
        pieces.append(rows[:VECS])
    total = jnp.concatenate(pieces, axis=0).astype(BF16)
    out_ref[...] = jnp.broadcast_to(total[None], out_ref.shape)


def vectors_of(mod_ref):
    rows = None
    for z in range(NZ):
        part = mod_ref[z].astype(F32)
        rows = part if rows is None else rows + part
    found = []
    for v in range(5):
        pieces = []
        for t in range(NX):
            for i in range(4):
                at = t * VECS + v * 4 + i
                pieces.append(rows[at : at + 1, :])
        found.append(jnp.concatenate(pieces, axis=1))
    return found


def normed(values):
    values = values.astype(F32)
    return values * lax.rsqrt(jnp.mean(values * values, axis=-1, keepdims=True) + NORM_EPSILON)


def head_norm(v, gain):
    return v * lax.rsqrt(jnp.mean(v * v, axis=-1, keepdims=True) + NORM_EPSILON) * gain


def rotated(v, cosine, sine):
    lane = lax.broadcasted_iota(jnp.int32, v.shape, 1)
    odd = ((lane // 32) % 2) == 1
    swapped = jnp.where(odd, pltpu.roll(v, 32, 1), pltpu.roll(v, 96, 1))
    return v * cosine + swapped * sine


def stage_weight_kernel(w_in, half_ref, sem):
    start = pl.multiple_of(lax.axis_index("dp") * (D // 2), D // 2)
    move = pltpu.make_async_copy(w_in.at[:, pl.ds(start, D // 2)], half_ref, sem)
    move.start()
    move.wait()


def rotation(refs, groups):
    row_cos, row_sin, col_cos, col_sin = refs
    cosines = [row_cos[pl.ds(g, 1), :] + col_cos[...] for g in groups]
    sines = [row_sin[pl.ds(g, 1), :] + col_sin[...] for g in groups]
    return jnp.concatenate(cosines), jnp.concatenate(sines)


def fill_tables(first_row, cos_ref, sin_ref, rows):
    shape = cos_ref.shape
    quarter = HEAD_DIM // 4
    at = lax.broadcasted_iota(jnp.int32, shape, 0) + first_row
    lane = lax.broadcasted_iota(jnp.int32, shape, 1)
    frequency = jnp.exp((lane % quarter).astype(F32) * (-math.log(ROPE_BASE) / quarter))
    angle = at.astype(F32) * frequency
    wanted = (lane < HEAD_DIM // 2) == rows
    sign = jnp.where((lane // quarter) % 2 == 0, -1.0, 1.0)
    cos_ref[...] = jnp.where(wanted, jnp.cos(angle), 0.0)
    sin_ref[...] = jnp.where(wanted, jnp.sin(angle) * sign, 0.0)


def prepare_kernel(
    lat_in, ctx_in, wk_in, wv_in,
    rows_ref, wkv_ref, rcos_ref, rsin_ref, ccos_ref, csin_ref, edge_ref, ctx_ref, sems,
):
    tok = lat_in.shape[0]
    moves = [
        pltpu.make_async_copy(source, to, sems.at[i])
        for i, (source, to) in enumerate(
            (
                (lat_in.at[:WINDOW, :], edge_ref.at[:WINDOW]),
                (lat_in.at[tok - WINDOW :, :], edge_ref.at[WINDOW:]),
                (ctx_in, ctx_ref),
                (wk_in, wkv_ref.at[:, :HEAD_DIM]),
                (wv_in, wkv_ref.at[:, HEAD_DIM:]),
            )
        )
    ]
    for move in moves:
        move.start()
    fill_tables((sp_index() * tok - WINDOW) // GRID_W, rcos_ref, rsin_ref, True)
    fill_tables(0, ccos_ref, csin_ref, False)
    for move in moves[:3]:
        move.wait()
    step = 64

    def body(i, carry):
        at = pl.ds(pl.multiple_of(i * step, step), step)
        rows_ref[at, :] = normed(edge_ref[at, :]).astype(BF16)
        return carry

    lax.fori_loop(0, 2 * WINDOW // step, body, 0)
    rows_ref[2 * WINDOW :, :] = normed(ctx_ref[...]).astype(BF16)
    for move in moves[3:]:
        move.wait()


def context_kernel(
    mod_ref, rows_in, wkv_ref, gain_ref, kgain_ref, rcos_ref, rsin_ref, ccos_ref, csin_ref,
    kv_ref, vec_ref, first_ref, last_ref, rows_ref,
):
    shift_lat, scale_lat, shift_ctx, scale_ctx, gate = vectors_of(mod_ref)
    gain = gain_ref[...]
    vec_ref[0:1, :] = gain * (1.0 + scale_lat)
    vec_ref[1:2, :] = shift_lat
    vec_ref[2:3, :] = gate
    rows_ref[2 * WINDOW :, :] = (
        rows_in[2 * WINDOW :, :].astype(F32) * (gain * (1.0 + scale_ctx)) + shift_ctx
    ).astype(BF16)
    step = 64

    def body(i, carry):
        at = pl.ds(pl.multiple_of(i * step, step), step)
        rows = rows_in[at, :].astype(F32) * vec_ref[0:1, :] + vec_ref[1:2, :]
        rows_ref[at, :] = rows.astype(BF16)
        return carry

    lax.fori_loop(0, 2 * WINDOW // step, body, 0)
    both = jnp.dot(rows_ref[...], wkv_ref[...], preferred_element_type=F32)
    keys = head_norm(both[:, :HEAD_DIM], kgain_ref[...])
    values = both[:, HEAD_DIM:].astype(BF16)
    refs = (rcos_ref, rsin_ref, ccos_ref, csin_ref)
    final = 1024 // GRID_W
    for ref, base, groups in ((first_ref, 0, (2, 3)), (last_ref, WINDOW, (final, final + 1))):
        at = slice(base, base + WINDOW)
        ref[:, :HEAD_DIM] = rotated(keys[at], *rotation(refs, groups)).astype(BF16)
        ref[:, HEAD_DIM:] = values[at]
    both = jnp.concatenate([keys[2 * WINDOW :].astype(BF16), values[2 * WINDOW :]], axis=1)
    kv_ref[...] = jnp.broadcast_to(both[None], kv_ref.shape)


def qkv_kernel(
    lat_in, wq_in, wkv_in, before_ref, after_ref,
    vec_ref, qgain_ref, kgain_ref, rcos_ref, rsin_ref, ccos_ref, csin_ref,
    packed_out, own_ref, out_ref, lat_ref, wq_ref, wkv_ref, k_ref, v_ref, even_ref, odd_ref,
    sum_ref, sems,
):
    step = 256
    tok = lat_in.shape[0]
    steps = tok // step
    qgain = qgain_ref[...] * QUERY_SCALE
    kgain = kgain_ref[...]

    def at(i, size=step):
        return pl.ds(pl.multiple_of(i * step, step), size)

    sources = [(lat_in.at[at(i), :], lat_ref.at[at(i), :]) for i in range(steps)]
    sources += [
        (wkv_in, wkv_ref), (wq_in, wq_ref),
    ]
    moves = [
        pltpu.make_async_copy(source, to, sems.at[i]) for i, (source, to) in enumerate(sources)
    ]
    for i in (0, steps, steps + 1, *range(1, steps)):
        moves[i].start()
    for ref, edge in ((k_ref, slice(0, HEAD_DIM)), (v_ref, slice(HEAD_DIM, 2 * HEAD_DIM))):
        ref[:WINDOW, :] = before_ref[:, edge]
        ref[tok + WINDOW :, :] = after_ref[:, edge]
    refs = (rcos_ref, rsin_ref, ccos_ref, csin_ref)

    def fill(i, to):
        values = lat_ref[at(i), :].astype(F32)
        inverse = lax.rsqrt(jnp.mean(values * values, axis=-1, keepdims=True) + NORM_EPSILON)
        to[...] = (values * inverse * vec_ref[0:1, :] + vec_ref[1:2, :]).astype(BF16)

    def keys_of(rows_ref, cosine, sine):
        both = jnp.dot(rows_ref[...], wkv_ref[...], preferred_element_type=F32)
        keys = rotated(head_norm(both[:, :HEAD_DIM], kgain), cosine, sine).astype(BF16)
        return keys, both[:, HEAD_DIM:].astype(BF16)

    def project(i, rows_ref):
        to = pl.ds(pl.multiple_of(i * step + WINDOW, WINDOW), step)
        first = 2 + i * (step // GRID_W)
        cosine, sine = rotation(refs, [first + g for g in range(step // GRID_W)])
        queries = jnp.dot(rows_ref[...], wq_ref[...], preferred_element_type=F32)
        k_ref[to, :], v_ref[to, :] = keys_of(rows_ref, cosine, sine)
        for h in range(4):
            head = slice(h * HEAD_DIM, (h + 1) * HEAD_DIM)
            turned = rotated(head_norm(queries[:, head], qgain), cosine, sine).astype(BF16)
            for half in range(2):
                out_ref[i * 2 + half, h * WINDOW : (h + 1) * WINDOW, :HEAD_DIM] = turned[
                    half * WINDOW : (half + 1) * WINDOW
                ]

    moves[0].wait()
    fill(0, even_ref)
    for i in range(steps, steps + 2):
        moves[i].wait()

    def wait_rows(i):
        pltpu.make_async_copy(lat_in.at[at(0), :], lat_ref.at[at(i), :], sems.at[i]).wait()

    def body(j, carry):
        wait_rows(2 * j + 1)

        @pl.when(j == 0)
        def _():
            wait_rows(2)

        fill(2 * j + 1, odd_ref)
        project(2 * j, even_ref)
        fill(jnp.minimum(2 * j + 2, steps - 1), even_ref)
        project(2 * j + 1, odd_ref)
        return carry

    lax.fori_loop(0, steps // 2, body, 0)
    own_move = pltpu.make_async_copy(
        lat_ref.at[at(lax.axis_index("tp"), own_ref.shape[0]), :], own_ref, sems.at[steps + 3]
    )
    own_move.start()

    def block_move(block):
        return pltpu.make_async_copy(
            out_ref.at[block], packed_out.at[block], sems.at[steps + 4 + block]
        )

    local_pass(out_ref, k_ref, v_ref, sum_ref, block_move)
    for block in range(packed_out.shape[0]):
        block_move(block).wait()
    own_move.wait()


def contract_last(a, b):
    return lax.dot_general(a, b, (((1,), (1,)), ((), ())), preferred_element_type=F32)


def lanes_summed(values):
    parts = [values[:, i : i + 128] for i in range(0, values.shape[1], 128)]
    while len(parts) > 1:
        parts = [sum(parts[i : i + 2]) for i in range(0, len(parts), 2)]
    return parts[0]


def local_pass(out_ref, k_ref, v_ref, sum_ref, block_move):
    sp = sp_index()
    blocks = out_ref.shape[0] - 1
    query_at = lax.broadcasted_iota(jnp.int32, (4 * WINDOW, WINDOW), 0) % WINDOW
    key_at = lax.broadcasted_iota(jnp.int32, (4 * WINDOW, WINDOW), 1)
    in_before, in_after = key_at >= query_at, key_at <= query_at

    sum_ref[...] = jnp.zeros(sum_ref.shape, F32)

    def one(block):
        near = pl.ds(pl.multiple_of(block * WINDOW, WINDOW), 3 * WINDOW)
        no_before = (block == 0) & (sp == 0)
        no_after = (block == blocks - 1) & (sp == NZ * NY - 1)
        local = jnp.exp2(contract_last(out_ref[block, :, :HEAD_DIM], k_ref[near, :]))
        local = jnp.concatenate(
            [
                jnp.where(in_before & jnp.logical_not(no_before), local[:, :WINDOW], 0.0),
                local[:, WINDOW : 2 * WINDOW],
                jnp.where(in_after & jnp.logical_not(no_after), local[:, 2 * WINDOW :], 0.0),
            ],
            axis=1,
        )
        total = jnp.sum(lanes_summed(local), axis=-1, keepdims=True)
        mixed = jnp.dot(local.astype(BF16), v_ref[near, :], preferred_element_type=F32)
        return total, mixed.astype(BF16)

    def body(i, carry):
        pair = (2 * i, 2 * i + 1)
        found = [one(block) for block in pair]
        sums = sum_ref[...]
        for block, (total, mixed) in zip(pair, found):
            sums = jnp.where(key_at == block, total, sums)
            out_ref[block, :, HEAD_DIM:] = mixed
        sum_ref[...] = sums
        for block in pair:
            block_move(block).start()
        return carry

    lax.fori_loop(0, blocks // 2, body, 0)
    high = sum_ref[...].astype(BF16)
    out_ref[blocks, :, :HEAD_DIM] = high
    out_ref[blocks, :, HEAD_DIM:] = (sum_ref[...] - high.astype(F32)).astype(BF16)
    block_move(blocks).start()


def attend_kernel(shifts, packed_ref, ctx_ref, sink_ref, *out_refs):
    head = HEAD_DIM
    last = packed_ref.shape[0] - 1
    tp = lax.axis_index("tp")
    sink = jnp.concatenate(
        [jnp.exp(jnp.full((WINDOW, 1), sink_ref[0, h], F32)) for h in range(4)], axis=0
    )
    lane = lax.broadcasted_iota(jnp.int32, (4 * WINDOW, 128), 1)
    sums = packed_ref[last, :, :head].astype(F32) + packed_ref[last, :, head:].astype(F32)

    for by, out_ref in zip(shifts, out_refs):
        quarter = (tp + by) % NX

        for i in range(2):
            block = quarter * 2 + i
            base = slice(i * WINDOW, (i + 1) * WINDOW)
            far = jnp.exp2(contract_last(packed_ref[block, :, :head], ctx_ref[:, :head]))
            near_sum = jnp.where(lane == block, sums, 0.0)
            total = jnp.sum(lanes_summed(far) + near_sum, axis=-1, keepdims=True) + sink
            mixed = packed_ref[block, :, head:].astype(F32) + jnp.dot(
                far.astype(BF16), ctx_ref[:, head:], preferred_element_type=F32
            )
            mixed = (mixed * (1.0 / total)).astype(BF16)
            for h in range(4):
                out_ref[base, h * head : (h + 1) * head] = mixed[h * WINDOW : (h + 1) * WINDOW]


def early_kernel(a0_ref, a2_ref, w0_ref, m2_in, o2_ref, sum_ref, m2_ref, sem):
    dp = lax.axis_index("dp")
    col = 512
    move = pltpu.make_async_copy(m2_in, m2_ref, sem)
    move.start()
    for part, weight in enumerate((o2_ref, m2_ref)):
        half = 1 - dp if part == 0 else dp
        if part == 1:
            move.wait()

        def body(j, carry, weight=weight, half=half):
            wide = pl.ds(pl.multiple_of(half * (D // 2) + j * col, col), col)
            sub = pl.ds(pl.multiple_of(j * col, col), col)
            sum_ref[:, wide] = jnp.dot(
                a0_ref[...], w0_ref[:, wide], preferred_element_type=F32
            ) + jnp.dot(a2_ref[...], weight[:, sub], preferred_element_type=F32)
            return carry

        lax.fori_loop(0, 2, body, 0)


def project_kernel(
    vec_ref, sum_ref, a1_ref, a3_ref, m1_in, m3_in, o1_ref, o3_ref, lat_ref, out_ref,
    m1_ref, m3_ref, done_ref, sems,
):
    dp = lax.axis_index("dp")
    col = 512
    moves = [
        pltpu.make_async_copy(source, to, sems.at[4 + i])
        for i, (source, to) in enumerate(((m1_in, m1_ref), (m3_in, m3_ref)))
    ]
    for move in moves:
        move.start()

    def copy(slot, column):
        return pltpu.make_async_copy(
            done_ref.at[slot], out_ref.at[:, pl.ds(column, col)], sems.at[slot]
        )

    for part, weights in enumerate(((o1_ref, o3_ref), (m1_ref, m3_ref))):
        half = 1 - dp if part == 0 else dp
        if part == 1:
            for move in moves:
                move.wait()

        def body(j, carry, part=part, weights=weights, half=half):
            column = pl.multiple_of(half * (D // 2) + j * col, col)
            wide = pl.ds(column, col)
            sub = pl.ds(pl.multiple_of(j * col, col), col)
            mixed = sum_ref[:, wide]
            for a, w in zip((a1_ref, a3_ref), weights):
                mixed = mixed + jnp.dot(a[...], w[:, sub], preferred_element_type=F32)
            slot = part * 2 + j
            result = lat_ref[:, wide].astype(F32) + vec_ref[2:3, wide] * mixed
            done_ref[slot] = result.astype(BF16)
            copy(slot, column).start()
            return carry

        lax.fori_loop(0, 2, body, 0)
    for slot in range(4):
        copy(slot, 0).wait()


def shifted(array, axis, by):
    peers = lax.axis_size(axis)
    return lax.ppermute(array, axis, [(i, (i + by) % peers) for i in range(peers)])


VMEM = pl.BlockSpec(memory_space=pltpu.VMEM)
SMEM = pl.BlockSpec(memory_space=pltpu.SMEM)
HBM = pl.BlockSpec(memory_space=pltpu.HBM)


def call(kernel, outs, args, estimate, limit, scratch=(), in_specs=None, out_specs=None):
    shapes = [jax.ShapeDtypeStruct(s, t) for s, t in outs]
    single = len(shapes) == 1
    return pl.pallas_call(
        kernel,
        in_specs=in_specs or [VMEM] * len(args),
        out_specs=out_specs or (VMEM if single else [VMEM] * len(shapes)),
        out_shape=shapes[0] if single else shapes,
        scratch_shapes=list(scratch),
        compiler_params=params(limit),
        cost_estimate=estimate,
    )(*args)


def per_device(
    latent, context, cond, ctx_cond, norm_gain, mod_shift, mod_scale, mod_gate,
    w_query, w_key, w_value, w_out, q_gain, k_gain, sinks,
):
    lat = latent[0]
    tok = lat.shape[0]
    sub = tok // NX
    width = 4 * HEAD_DIM

    peers = NZ * NY
    part = call(
        partial_kernel, [((NY * NX, 24, 128), BF16)],
        (cond, ctx_cond[None], mod_shift, mod_scale, mod_gate), cost(1 << 20, 1 << 18), 62,
        scratch=[
            pltpu.VMEM((1, D), F32), pltpu.VMEM((1, D), F32), pltpu.VMEM((64, 512), BF16),
            pltpu.VMEM((64, 512), BF16), pltpu.VMEM((64, 512), BF16),
            pltpu.SemaphoreType.DMA((5,)),
        ],
        in_specs=[HBM] * 5,
    )
    part = lax.all_to_all(part, ("y", "tp"), 0, 0, tiled=True)
    part = call(resum_kernel, [((NZ, NX * VECS, 128), BF16)], (part,), cost(1 << 20, 1 << 18), 4)
    mod = lax.all_to_all(part, "z", 0, 0, tiled=True)

    half = call(
        stage_weight_kernel, [((width, D // 2), BF16)], (w_out,),
        cost(1 << 24, 2 << 20), 60, scratch=[pltpu.SemaphoreType.DMA], in_specs=[HBM],
    )
    mine, other = {}, {}
    for s in (1, 3, 2):
        mine[s] = shifted(half, "tp", s)
        other[s] = shifted(mine[s], "dp", 1)

    rows = tok + 2 * WINDOW
    gain, qgain, kgain = norm_gain[None], q_gain[None], k_gain[None]
    n_ctx = context.shape[1]
    table, column_table = ((24, HEAD_DIM), F32), ((GRID_W, HEAD_DIM), F32)
    prepared, w_kv, row_cos, row_sin, col_cos, col_sin = call(
        prepare_kernel,
        [
            ((2 * WINDOW + n_ctx, D), BF16), ((D, 2 * HEAD_DIM), BF16),
            table, table, column_table, column_table,
        ],
        (lat, context[0], w_key, w_value), cost(1 << 24, 4 << 20), 60,
        scratch=[
            pltpu.VMEM((2 * WINDOW, D), BF16), pltpu.VMEM((n_ctx, D), BF16),
            pltpu.SemaphoreType.DMA((5,)),
        ],
        in_specs=[HBM] * 4,
    )
    edge = ((WINDOW, 2 * HEAD_DIM), BF16)
    ctx_kv, vec, first_kv, last_kv = call(
        context_kernel,
        [((peers, n_ctx, 2 * HEAD_DIM), BF16), ((8, D), F32), edge, edge],
        (mod, prepared, w_kv, gain, kgain, row_cos, row_sin, col_cos, col_sin),
        cost(2 * (n_ctx + 2 * WINDOW) * D * 256, D * 512), 63,
        scratch=[pltpu.VMEM((2 * WINDOW + n_ctx, D), BF16)],
    )
    up = [(i, i + 1) for i in range(peers - 1)]
    before = lax.ppermute(last_kv, SP, up)
    after = lax.ppermute(first_kv, SP, [(j, i) for i, j in up])
    ctx_all = lax.all_to_all(ctx_kv, SP, 0, 0, tiled=True).reshape(-1, 2 * HEAD_DIM)

    packed_shape = (tok // WINDOW + 1, 4 * WINDOW, 2 * HEAD_DIM)
    packed, own = call(
        qkv_kernel, [(packed_shape, BF16), ((sub, D), BF16)],
        (
            lat, w_query, w_kv, before, after, vec, qgain, kgain,
            row_cos, row_sin, col_cos, col_sin,
        ),
        cost(2 * tok * D * 768 + 16 * tok * 384 * HEAD_DIM, tok * D * 2 + D * 768 * 2), 60,
        scratch=[
            pltpu.VMEM(packed_shape, BF16),
            pltpu.VMEM((tok, D), BF16), pltpu.VMEM((D, width), BF16),
            pltpu.VMEM((D, 2 * HEAD_DIM), BF16),
            pltpu.VMEM((rows, HEAD_DIM), BF16), pltpu.VMEM((rows, HEAD_DIM), BF16),
            pltpu.VMEM((256, D), BF16), pltpu.VMEM((256, D), BF16),
            pltpu.VMEM((4 * WINDOW, 128), F32),
            pltpu.SemaphoreType.DMA((tok // 256 + 4 + packed_shape[0],)),
        ],
        in_specs=[HBM] * 3 + [VMEM] * 9,
        out_specs=[HBM, HBM],
    )

    arrived = {}
    for shifts in ((2,), (1, 3), (0,)):
        pieces = call(
            lambda *refs, shifts=shifts: attend_kernel(shifts, *refs),
            [((sub, width), BF16)] * len(shifts), (packed, ctx_all, sinks[None]),
            cost(16 * len(shifts) * sub * 768 * HEAD_DIM, 2 << 20, 4 * len(shifts) * sub * 768), 8,
            in_specs=[VMEM] * 2 + [SMEM],
        )
        for s, piece in zip(shifts, pieces if len(shifts) > 1 else [pieces]):
            if s == 0:
                arrived[s] = piece
            else:
                arrived[s] = shifted(piece, "tp", s)

    matrix = pltpu.VMEM((width, D // 2), BF16)
    early = call(
        early_kernel, [((sub, D), F32)],
        (arrived[0], arrived[2], w_out, mine[2], other[2]),
        cost(sub * D * D, D * D), 24,
        scratch=[matrix, pltpu.SemaphoreType.DMA], in_specs=[VMEM] * 3 + [HBM, VMEM],
    )
    result = call(
        project_kernel, [((sub, D), BF16)],
        (
            vec, early, arrived[1], arrived[3], mine[1], mine[3], other[1], other[3], own,
        ),
        cost(sub * D * D, D * D), 24,
        scratch=[
            matrix, matrix, pltpu.VMEM((4, sub, 512), BF16), pltpu.SemaphoreType.DMA((6,)),
        ],
        in_specs=[VMEM] * 4 + [HBM] * 2 + [VMEM] * 3,
        out_specs=HBM,
    )
    return result[None]


def solution(mesh):
    grid = Mesh(mesh.devices.reshape(NZ, NY, NX, 2), ("z", "y", "tp", "dp"))
    in_specs = (
        P("dp", SP, None),
        P("dp", SP, None),
        P("dp", None),
        P(),
        P(),
        P(SP, "tp"),
        P(SP, "tp"),
        P(SP, "tp"),
        P(None, "tp"),
        P(None, "tp"),
        P(None, "tp"),
        P("tp", None),
        P(),
        P(),
        P("tp"),
    )
    out_specs = P("dp", ("z", "y", "tp"), None)

    return jax.shard_map(
        per_device, mesh=grid, in_specs=in_specs, out_specs=out_specs, check_vma=False
    )
```
